128 devices in a mesh: sp: 16 (over z, x), tp: 8 (over y, core).
Axes of the slice: x: 4, y: 4, z: 4, core: 2. Of those that a mesh axis runs over, the one named last changes fastest.
Arguments:
- queries: bfloat16 [16384, 1024], P('sp', 'tp'), may hold values from -6 to 6, as said below
- key_rows: bfloat16 [16384, 1024], P('sp', 'tp'), may hold values from -6 to 6, as said below
- value_rows: bfloat16 [16384, 1024], P('sp', 'tp'), may hold values from -6 to 6
- lambdas: float32 [8], P('tp'), may hold values from 0.3 to 0.8
- head_gain: float32 [128], replicated, may hold values from 0.1 to 1.9
- out_weight: bfloat16 [1024, 2048], replicated, may hold values from -0.1875 to 0.1875
- stream: bfloat16 [16384, 2048], P(('sp', 'tp')), may hold values from -6 to 6
- ffn_gain: float32 [2048], replicated, may hold values from 0.1 to 1.9
- routes: int32 [16384, 2], P(('sp', 'tp')), may hold values from 0 to 15, all different within a row; in each aligned block of 128 rows (0 to 127, 128 to 255, ...) at most 20 rows name the same one
- route_weight: float32 [16384, 2], P(('sp', 'tp')), may hold values from 0.1 to 1
- gate_weight: bfloat16 [16, 2048, 5120], P('sp', None, 'tp'), may hold values from -0.125 to 0.125
- up_weight: bfloat16 [16, 2048, 5120], P('sp', None, 'tp'), may hold values from -0.125 to 0.125
- down_weight: bfloat16 [16, 5120, 2048], P('sp', 'tp'), may hold values from -0.078125 to 0.078125
Outputs:
- layer_out: bfloat16 [16384, 2048], P(('sp', 'tp'))
The draws below stay inside these ranges and needn't reach their ends.
Inputs may be any that keep to these rules, and one draw needn't show every extreme that they name: Custom draw; the queries of a position meet only keys of the same or earlier positions. `key_rows`: custom draw. `routes`: each row names 2 different experts. In the 128 rows of one device no expert is named by more than 20 rows, and every draw reaches 20 on some device.
All inputs are finite; a program needn't handle non-finite values.
Results may differ from the reference program's by a relative error of at most 0.01.
Values may be sent and summed in bfloat16 or wider, within the bound.
A program may use at most 128 MiB of HBM per device.

```python
import math
import jax
import jax.numpy as jnp
import numpy as np
from jax import lax

D = 2048
HEADS = 8
DH = 64
FE = 5120
TOPK = 2
TOKENS = 16384
TOK_POST = 128
EXPERTS = 16
SLOTS = 20
N_TP = 8


def draw_pair(key):
    width = HEADS * 2 * DH
    base_query = jax.random.fold_in(key, 101)
    base_key = jax.random.fold_in(key, 202)
    query_part = jnp.clip(1.3 * jax.random.normal(base_query, (TOKENS, width), jnp.float32), -6.0, 6.0)
    key_part = jnp.clip(1.3 * jax.random.normal(base_key, (TOKENS, width), jnp.float32), -6.0, 6.0)
    return (query_part, key_part)


def draw_queries(key, part):
    return draw_pair(key)[0].astype(jnp.bfloat16)


def draw_key_rows(key, part):
    return draw_pair(key)[1].astype(jnp.bfloat16)


def block_levels(stream_key, dims, split, least, high):
    def one(axis_at, blocks):
        draws = jax.random.uniform(jax.random.fold_in(jax.random.fold_in(stream_key, 6), axis_at), (blocks,), jnp.float32, least / len(split), high / len(split))
        return jnp.repeat(jnp.exp(draws), dims[axis_at] // blocks).reshape((-1,) + (1,) * (len(dims) - axis_at - 1))

    loudness = one(*split[0])
    for cut in split[1:]:
        loudness = loudness * one(*cut)
    return loudness


def deal_out(own_key, own, number, rows, number_of, top, bound, slope):
    sequence = jax.random.permutation(own_key, number_of)
    packed, ordinary = load_shares(number_of, rows * top, bound, slope, True), load_shares(number_of, rows * top, bound, slope, False)
    places = jnp.arange(number_of)

    def named(tallies, offset_by):
        used = int((tallies > 0).sum())
        fixed = max(1, used // 4)
        passed = fixed + (places - fixed + offset_by * (used - fixed)) % max(1, number_of - fixed)
        return jnp.zeros((number_of,), jnp.int32).at[sequence[jnp.where(places < fixed, places, passed)]].set(jnp.asarray(tallies, jnp.int32))

    tallies = jnp.where(number % 4 == 0, named(packed, number // 4), named(ordinary, number - number // 4 - 1))
    mixed = jax.random.permutation(jax.random.fold_in(own, 3), number_of)
    donor, taker = mixed[0:number_of // 2 * 2:2], mixed[1:number_of // 2 * 2:2]
    margin = jnp.minimum(tallies[donor] - 1, bound - tallies[taker]) // 2
    margin = jnp.where((donor == sequence[0]) | (taker == sequence[0]) | (tallies[taker] == 0), 0, jnp.maximum(margin, 0))
    passed = jax.random.randint(jax.random.fold_in(own, 4), (number_of // 2,), 0, 1 << 20) % (margin + 1)
    tallies = tallies.at[donor].add(-passed).at[taker].add(passed)
    members = jnp.searchsorted(jnp.cumsum(tallies), jnp.arange(rows * top), side="right").astype(jnp.int32)
    listing = members.reshape(top, rows).T
    listing = listing[jax.random.permutation(jax.random.fold_in(own, 1), rows)]
    offset_by = jax.random.randint(jax.random.fold_in(own, 2), (rows, 1), 0, top)
    return jnp.take_along_axis(listing, (jnp.arange(top)[None, :] + offset_by) % top, axis=1)


def load_shares(amount, total, bound, lean, full):
    portions = [(1 << 20) // math.isqrt(grade ** lean) + 1 for grade in range(1, amount + 1)]
    largest = bound if full else min(bound, max(-(-total // amount), total * portions[0] // sum(portions)))
    least = 1 if total - largest >= amount - 1 else 0
    counts, surplus = [largest] + [least] * (amount - 1), total - largest - least * (amount - 1)
    while surplus > 0:
        free = [i for i in range(1, amount) if counts[i] < largest] or [i for i in range(1, amount) if counts[i] < bound]
        pool, budget = sum([portions[i] for i in free]), surplus
        for i in free:
            addition = min(bound - counts[i], max(1, budget * portions[i] // pool), surplus)
            counts[i] = counts[i] + addition
            surplus = surplus - addition
    return np.array(counts)


def normal_values(rng, dims, scale, limit, pieces=(), kind=jnp.bfloat16):
    entries = jax.random.normal(rng, dims, jnp.float32) * scale
    if len(pieces) > 0:
        entries = block_levels(rng, dims, pieces, -0.22, 0.18) * entries
    return jnp.clip(entries, min=-limit, max=limit).astype(kind)


def setup_inputs(seed: int = 0) -> dict:
    streams_of = jax.random.split(jax.random.key(seed), 14)
    queries = draw_queries(jax.random.fold_in(streams_of[13], 71), 0)
    key_rows = draw_key_rows(jax.random.fold_in(streams_of[13], 71), 0)
    value_rows = normal_values(streams_of[2], (TOKENS, HEADS * 2 * DH), 1.0, 6.0, ((0, 16), (1, 8)))
    lambdas = jnp.clip(0.3 + 0.5 * jax.random.uniform(streams_of[3], (HEADS,), jnp.float32) ** block_levels(streams_of[3], (HEADS,), ((0, 8),), -0.2, 0.2), 0.3, 0.8)
    head_gain = jnp.clip(1.0 + 0.18 * jax.random.normal(streams_of[4], (2 * DH,), jnp.float32), 0.1, 1.9)
    out_weight = normal_values(streams_of[5], (HEADS * 2 * DH, D), (HEADS * 2 * DH) ** -0.5, 0.1875)
    stream = normal_values(streams_of[6], (TOKENS, D), 1.0, 6.0, ((0, 128),))
    ffn_gain = jnp.clip(1.0 + 0.18 * jax.random.normal(streams_of[7], (D,), jnp.float32), 0.1, 1.9)
    routes_keys = jax.random.split(jax.random.fold_in(streams_of[8], 1), TOKENS // TOK_POST)
    routes_turns = jax.random.permutation(jax.random.fold_in(streams_of[8], 3), TOKENS // TOK_POST)
    routes = jax.vmap(lambda own, number: deal_out(jax.random.fold_in(streams_of[8], 2), own, number, TOK_POST, EXPERTS, TOPK, SLOTS, 1))(routes_keys, routes_turns).reshape((TOKENS, TOPK))
    route_weight = jnp.clip(0.1 + 0.9 * jax.random.uniform(streams_of[9], (TOKENS, TOPK), jnp.float32) ** block_levels(streams_of[9], (TOKENS, TOPK), ((0, 128),), -0.2, 0.2), 0.1, 1.0)
    gate_weight = normal_values(streams_of[10], (EXPERTS, D, FE), D ** -0.5, 0.125, ((0, 16), (2, 8)))
    up_weight = normal_values(streams_of[11], (EXPERTS, D, FE), D ** -0.5, 0.125, ((0, 16), (2, 8)))
    down_weight = normal_values(streams_of[12], (EXPERTS, FE, D), FE ** -0.5, 0.078125, ((0, 16), (1, 8)))
    return dict(queries=queries, key_rows=key_rows, value_rows=value_rows, lambdas=lambdas, head_gain=head_gain, out_weight=out_weight, stream=stream, ffn_gain=ffn_gain, routes=routes, route_weight=route_weight, gate_weight=gate_weight, up_weight=up_weight, down_weight=down_weight)


def attention(queries, key_rows, value_rows, lambdas, head_gain):
    tokens = queries.shape[0]
    q_all = queries.astype(jnp.float32).reshape(tokens, HEADS, 2, DH)
    k_all = key_rows.astype(jnp.float32).reshape(tokens, HEADS, 2, DH)
    v_all = value_rows.astype(jnp.float32).reshape(tokens, HEADS, 2 * DH)
    block = math.gcd(tokens, 256)
    key_pos = jnp.arange(tokens, dtype=jnp.int32)

    def attend(start):
        q_block = lax.dynamic_slice_in_dim(q_all, start, block, 0)
        scores = jnp.einsum('qhmd,khmd->hmqk', q_block, k_all) * DH ** (-0.5)
        query_pos = start + jnp.arange(block, dtype=jnp.int32)
        mask = key_pos[None, :] <= query_pos[:, None]
        scores = jnp.where(mask, scores, -jnp.inf)
        top = lax.optimization_barrier(jnp.max(scores, axis=-1, keepdims=True))
        expo = jnp.exp(scores - top)
        total = lax.optimization_barrier(jnp.sum(expo, axis=-1))
        weights = lax.optimization_barrier(expo.astype(jnp.bfloat16)).astype(jnp.float32)
        mixed = jnp.einsum('hmqk,khe->hmqe', weights, v_all) / total[..., None]
        contrast = mixed[:, 0] - lambdas[:, None, None] * mixed[:, 1]
        contrast = contrast * lax.rsqrt(lax.optimization_barrier(jnp.mean(contrast * contrast, axis=-1, keepdims=True)) + 1e-05) * head_gain
        return jnp.transpose(contrast, (1, 0, 2)).reshape(block, HEADS * 2 * DH).astype(jnp.bfloat16)
    starts = jnp.arange(tokens // block, dtype=jnp.int32) * block
    return lax.map(attend, starts).reshape(tokens, HEADS * 2 * DH)

def reference(queries, key_rows, value_rows, lambdas, head_gain, out_weight, stream, ffn_gain, routes, route_weight, gate_weight, up_weight, down_weight):
    tokens = queries.shape[0]
    heads_out = attention(queries, key_rows, value_rows, lambdas, head_gain)
    attended = stream.astype(jnp.float32) + jnp.dot(heads_out, out_weight, preferred_element_type=jnp.float32)
    normed = (attended * lax.rsqrt(lax.optimization_barrier(jnp.mean(attended * attended, axis=-1, keepdims=True)) + 1e-06) * ffn_gain).astype(jnp.bfloat16)
    capacity = tokens // TOK_POST * SLOTS

    def expert(carry, index):
        hits = routes == index
        weight = lax.optimization_barrier(jnp.sum(jnp.where(hits, route_weight, 0.0), axis=1))
        chosen = jnp.any(hits, axis=1)
        count = jnp.sum(chosen.astype(jnp.int32))
        picked = jnp.nonzero(chosen, size=capacity, fill_value=0)[0].astype(jnp.int32)
        rows = normed[picked]
        gate = jnp.dot(rows, gate_weight[index], preferred_element_type=jnp.float32)
        upper = jnp.dot(rows, up_weight[index], preferred_element_type=jnp.float32)
        act = (jax.nn.silu(gate) * upper).astype(jnp.bfloat16)
        parts = jnp.einsum('rcf,cfd->rcd', act.astype(jnp.float32).reshape(capacity, N_TP, FE // N_TP), down_weight[index].astype(jnp.float32).reshape(N_TP, FE // N_TP, D))
        parts = lax.optimization_barrier(parts.astype(jnp.bfloat16)).astype(jnp.float32)
        summed = lax.optimization_barrier(lax.optimization_barrier(jnp.sum(parts, axis=1)).astype(jnp.bfloat16)).astype(jnp.float32)
        valid = jnp.arange(capacity, dtype=jnp.int32) < count
        scale = jnp.where(valid, weight[picked], 0.0)
        return (carry.at[picked].add(summed * scale[:, None]), None)
    start = jnp.zeros((tokens, D), jnp.float32)
    routed, _ = lax.scan(expert, start, jnp.arange(EXPERTS, dtype=jnp.int32))
    return (attended + routed).astype(jnp.bfloat16)
```

```python
import jax
import jax.numpy as jnp
from jax import lax
from jax.experimental import pallas as pl
from jax.experimental.pallas import tpu as pltpu
from jax.sharding import PartitionSpec as P

DH = 64


LOG2E = 1.4426950408889634
MESH = pl.DeviceIdType.MESH
NZ = 4
NX = 4
BLK = 1024
HALF = 512
ORDER = (
    (0, 0), (0, -1), (0, 1), (-1, 0), (1, 0), (-1, -1), (-1, 1), (1, -1), (1, 1),
    (0, 2), (2, 0), (-1, 2), (2, -1), (1, 2), (2, 1), (2, 2),
)
EVENTS = {
    1: [((0, -1), (-1, 0)), ((0, 1), (1, 0)), ((-1, 0), (0, -1)), ((1, 0), (0, 1))],
    3: [((0, 2), (2, 0))],
    5: [((-1, -1), (-1, -1)), ((1, -1), (-1, 1))],
    6: [((-1, 1), (1, -1)), ((1, 1), (1, 1))],
    9: [((2, 0), (0, 2))],
    10: [((-1, 2), (2, -1)), ((1, 2), (2, 1))],
    11: [((2, -1), (-1, 2))],
    13: [((2, 1), (1, 2))],
    15: [((2, 2), (2, 2))],
}


def attention_kernel(
    lam_ref, gain_ref, q_hbm, k_hbm, v_hbm, out_ref,
    kv, qin, qs, mx, acc, obuf,
    load_sem, qsend, qrecv, send_sem, recv_sem, osend, orecv,
):
    s = lax.axis_index("sp")
    t = lax.axis_index("tp")
    z, x = s // NX, s % NX
    mirror = NZ * NX - 1 - s

    def at(dz, dx):
        return ((z + dz + NZ) % NZ) * NX + (x + dx + NX) % NX

    loads = [
        pltpu.make_async_copy(q_hbm.at[pl.ds(HALF, HALF), :], qin.at[2], load_sem.at[0]),
        pltpu.make_async_copy(k_hbm, kv.at[0, s], load_sem.at[1]),
        pltpu.make_async_copy(v_hbm, kv.at[1, s], load_sem.at[2]),
        pltpu.make_async_copy(q_hbm.at[pl.ds(0, HALF), :], qin.at[0], load_sem.at[3]),
    ]
    for load in loads:
        load.start()

    barrier = pltpu.get_barrier_semaphore()
    for dz, dx in ((0, 1), (0, -1), (1, 0), (-1, 0)):
        pl.semaphore_signal(barrier, inc=1, device_id=(at(dz, dx), t), device_id_type=MESH)
    for j in range(1, 8):
        pl.semaphore_signal(barrier, inc=1, device_id=(s, (t + j) % 8), device_id_type=MESH)
    for j in range(8):
        pl.semaphore_signal(barrier, inc=1, device_id=(mirror, j), device_id_type=MESH)
    pl.semaphore_wait(barrier, 19)

    def remote_q():
        return pltpu.make_async_remote_copy(
            src_ref=qin.at[2], dst_ref=qin.at[1], send_sem=qsend, recv_sem=qrecv,
            device_id=(mirror, t), device_id_type=MESH,
        )

    def block_copy(which, block, part, lane, device):
        rows = pl.ds(0, BLK) if part == 2 else pl.ds(part * HALF, HALF)
        return pltpu.make_async_remote_copy(
            src_ref=kv.at[which, block, rows, :],
            dst_ref=kv.at[which, block, rows, :],
            send_sem=send_sem.at[which, block, lane],
            recv_sem=recv_sem.at[which, block, part % 2],
            device_id=(device, t), device_id_type=MESH,
        )

    lanes = ((0, 1), (0, -1), (1, 0), (-1, 0))

    def sends(which, d):
        first = which
        dz, dx = d
        near, far = (dx, dz) if first == 0 else (dz, dx)
        near_lanes, far_lanes = ((0, 1), (2, 3)) if first == 0 else ((2, 3), (0, 1))
        if d == (0, 0):
            return [(2, near_lanes[0]), (2, near_lanes[1]), (2, far_lanes[0]), (2, far_lanes[1])]
        if far == 0:
            out = [(2, far_lanes[0]), (2, far_lanes[1])]
            if near == -1:
                out = [(0, near_lanes[0])] + out
            if near == 1:
                out = [(1, near_lanes[1])] + out
            return out
        if far == -1:
            return [(0, far_lanes[0])]
        if far == 1:
            return [(1, far_lanes[1])]
        return []

    def halves(which, d):
        dz, dx = d
        near, far = (dx, dz) if which == 0 else (dz, dx)
        return far == 2 or (far == 0 and near == 2)

    def pass_on(which, d):
        block = at(*d)
        for part, lane in sends(which, d):
            block_copy(which, block, part, lane, at(*lanes[lane])).start()

    def arrive(which, d):
        block = at(*d)
        for part in (0, 1) if halves(which, d) else (2,):
            block_copy(which, block, part, 0, s).wait_recv()

    loads[0].wait()
    remote_q().start()
    loads[1].wait()
    loads[2].wait()
    own_k, own_v = sends(0, (0, 0)), sends(1, (0, 0))
    for which, part, lane in (
        [(0,) + own_k[0], (0,) + own_k[1], (1,) + own_v[0], (1,) + own_v[1]]
        + [(0,) + own_k[2], (0,) + own_k[3], (1,) + own_v[2], (1,) + own_v[3]]
    ):
        block_copy(which, s, part, lane, at(*lanes[lane])).start()
    loads[3].wait()

    mx[...] = jnp.full(mx.shape, -1e30, jnp.float32)
    acc[...] = jnp.zeros(acc.shape, jnp.float32)
    lane_ids = lax.broadcasted_iota(jnp.int32, (HALF, 2 * DH), 1)

    def split_maps(half):
        q = qin[half]
        zero = jnp.zeros_like(q)
        qs[half, 0] = jnp.where(lane_ids < DH, q, zero)
        qs[half, 1] = jnp.where(lane_ids < DH, zero, q)

    split_maps(0)
    remote_q().wait_recv()
    split_maps(1)

    scale = LOG2E * DH ** (-0.5)
    TQ = 256

    def tiles(half, block, masked):
        k = kv[0, block]
        v = kv[1, block]
        ones = jnp.ones_like(v)
        vv = jnp.concatenate([v, ones], axis=1)
        for m in range(2):
            for r in range(HALF // TQ):
                rows = pl.ds(r * TQ, TQ)
                scores = lax.dot_general(
                    qs[half, m, rows, :], k, (((1,), (1,)), ((), ())),
                    preferred_element_type=jnp.float32,
                ) * scale
                if masked:
                    row_id = lax.broadcasted_iota(jnp.int32, scores.shape, 0) + (half * HALF + r * TQ)
                    col_id = lax.broadcasted_iota(jnp.int32, scores.shape, 1)
                    scores = jnp.where(col_id <= row_id, scores, -1e30)
                old = mx[half, m, rows, :]
                new = jnp.maximum(old, jnp.max(scores, axis=1, keepdims=True))
                factor = jnp.exp2(old - new)
                wide = jnp.concatenate([new] * (BLK // 128), axis=1)
                weights = jnp.exp2(scores - wide).astype(jnp.bfloat16)
                pv = jnp.dot(weights, vv, preferred_element_type=jnp.float32)
                mx[half, m, rows, :] = new
                acc[half, m, rows, :] = acc[half, m, rows, :] * jnp.concatenate([factor, factor], axis=1) + pv

    def step(i, carry):
        for k, events in EVENTS.items():
            @pl.when(i == k)
            def _(events=events):
                for kd, vd in events:
                    arrive(0, kd)
                    pass_on(0, kd)
                    arrive(1, vd)
                    pass_on(1, vd)

        dz = jnp.int32(0)
        dx = jnp.int32(0)
        for k, (a, b) in enumerate(ORDER):
            dz = jnp.where(i == k, a, dz)
            dx = jnp.where(i == k, b, dx)
        block = at(dz, dx)

        def one_half(half, c):
            limit = jnp.where(half == 0, s, mirror)

            @pl.when(block < limit)
            def _():
                tiles(half, block, False)

            @pl.when(block == limit)
            def _():
                tiles(half, block, True)

            return c

        return lax.fori_loop(0, 2, one_half, carry)

    lax.fori_loop(0, NZ * NX, step, 0)

    lam = lam_ref[0]
    gain = gain_ref[...]
    for half in range(2):
        for r in range(HALF // 128):
            rows = pl.ds(r * 128, 128)
            mixed = [acc[half, m, rows, :128] / acc[half, m, rows, 128:] for m in range(2)]
            contrast = mixed[0] - lam * mixed[1]
            mean = jnp.mean(contrast * contrast, axis=1, keepdims=True)
            obuf[half, rows, :] = (contrast * lax.rsqrt(mean + 1e-05) * gain).astype(jnp.bfloat16)
    columns = pl.ds(pl.multiple_of(t * 128, 128), 128)

    def out_copy(half, j, sender):
        rows = pl.ds(j * 128, 128)
        cols = pl.ds(pl.multiple_of(sender * 128, 128), 128)
        return pltpu.make_async_remote_copy(
            src_ref=obuf.at[half, rows, :], dst_ref=out_ref.at[:, cols],
            send_sem=osend.at[half, j], recv_sem=orecv.at[sender],
            device_id=(s if half == 0 else mirror, 4 * half + j), device_id_type=MESH,
        )

    for j in range(4):
        out_copy(1, j, t).start()
        @pl.when(t != j)
        def _():
            out_copy(0, j, t).start()
        @pl.when(t == j)
        def _():
            out_ref[:, columns] = obuf[0, j * 128:(j + 1) * 128, :]
    for j in range(8):
        @pl.when(jnp.logical_or(t >= 4, t != j))
        def _():
            out_copy(0, 0, j).wait_recv()
    for j in range(4):
        out_copy(1, j, t).wait_send()
        @pl.when(t != j)
        def _():
            out_copy(0, j, t).wait_send()
    remote_q().wait_send()
    for which in range(2):
        for d in ORDER:
            for part, lane in sends(which, d):
                block_copy(which, at(*d), part, lane, s).wait_send()


def attention(lambdas, head_gain, queries, key_rows, value_rows):
    any_space = pl.BlockSpec(memory_space=pl.ANY)
    return pl.pallas_call(
        attention_kernel,
        out_shape=jax.ShapeDtypeStruct((128, 1024), jnp.bfloat16),
        in_specs=[
            pl.BlockSpec(memory_space=pltpu.SMEM),
            pl.BlockSpec(memory_space=pltpu.VMEM),
            any_space, any_space, any_space,
        ],
        out_specs=pl.BlockSpec(memory_space=pltpu.VMEM),
        scratch_shapes=[
            pltpu.VMEM((2, NZ * NX, BLK, 128), jnp.bfloat16),
            pltpu.VMEM((3, HALF, 128), jnp.bfloat16),
            pltpu.VMEM((2, 2, HALF, 128), jnp.bfloat16),
            pltpu.VMEM((2, 2, HALF, 128), jnp.float32),
            pltpu.VMEM((2, 2, HALF, 256), jnp.float32),
            pltpu.VMEM((2, HALF, 128), jnp.bfloat16),
            pltpu.SemaphoreType.DMA((4,)),
            pltpu.SemaphoreType.DMA,
            pltpu.SemaphoreType.DMA,
            pltpu.SemaphoreType.DMA((2, NZ * NX, 4)),
            pltpu.SemaphoreType.DMA((2, NZ * NX, 2)),
            pltpu.SemaphoreType.DMA((2, 4)),
            pltpu.SemaphoreType.DMA((8,)),
        ],
        compiler_params=pltpu.CompilerParams(
            collective_id=0, has_side_effects=True, vmem_limit_bytes=48 * 1024 * 1024
        ),
        name="attention",
    )(lambdas, head_gain.reshape(1, -1), queries, key_rows, value_rows)


def expert_rows(rows_in, gate_local, up_local, down_local):
    flat = rows_in.reshape(-1, rows_in.shape[-1])
    gate = jnp.dot(flat, gate_local, preferred_element_type=jnp.float32)
    upper = jnp.dot(flat, up_local, preferred_element_type=jnp.float32)
    act = (jax.nn.silu(gate) * upper).astype(jnp.bfloat16)
    result = jnp.dot(act, down_local, preferred_element_type=jnp.float32)
    return result.reshape(rows_in.shape)


def local(
    queries,
    key_rows,
    value_rows,
    lambdas,
    head_gain,
    out_weight,
    stream,
    ffn_gain,
    routes,
    route_weight,
    gate_weight,
    up_weight,
    down_weight,
):
    heads_local = attention(lambdas, head_gain, queries, key_rows, value_rows)
    attended = stream.astype(jnp.float32) + jnp.dot(
        heads_local, out_weight, preferred_element_type=jnp.float32
    )
    normed = (
        attended
        * lax.rsqrt(jnp.mean(attended * attended, axis=-1, keepdims=True) + 1e-06)
        * ffn_gain
    ).astype(jnp.bfloat16)
    rows_local = normed.shape[0]
    width = normed.shape[1]
    top_count = routes.shape[1]
    sp_size = lax.axis_size("sp")
    experts = sp_size * gate_weight.shape[0]
    slots = max(2, (rows_local * top_count * 5 + 4 * experts - 1) // (4 * experts))
    flat_routes = routes.reshape(-1)
    onehot = (flat_routes[:, None] == jnp.arange(experts, dtype=jnp.int32)[None, :]).astype(
        jnp.int32
    )
    before = jnp.cumsum(onehot, axis=0) - onehot
    slot = jnp.sum(before * onehot, axis=1)
    target = flat_routes * slots + slot
    placed = (target[:, None] == jnp.arange(experts * slots, dtype=jnp.int32)[None, :]).astype(
        jnp.float32
    )
    placed = placed.reshape(rows_local, top_count, experts * slots)
    dispatch = jnp.transpose(jnp.sum(placed, axis=1)).astype(jnp.bfloat16)
    combine = jnp.einsum("tk,tks->ts", route_weight, placed)
    outgoing = (
        jnp.dot(dispatch, normed, preferred_element_type=jnp.float32)
        .astype(jnp.bfloat16)
        .reshape(experts, slots, width)
    )
    gate_local = gate_weight[0]
    up_local = up_weight[0]
    down_local = down_weight[0]
    arrived = lax.all_to_all(outgoing, "sp", split_axis=0, concat_axis=0, tiled=True)
    partial_value = expert_rows(
        lax.all_gather(arrived[:, None], "tp", axis=1, tiled=True), gate_local, up_local, down_local
    )
    summed = lax.psum_scatter(
        partial_value.astype(jnp.bfloat16), "tp", scatter_dimension=1, tiled=True
    )
    returned = lax.all_to_all(summed, "sp", split_axis=0, concat_axis=0, tiled=True).reshape(
        experts * slots, width
    )
    routed = jnp.dot(combine, returned.astype(jnp.float32))
    return (attended + routed).astype(jnp.bfloat16)


def solution(mesh):
    placed = (
        P("sp", "tp"),
        P("sp", "tp"),
        P("sp", "tp"),
        P("tp"),
        P(),
        P(),
        P(("sp", "tp"), None),
        P(),
        P(("sp", "tp"), None),
        P(("sp", "tp"), None),
        P("sp", None, "tp"),
        P("sp", None, "tp"),
        P("sp", "tp", None),
    )
    return jax.shard_map(
        local, mesh=mesh, in_specs=placed, out_specs=P(("sp", "tp"), None), check_vma=False
    )
```

```python
import jax
import jax.numpy as jnp
from jax import lax
from jax.experimental import pallas as pl
from jax.experimental.pallas import tpu as pltpu
from jax.sharding import PartitionSpec as P

DH = 64


LOG2E = 1.4426950408889634
MESH = pl.DeviceIdType.MESH
NZ = 4
NX = 4
BLK = 1024
HALF = 512
ORDER = (
    (0, 0), (0, -1), (0, 1), (-1, 0), (1, 0), (-1, -1), (-1, 1), (1, -1), (1, 1),
    (0, 2), (2, 0), (-1, 2), (2, -1), (1, 2), (2, 1), (2, 2),
)
EVENTS = {
    1: [((0, -1), (-1, 0)), ((0, 1), (1, 0)), ((-1, 0), (0, -1)), ((1, 0), (0, 1))],
    3: [((0, 2), (2, 0))],
    5: [((-1, -1), (-1, -1)), ((1, -1), (-1, 1))],
    6: [((-1, 1), (1, -1)), ((1, 1), (1, 1))],
    9: [((2, 0), (0, 2))],
    10: [((-1, 2), (2, -1)), ((1, 2), (2, 1))],
    11: [((2, -1), (-1, 2))],
    13: [((2, 1), (1, 2))],
    15: [((2, 2), (2, 2))],
}


def attention_kernel(
    lam_ref, gain_ref, q_hbm, k_hbm, v_hbm, out_ref,
    kv, qin, qs, mx, acc, obuf,
    load_sem, qsend, qrecv, send_sem, recv_sem, osend, orecv,
):
    s = lax.axis_index("sp")
    t = lax.axis_index("tp")
    z, x = s // NX, s % NX
    mirror = NZ * NX - 1 - s

    def at(dz, dx):
        return ((z + dz + NZ) % NZ) * NX + (x + dx + NX) % NX

    loads = [
        pltpu.make_async_copy(q_hbm.at[pl.ds(HALF, HALF), :], qin.at[2], load_sem.at[0]),
        pltpu.make_async_copy(k_hbm, kv.at[0, s], load_sem.at[1]),
        pltpu.make_async_copy(v_hbm, kv.at[1, s], load_sem.at[2]),
        pltpu.make_async_copy(q_hbm.at[pl.ds(0, HALF), :], qin.at[0], load_sem.at[3]),
    ]
    for load in loads:
        load.start()

    barrier = pltpu.get_barrier_semaphore()
    for dz, dx in ((0, 1), (0, -1), (1, 0), (-1, 0)):
        pl.semaphore_signal(barrier, inc=1, device_id=(at(dz, dx), t), device_id_type=MESH)
    for j in range(1, 8):
        pl.semaphore_signal(barrier, inc=1, device_id=(s, (t + j) % 8), device_id_type=MESH)
    for j in range(8):
        pl.semaphore_signal(barrier, inc=1, device_id=(mirror, j), device_id_type=MESH)
    pl.semaphore_wait(barrier, 19)

    def remote_q():
        return pltpu.make_async_remote_copy(
            src_ref=qin.at[2], dst_ref=qin.at[1], send_sem=qsend, recv_sem=qrecv,
            device_id=(mirror, t), device_id_type=MESH,
        )

    def block_copy(which, block, part, lane, device):
        rows = pl.ds(0, BLK) if part == 2 else pl.ds(part * HALF, HALF)
        return pltpu.make_async_remote_copy(
            src_ref=kv.at[which, block, rows, :],
            dst_ref=kv.at[which, block, rows, :],
            send_sem=send_sem.at[which, block, lane],
            recv_sem=recv_sem.at[which, block, part % 2],
            device_id=(device, t), device_id_type=MESH,
        )

    lanes = ((0, 1), (0, -1), (1, 0), (-1, 0))

    def sends(which, d):
        first = which
        dz, dx = d
        near, far = (dx, dz) if first == 0 else (dz, dx)
        near_lanes, far_lanes = ((0, 1), (2, 3)) if first == 0 else ((2, 3), (0, 1))
        if d == (0, 0):
            return [(2, near_lanes[0]), (2, near_lanes[1]), (2, far_lanes[0]), (2, far_lanes[1])]
        if far == 0:
            out = [(2, far_lanes[0]), (2, far_lanes[1])]
            if near == -1:
                out = [(0, near_lanes[0])] + out
            if near == 1:
                out = [(1, near_lanes[1])] + out
            return out
        if far == -1:
            return [(0, far_lanes[0])]
        if far == 1:
            return [(1, far_lanes[1])]
        return []

    def halves(which, d):
        dz, dx = d
        near, far = (dx, dz) if which == 0 else (dz, dx)
        return far == 2 or (far == 0 and near == 2)

    def pass_on(which, d):
        block = at(*d)
        for part, lane in sends(which, d):
            block_copy(which, block, part, lane, at(*lanes[lane])).start()

    def arrive(which, d):
        block = at(*d)
        for part in (0, 1) if halves(which, d) else (2,):
            block_copy(which, block, part, 0, s).wait_recv()

    loads[0].wait()
    remote_q().start()
    loads[1].wait()
    loads[2].wait()
    own_k, own_v = sends(0, (0, 0)), sends(1, (0, 0))
    for which, part, lane in (
        [(0,) + own_k[0], (0,) + own_k[1], (1,) + own_v[0], (1,) + own_v[1]]
        + [(0,) + own_k[2], (0,) + own_k[3], (1,) + own_v[2], (1,) + own_v[3]]
    ):
        block_copy(which, s, part, lane, at(*lanes[lane])).start()
    loads[3].wait()

    mx[...] = jnp.full(mx.shape, -1e30, jnp.float32)
    acc[...] = jnp.zeros(acc.shape, jnp.float32)
    lane_ids = lax.broadcasted_iota(jnp.int32, (HALF, 2 * DH), 1)

    def split_maps(half):
        q = qin[half]
        zero = jnp.zeros_like(q)
        qs[half, 0] = jnp.where(lane_ids < DH, q, zero)
        qs[half, 1] = jnp.where(lane_ids < DH, zero, q)

    split_maps(0)
    remote_q().wait_recv()
    split_maps(1)

    scale = LOG2E * DH ** (-0.5)
    TQ = 256

    def tiles(half, block, masked):
        k = kv[0, block]
        v = kv[1, block]
        ones = jnp.ones_like(v)
        vv = jnp.concatenate([v, ones], axis=1)
        for m in range(2):
            for r in range(HALF // TQ):
                rows = pl.ds(r * TQ, TQ)
                scores = lax.dot_general(
                    qs[half, m, rows, :], k, (((1,), (1,)), ((), ())),
                    preferred_element_type=jnp.float32,
                ) * scale
                if masked:
                    row_id = lax.broadcasted_iota(jnp.int32, scores.shape, 0) + (half * HALF + r * TQ)
                    col_id = lax.broadcasted_iota(jnp.int32, scores.shape, 1)
                    scores = jnp.where(col_id <= row_id, scores, -1e30)
                old = mx[half, m, rows, :]
                new = jnp.maximum(old, jnp.max(scores, axis=1, keepdims=True))
                factor = jnp.exp2(old - new)
                wide = jnp.concatenate([new] * (BLK // 128), axis=1)
                weights = jnp.exp2(scores - wide).astype(jnp.bfloat16)
                pv = jnp.dot(weights, vv, preferred_element_type=jnp.float32)
                mx[half, m, rows, :] = new
                acc[half, m, rows, :] = acc[half, m, rows, :] * jnp.concatenate([factor, factor], axis=1) + pv

    def step(i, carry):
        for k, events in EVENTS.items():
            @pl.when(i == k)
            def _(events=events):
                for kd, vd in events:
                    arrive(0, kd)
                    pass_on(0, kd)
                    arrive(1, vd)
                    pass_on(1, vd)

        dz = jnp.int32(0)
        dx = jnp.int32(0)
        for k, (a, b) in enumerate(ORDER):
            dz = jnp.where(i == k, a, dz)
            dx = jnp.where(i == k, b, dx)
        block = at(dz, dx)

        def one_half(half, c):
            limit = jnp.where(half == 0, s, mirror)

            @pl.when(block < limit)
            def _():
                tiles(half, block, False)

            @pl.when(block == limit)
            def _():
                tiles(half, block, True)

            return c

        return lax.fori_loop(0, 2, one_half, carry)

    lax.fori_loop(0, NZ * NX, step, 0)

    lam = lam_ref[0]
    gain = gain_ref[...]
    for half in range(2):
        for r in range(HALF // 128):
            rows = pl.ds(r * 128, 128)
            mixed = [acc[half, m, rows, :128] / acc[half, m, rows, 128:] for m in range(2)]
            contrast = mixed[0] - lam * mixed[1]
            mean = jnp.mean(contrast * contrast, axis=1, keepdims=True)
            obuf[half, rows, :] = (contrast * lax.rsqrt(mean + 1e-05) * gain).astype(jnp.bfloat16)
    columns = pl.ds(pl.multiple_of(t * 128, 128), 128)

    def out_copy(half, j, sender):
        rows = pl.ds(j * 128, 128)
        cols = pl.ds(pl.multiple_of(sender * 128, 128), 128)
        return pltpu.make_async_remote_copy(
            src_ref=obuf.at[half, rows, :], dst_ref=out_ref.at[:, cols],
            send_sem=osend.at[half, j], recv_sem=orecv.at[sender],
            device_id=(s if half == 0 else mirror, 4 * half + j), device_id_type=MESH,
        )

    for j in range(4):
        out_copy(1, j, t).start()
        @pl.when(t != j)
        def _():
            out_copy(0, j, t).start()
        @pl.when(t == j)
        def _():
            out_ref[:, columns] = obuf[0, j * 128:(j + 1) * 128, :]
    for j in range(8):
        @pl.when(jnp.logical_or(t >= 4, t != j))
        def _():
            out_copy(0, 0, j).wait_recv()
    for j in range(4):
        out_copy(1, j, t).wait_send()
        @pl.when(t != j)
        def _():
            out_copy(0, j, t).wait_send()
    remote_q().wait_send()
    for which in range(2):
        for d in ORDER:
            for part, lane in sends(which, d):
                block_copy(which, at(*d), part, lane, s).wait_send()


def attention(lambdas, head_gain, queries, key_rows, value_rows):
    any_space = pl.BlockSpec(memory_space=pl.ANY)
    return pl.pallas_call(
        attention_kernel,
        out_shape=jax.ShapeDtypeStruct((128, 1024), jnp.bfloat16),
        in_specs=[
            pl.BlockSpec(memory_space=pltpu.SMEM),
            pl.BlockSpec(memory_space=pltpu.VMEM),
            any_space, any_space, any_space,
        ],
        out_specs=pl.BlockSpec(memory_space=pltpu.VMEM),
        scratch_shapes=[
            pltpu.VMEM((2, NZ * NX, BLK, 128), jnp.bfloat16),
            pltpu.VMEM((3, HALF, 128), jnp.bfloat16),
            pltpu.VMEM((2, 2, HALF, 128), jnp.bfloat16),
            pltpu.VMEM((2, 2, HALF, 128), jnp.float32),
            pltpu.VMEM((2, 2, HALF, 256), jnp.float32),
            pltpu.VMEM((2, HALF, 128), jnp.bfloat16),
            pltpu.SemaphoreType.DMA((4,)),
            pltpu.SemaphoreType.DMA,
            pltpu.SemaphoreType.DMA,
            pltpu.SemaphoreType.DMA((2, NZ * NX, 4)),
            pltpu.SemaphoreType.DMA((2, NZ * NX, 2)),
            pltpu.SemaphoreType.DMA((2, 4)),
            pltpu.SemaphoreType.DMA((8,)),
        ],
        compiler_params=pltpu.CompilerParams(
            collective_id=0, has_side_effects=True, vmem_limit_bytes=48 * 1024 * 1024
        ),
        name="attention",
    )(lambdas, head_gain.reshape(1, -1), queries, key_rows, value_rows)


GROUPS = (0, -1, 1, 2)
MAIN = 16
CH = 80
WID = 2048
HW = 1024
REM = 512
BAND = WID + REM
NT = 8


def expert_kernel(
    heads_ref, stream_ref, gain_ref, routes_ref, rw_ref, ow_hbm, gate_hbm, up_hbm, down_hbm,
    out_ref,
    ow, gw, uw, dw, att, nrm, outg, arr, reto, ret, xs, act, ps, pr, rh, rf, cm, cr,
    load_sem, psend, precv, xsend, xrecv, qsend, qrecv, rsend, rhrecv, rfrecv, bsend, brecv,
):
    s = lax.axis_index("sp")
    t = lax.axis_index("tp")
    z, x = s // NX, s % NX
    y, c = t // 2, t % 2
    mate = 2 * y + 1 - c
    bf16, f32 = jnp.bfloat16, jnp.float32

    def at(dz, dx):
        return ((z + dz + NZ) % NZ) * NX + (x + dx + NX) % NX

    def lane(dy, core):
        return 2 * ((y + dy + 4) % 4) + core

    loads = [
        pltpu.make_async_copy(ow_hbm, ow, load_sem.at[0]),
        pltpu.make_async_copy(gate_hbm.at[0], gw, load_sem.at[1]),
        pltpu.make_async_copy(up_hbm.at[0], uw, load_sem.at[2]),
        pltpu.make_async_copy(down_hbm.at[0], dw, load_sem.at[3]),
    ]
    for load in loads:
        load.start()

    barrier = pltpu.get_barrier_semaphore()
    others = [(dz, dx) for dz in GROUPS for dx in (0, 1, -1, 2) if (dz, dx) != (0, 0)]
    for dz, dx in others:
        pl.semaphore_signal(barrier, inc=1, device_id=(at(dz, dx), t), device_id_type=MESH)
    for peer in (lane(1, c), lane(-1, c), mate):
        pl.semaphore_signal(barrier, inc=1, device_id=(s, peer), device_id_type=MESH)

    loads[0].wait()
    heads = heads_ref[...]
    square = jnp.zeros((128, 1), f32)
    for k in range(0, WID, 512):
        cols = pl.ds(k, 512)
        value = stream_ref[:, cols].astype(f32) + jnp.dot(heads, ow[:, cols], preferred_element_type=f32)
        att[:, cols] = value
        square = square + jnp.sum(value * value, axis=1, keepdims=True)
    inverse = lax.rsqrt(square * (1.0 / WID) + 1e-06)
    for k in range(0, WID, 512):
        cols = pl.ds(k, 512)
        nrm[:, cols] = (att[:, cols] * inverse * gain_ref[:, cols]).astype(bf16)

    experts = lax.broadcasted_iota(jnp.int32, (128, 16), 1)
    route = [routes_ref[:, k:k + 1] for k in range(2)]
    hot = [(r == experts).astype(f32) for r in route]
    row_id = lax.broadcasted_iota(jnp.int32, (128, 128), 0)
    col_id = lax.broadcasted_iota(jnp.int32, (128, 128), 1)
    earlier = (col_id < row_id).astype(f32).astype(bf16)
    before = jnp.dot(earlier, (hot[0] + hot[1]).astype(bf16), preferred_element_type=f32)
    place = lax.broadcasted_iota(jnp.int32, (128, 256), 1).astype(f32)
    main_hit, rem_hit = [], []
    for k in range(2):
        slot = jnp.sum(before * hot[k], axis=1, keepdims=True)
        base = route[k].astype(f32) * 16.0 + slot
        low = slot < float(MAIN)
        main_hit.append((jnp.where(low, base, -1.0) == place).astype(f32))
        rem_hit.append([
            (jnp.where(low, -1.0, base + (4.0 * j - 16.0)) == place).astype(f32) for j in range(4)
        ])
    weight = [rw_ref[:, k:k + 1] for k in range(2)]
    over_rows = (((0,), (0,)), ((), ()))
    chosen = (main_hit[0] + main_hit[1]).astype(bf16)
    for k in range(0, WID, 512):
        cols = pl.ds(k, 512)
        outg[:, cols] = lax.dot_general(
            chosen, nrm[:, cols], over_rows, preferred_element_type=f32
        ).astype(bf16)
    extra = jnp.zeros((256, REM), f32)
    for j in range(4):
        extra = extra + lax.dot_general(
            (rem_hit[0][j] + rem_hit[1][j]).astype(bf16), nrm[:, pl.ds(j * REM, REM)], over_rows,
            preferred_element_type=f32,
        )
    outg[:, pl.ds(WID, REM)] = extra.astype(bf16)

    def keep_split(ref, value):
        high = value.astype(bf16)
        ref[:, pl.ds(0, 256)] = high
        ref[:, pl.ds(256, 256)] = (value - high.astype(f32)).astype(bf16)

    pl.semaphore_wait(barrier, len(others) + 3)

    def band(device):
        return pl.ds(pl.multiple_of(device * MAIN, MAIN), MAIN)

    def plane_copy(source, target, ssem, rsem, to, sender):
        return pltpu.make_async_remote_copy(
            src_ref=source.at[band(to), :], dst_ref=target.at[band(sender), :],
            send_sem=ssem.at[to], recv_sem=rsem.at[sender],
            device_id=(to, t), device_id_type=MESH,
        )

    for dz, dx in others:
        plane_copy(outg, arr, psend, precv, at(-dz, -dx), s).start()
    arr[band(s), :] = outg[band(s), :]
    keep_split(cm, weight[0] * main_hit[0] + weight[1] * main_hit[1])
    for j in range(4):
        keep_split(cr.at[j], weight[0] * rem_hit[0][j] + weight[1] * rem_hit[1][j])

    fold_row = lax.broadcasted_iota(jnp.int32, (16, 64), 0)
    fold_col = lax.broadcasted_iota(jnp.int32, (16, 64), 1)
    fold = [
        (fold_col == 16 * (fold_row >> 2) + 4 * j + (fold_row & 3)).astype(f32).astype(bf16)
        for j in range(4)
    ]

    def rows_of(position):
        return pl.ds(pl.multiple_of(position * CH, 16), CH)

    def x_copy(g, position, part, send, to, slot=None):
        cols = pl.ds(0, WID) if part == 2 else pl.ds(part * HW, HW)
        return pltpu.make_async_remote_copy(
            src_ref=xs.at[g, rows_of(position), cols], dst_ref=xs.at[g, rows_of(position), cols],
            send_sem=xsend.at[g, send], recv_sem=xrecv.at[g, position, part % 2],
            device_id=(s, to), device_id_type=MESH,
        )

    def x_sends(g):
        return [
            (g, t, 2, 0, lane(1, c)), (g, t, 2, 1, lane(-1, c)), (g, t, 2, 2, mate),
            (g, lane(-1, c), 0, 3, lane(1, c)), (g, lane(-1, c), 2, 4, mate),
            (g, lane(1, c), 1, 5, lane(-1, c)), (g, lane(1, c), 2, 6, mate),
            (g, lane(2, c), 2, 7, mate),
        ]

    def group_rows(g):
        zz = (z + GROUPS[g] + NZ) % NZ
        return pl.ds(pl.multiple_of(zz * 64, 64), 64)

    def build(g):
        for dx in (0, 1, -1, 2):
            if (GROUPS[g], dx) != (0, 0):
                plane_copy(outg, arr, psend, precv, s, at(GROUPS[g], dx)).wait_recv()
        rows = group_rows(g)
        first = pl.multiple_of(t * CH, 16)
        for k in range(0, WID, 512):
            xs[g, pl.ds(first, 64), pl.ds(k, 512)] = arr[rows, pl.ds(k, 512)]
        for j in range(4):
            xs[g, pl.ds(first + 64, 16), pl.ds(j * REM, REM)] = jnp.dot(
                fold[j], arr[rows, pl.ds(WID, REM)], preferred_element_type=f32
            ).astype(bf16)
        for copy in x_sends(g)[:3]:
            x_copy(*copy).start()

    def forward(g):
        todo = x_sends(g)
        x_copy(g, lane(-1, c), 2, 0, t).wait_recv()
        x_copy(*todo[3]).start()
        x_copy(*todo[4]).start()
        x_copy(g, lane(1, c), 2, 0, t).wait_recv()
        x_copy(*todo[5]).start()
        x_copy(*todo[6]).start()

    def far(g):
        x_copy(g, lane(2, c), 0, 0, t).wait_recv()
        x_copy(g, lane(2, c), 1, 0, t).wait_recv()
        x_copy(*x_sends(g)[7]).start()

    def pair_copy(g, yy):
        return pltpu.make_async_remote_copy(
            src_ref=ps.at[g, rows_of(2 * yy + 1 - c), :], dst_ref=pr.at[g, yy],
            send_sem=qsend.at[g, yy], recv_sem=qrecv.at[g, yy],
            device_id=(s, mate), device_id_type=MESH,
        )

    TURN = (2, 1, 3, 0)

    def compute(g):
        for dy in (0, -1, 1, 2):
            x_copy(g, lane(dy, 1 - c), 2, 0, t).wait_recv()
        if g == 0:
            for load in loads[1:]:
                load.wait()

        def block(i, carry):
            dy = jnp.where(i == 0, 2, jnp.where(i == 1, 1, jnp.where(i == 2, 3, 0)))
            yy = (y + dy) % 4
            rows = pl.ds(pl.multiple_of(yy * 2 * CH, 32), 2 * CH)
            value = xs[g, rows, :]
            gate = jnp.dot(value, gw[...], preferred_element_type=f32)
            upper = jnp.dot(value, uw[...], preferred_element_type=f32)
            act[...] = (gate / (1.0 + jnp.exp(-gate)) * upper).astype(bf16)
            ps[g, rows, :] = jnp.dot(act[...], dw[...], preferred_element_type=f32).astype(bf16)
            pair_copy(g, yy).start()
            return carry

        lax.fori_loop(0, 4, block, 0)

    def add_into(g, position, cols, terms):
        rows = rows_of(position)
        total = ps[g, rows, cols].astype(f32)
        for term in terms:
            total = total + term.astype(f32)
        ps[g, rows, cols] = total.astype(bf16)

    def r_copy(g, dy, part, send, direction, ref, sem, slot):
        cols = pl.ds(part * HW, HW)
        return pltpu.make_async_remote_copy(
            src_ref=ps.at[g, rows_of(lane(dy, c)), cols], dst_ref=ref.at[(g,) + slot],
            send_sem=rsend.at[g, send], recv_sem=sem.at[(g,) + slot],
            device_id=(s, lane(direction, c)), device_id_type=MESH,
        )

    def r_sends(g):
        return [
            (g, 2, 0, 0, 1, rh, rhrecv, (0,)), (g, 2, 1, 1, -1, rh, rhrecv, (1,)),
            (g, 1, 1, 2, 1, rf, rfrecv, (0, 1)), (g, -1, 0, 3, -1, rf, rfrecv, (1, 0)),
            (g, 1, 0, 4, 1, rf, rfrecv, (0, 0)), (g, -1, 1, 5, -1, rf, rfrecv, (1, 1)),
        ]

    def pair(g):
        todo = r_sends(g)
        for turn, dy in enumerate(TURN):
            yy = (y + dy) % 4
            pair_copy(g, yy).wait_recv()
            for k in range(2):
                cols = pl.ds(k * HW, HW)
                add_into(g, 2 * yy + c, cols, [pr[g, yy, :, cols]])
            if turn == 0:
                r_copy(*todo[0]).start()
                r_copy(*todo[1]).start()
            if turn == 1:
                r_copy(*todo[2]).start()
            if turn == 2:
                r_copy(*todo[3]).start()

    def middle(g):
        todo = r_sends(g)
        r_copy(*todo[0]).wait_recv()
        add_into(g, lane(1, c), pl.ds(0, HW), [rh[g, 0]])
        r_copy(*todo[4]).start()
        r_copy(*todo[1]).wait_recv()
        add_into(g, lane(-1, c), pl.ds(HW, HW), [rh[g, 1]])
        r_copy(*todo[5]).start()

    def finish(g):
        todo = r_sends(g)
        for k in range(2, 6):
            r_copy(*todo[k]).wait_recv()
        rows = group_rows(g)
        own = pl.multiple_of(t * CH, 16)
        extra = jnp.zeros((64, REM), f32)
        for j in range(4):
            cols = pl.ds(j * REM, REM)
            inner = pl.ds((j % 2) * REM, REM)
            total = (
                ps[g, pl.ds(own, CH), cols].astype(f32)
                + rf[g, 0, j // 2, :, inner].astype(f32)
                + rf[g, 1, j // 2, :, inner].astype(f32)
            ).astype(bf16)
            reto[rows, cols] = total[:64]
            extra = extra + lax.dot_general(fold[j], total[64:], over_rows, preferred_element_type=f32)
        reto[rows, pl.ds(WID, REM)] = extra.astype(bf16)
        for dx in (0, 1, -1, 2):
            to = at(GROUPS[g], dx)
            if (GROUPS[g], dx) == (0, 0):
                ret[band(s), :] = reto[band(s), :]
            else:
                plane_copy(reto, ret, bsend, brecv, to, s).start()

    for stage, g in (
        (build, 0), (build, 1), (forward, 0), (build, 2), (forward, 1), (build, 3), (far, 0),
        (compute, 0), (pair, 0), (forward, 2), (far, 1), (compute, 1), (pair, 1), (middle, 0),
        (forward, 3), (far, 2), (compute, 2), (pair, 2), (finish, 0), (middle, 1), (far, 3),
        (compute, 3), (pair, 3), (middle, 2), (finish, 1), (middle, 3), (finish, 2), (finish, 3),
    ):
        stage(g)

    for dz, dx in others:
        plane_copy(reto, ret, bsend, brecv, s, at(dz, dx)).wait_recv()
    for j in range(4):
        cols = pl.ds(j * REM, REM)
        back = ret[:, cols]
        tail = ret[:, pl.ds(WID, REM)]
        routed = jnp.dot(cm[...], jnp.concatenate([back, back], axis=0), preferred_element_type=f32)
        routed = routed + jnp.dot(
            cr[j], jnp.concatenate([tail, tail], axis=0), preferred_element_type=f32
        )
        out_ref[:, cols] = (att[:, cols] + routed).astype(bf16)

    for dz, dx in others:
        plane_copy(outg, arr, psend, precv, at(dz, dx), s).wait_send()
        plane_copy(reto, ret, bsend, brecv, at(dz, dx), s).wait_send()
    for g in range(4):
        for copy in x_sends(g):
            x_copy(*copy).wait_send()
        for yy in range(4):
            pair_copy(g, yy).wait_send()
        for copy in r_sends(g):
            r_copy(*copy).wait_send()


def routed_experts(
    heads, stream, ffn_gain, routes, route_weight, out_weight, gate_weight, up_weight, down_weight
):
    any_space = pl.BlockSpec(memory_space=pl.ANY)
    vmem = pl.BlockSpec(memory_space=pltpu.VMEM)
    bf16, f32 = jnp.bfloat16, jnp.float32
    dma = pltpu.SemaphoreType.DMA
    return pl.pallas_call(
        expert_kernel,
        out_shape=jax.ShapeDtypeStruct((128, WID), bf16),
        in_specs=[vmem] * 5 + [any_space] * 4,
        out_specs=vmem,
        scratch_shapes=[
            pltpu.VMEM((1024, WID), bf16),
            pltpu.VMEM((WID, 640), bf16),
            pltpu.VMEM((WID, 640), bf16),
            pltpu.VMEM((640, WID), bf16),
            pltpu.VMEM((128, WID), f32),
            pltpu.VMEM((128, WID), bf16),
            pltpu.VMEM((256, BAND), bf16),
            pltpu.VMEM((256, BAND), bf16),
            pltpu.VMEM((256, BAND), bf16),
            pltpu.VMEM((256, BAND), bf16),
            pltpu.VMEM((4, NT * CH, WID), bf16),
            pltpu.VMEM((2 * CH, 640), bf16),
            pltpu.VMEM((4, NT * CH, WID), bf16),
            pltpu.VMEM((4, 4, CH, WID), bf16),
            pltpu.VMEM((4, 2, CH, HW), bf16),
            pltpu.VMEM((4, 2, 2, CH, HW), bf16),
            pltpu.VMEM((128, 512), bf16),
            pltpu.VMEM((4, 128, 512), bf16),
            dma((4,)),
            dma((16,)), dma((16,)),
            dma((4, 8)), dma((4, 8, 2)),
            dma((4, 4)), dma((4, 4)),
            dma((4, 6)), dma((4, 2)), dma((4, 2, 2)),
            dma((16,)), dma((16,)),
        ],
        compiler_params=pltpu.CompilerParams(
            collective_id=1, has_side_effects=True, vmem_limit_bytes=63 * 1024 * 1024
        ),
        name="experts",
    )(
        heads, stream, ffn_gain.reshape(1, -1), routes, route_weight,
        out_weight, gate_weight, up_weight, down_weight,
    )


def local(
    queries,
    key_rows,
    value_rows,
    lambdas,
    head_gain,
    out_weight,
    stream,
    ffn_gain,
    routes,
    route_weight,
    gate_weight,
    up_weight,
    down_weight,
):
    heads_local = attention(lambdas, head_gain, queries, key_rows, value_rows)
    return routed_experts(
        heads_local, stream, ffn_gain, routes, route_weight,
        out_weight, gate_weight, up_weight, down_weight,
    )


def solution(mesh):
    placed = (
        P("sp", "tp"),
        P("sp", "tp"),
        P("sp", "tp"),
        P("tp"),
        P(),
        P(),
        P(("sp", "tp"), None),
        P(),
        P(("sp", "tp"), None),
        P(("sp", "tp"), None),
        P("sp", None, "tp"),
        P("sp", None, "tp"),
        P("sp", "tp", None),
    )
    return jax.shard_map(
        local, mesh=mesh, in_specs=placed, out_specs=P(("sp", "tp"), None), check_vma=False
    )
```

```python
import functools

import jax
import jax.numpy as jnp
from jax import lax
from jax.experimental import pallas as pl
from jax.experimental.pallas import tpu as pltpu
from jax.sharding import PartitionSpec as P

DH = 64


LOG2E = 1.4426950408889634
MESH = pl.DeviceIdType.MESH
NZ = 4
NX = 4
BLK = 1024
HALF = 512
NEG = -1e30
VROWS = 144
TQ = 512
KB = 256
WORK = (
    (0, 0), (3, 0), (1, 0), (3, 3), (1, 3), (3, 1), (1, 1),
    (2, 0), (2, 3), (2, 1), (2, 2), (3, 2), (1, 2), (0, 3), (0, 1), (0, 2),
)


def attention_kernel(
    lam_ref, gain_ref, q_hbm, k_hbm, v_hbm, out_ref,
    vin, lamv, qfull, qother, kb, vb, qm, mx, acc, pout, pin, sout, sin, obuf, sbuf0, sbuf1, fbuf0, fbuf1, nbuf0, nbuf1,
    load_sem, lsend, lrecv, send_sem, recv_sem, msend, mrecv, psend, precv, ssend, srecv, osend, orecv,
):
    sp = lax.axis_index("sp")
    t = lax.axis_index("tp")
    z, x = sp // NX, sp % NX
    y, c = t // 2, t % 2
    mate = 2 * y + 1 - c
    f32, bf16 = jnp.float32, jnp.bfloat16
    sbuf, fbuf, nbuf = (sbuf0, sbuf1), (fbuf0, fbuf1), (nbuf0, nbuf1)

    def at(dz, dx):
        return ((z + dz + NZ) % NZ) * NX + (x + dx + NX) % NX

    loads = [
        pltpu.make_async_copy(q_hbm, qfull.at[0], load_sem.at[0]),
        pltpu.make_async_copy(k_hbm, kb.at[0, 0], load_sem.at[1]),
        pltpu.make_async_copy(v_hbm, vin, load_sem.at[2]),
    ]
    for load in loads:
        load.start()

    lamv[0] = jnp.full((8, HALF), lam_ref[0], f32)

    barrier = pltpu.get_barrier_semaphore()
    for dz, dx in ((0, 1), (0, -1), (1, 0), (-1, 0), (2, 0), (0, 2)):
        pl.semaphore_signal(barrier, inc=1, device_id=(at(dz, dx), t), device_id_type=MESH)
    for j in range(1, 8):
        pl.semaphore_signal(barrier, inc=1, device_id=(sp, (t + j) % 8), device_id_type=MESH)

    def along(e, queries, d):
        own = c if e == 0 else 1 - c
        first = at(d, 0) if queries else at(0, d)
        second = at(0, d) if queries else at(d, 0)
        return jnp.where(own == 0, first, second)

    def piece(kind, slot, part):
        span = pl.ds(0, BLK) if part == 2 else pl.ds(part * HALF, HALF)
        if kind == 0:
            return qfull.at[slot, span, :]
        if kind == 1:
            return kb.at[0, slot, span, :]
        return vb.at[0, slot, :, span]

    def ring_copy(kind, slot, part, lane):
        d = 1 if lane == 0 else -1
        return pltpu.make_async_remote_copy(
            src_ref=piece(kind, slot, part), dst_ref=piece(kind, (slot - d) % 4, part),
            send_sem=send_sem.at[kind, slot, lane],
            recv_sem=recv_sem.at[kind, (slot - d) % 4, part % 2],
            device_id=(along(0, kind == 0, d), t), device_id_type=MESH,
        )

    RING = ((0, 2, 0), (0, 2, 1), (3, 0, 0), (1, 1, 1))

    def ring_wait(kind, slot):
        for part in (0, 1) if slot == 2 else (2,):
            pltpu.make_async_remote_copy(
                src_ref=piece(kind, slot, part), dst_ref=piece(kind, slot, part),
                send_sem=send_sem.at[kind, 0, 0], recv_sem=recv_sem.at[kind, slot, part % 2],
                device_id=(sp, mate), device_id_type=MESH,
            ).wait_recv()

    def mate_copy(kind, slot):
        if kind == 0:
            source = qfull.at[slot, pl.ds(pl.multiple_of((1 - c) * HALF, HALF), HALF), :]
            target = qother.at[slot]
        elif kind == 1:
            source, target = kb.at[0, slot], kb.at[1, slot]
        else:
            source, target = vb.at[0, slot], vb.at[1, slot]
        return pltpu.make_async_remote_copy(
            src_ref=source, dst_ref=target,
            send_sem=msend.at[kind, slot], recv_sem=mrecv.at[kind, slot],
            device_id=(sp, mate), device_id_type=MESH,
        )

    def lambda_copy():
        return pltpu.make_async_remote_copy(
            src_ref=lamv.at[0], dst_ref=lamv.at[1], send_sem=lsend, recv_sem=lrecv,
            device_id=(sp, mate), device_id_type=MESH,
        )

    lane_ids = lax.broadcasted_iota(jnp.int32, (HALF, 2 * DH), 1)

    def split_maps(e, slot):
        if e == 0:
            q = qfull[slot, pl.ds(pl.multiple_of(c * HALF, HALF), HALF), :]
        else:
            q = qother[slot]
        zero = jnp.zeros_like(q)
        qm[e, slot, 0] = jnp.where(lane_ids < DH, q, zero)
        qm[e, slot, 1] = jnp.where(lane_ids < DH, zero, q)

    def arrive(kind, slot):
        ring_wait(kind, slot)
        if slot == 3:
            ring_copy(kind, 3, 0, 0).start()
        if slot == 1:
            ring_copy(kind, 1, 1, 1).start()
        mate_copy(kind, slot).start()

    def settle(kind, slot):
        mate_copy(kind, slot).wait_recv()
        if kind == 0:
            split_maps(0, slot)
            split_maps(1, slot)

    for load in loads:
        load.wait()
    pl.semaphore_wait(barrier, 13)
    for kind in (0, 1):
        for lane in range(2):
            ring_copy(kind, 0, 2, lane).start()
    mate_copy(1, 0).start()
    mate_copy(0, 0).start()
    lambda_copy().start()
    for k in range(4):
        span = pl.ds(k * 256, 256)
        vb[0, 0, :, span] = vin[span, :].astype(f32).T.astype(bf16)
    for lane in range(2):
        ring_copy(2, 0, 2, lane).start()
    mate_copy(2, 0).start()

    mx[...] = jnp.full(mx.shape, NEG, f32)
    acc[...] = jnp.zeros(acc.shape, f32)

    scale = LOG2E * DH ** (-0.5)

    always = sp >= 0

    def tiles(e, di, dk, masked):
        chunks = [(m, r) for m in range(2) for r in range(HALF // TQ)]

        def phase(now, later):
            tops, pv = [], None
            for kk in range(BLK // KB):
                keys = pl.ds(kk * KB, KB)
                if later is not None:
                    m, r = chunks[later]
                    scores = lax.dot_general(
                        kb[e, dk, keys, :], qm[e, di, m, pl.ds(r * TQ, TQ), :],
                        (((1,), (1,)), ((), ())), preferred_element_type=f32,
                    ) * scale
                    if masked:
                        key_id = lax.broadcasted_iota(jnp.int32, scores.shape, 0) + kk * KB
                        query_id = lax.broadcasted_iota(jnp.int32, scores.shape, 1) + (c * HALF + r * TQ)
                        scores = jnp.where(key_id <= query_id, scores, NEG)
                    sbuf[later % 2][keys, :] = scores
                    tops.append(jnp.max(scores, axis=0, keepdims=True))
                if now is not None:
                    m, r = chunks[now]
                    values = jnp.concatenate(
                        [vb[e, dk, :, keys], jnp.ones((VROWS - 128, KB), bf16)], axis=0
                    )
                    weights = jnp.exp2(sbuf[now % 2][keys, :] - nbuf[now % 2][...]).astype(bf16)
                    term = jnp.dot(values, weights, preferred_element_type=f32)
                    pv = term if pv is None else pv + term
            if now is not None:
                m, r = chunks[now]
                cols = pl.ds(r * TQ, TQ)
                acc[e, di, m, :, cols] = acc[e, di, m, :, cols] * fbuf[now % 2][...] + pv
            if later is not None:
                m, r = chunks[later]
                cols = pl.ds(r * TQ, TQ)
                old = mx[e, di, m, :, cols]
                new = functools.reduce(jnp.maximum, tops, old)
                fbuf[later % 2][...] = jnp.exp2(old - new)
                nbuf[later % 2][...] = new
                mx[e, di, m, :, cols] = new

        phase(None, 0)
        for n in range(len(chunks)):
            @pl.when(always)
            def _(n=n):
                phase(n, n + 1 if n + 1 < len(chunks) else None)

    def partial_copies(e, d):
        to = along(e, True, d)
        slot = (4 - d) % 4
        return [
            pltpu.make_async_remote_copy(
                src_ref=pout.at[e, d], dst_ref=pin.at[e, slot],
                send_sem=psend.at[e, d], recv_sem=precv.at[e, slot],
                device_id=(to, t), device_id_type=MESH,
            ),
            pltpu.make_async_remote_copy(
                src_ref=sout.at[e, d], dst_ref=sin.at[e, slot],
                send_sem=ssend.at[e, d], recv_sem=srecv.at[e, slot],
                device_id=(to, t), device_id_type=MESH,
            ),
        ]

    def normal(e, d, m):
        total = acc[e, d, m, pl.ds(128, 1), :]
        some = total > 0.0
        safe = jnp.where(some, total, 1.0)
        level = jnp.where(some, mx[e, d, m] + jnp.log2(safe), NEG)
        return acc[e, d, m, pl.ds(0, 128), :] / safe, level

    def send_partial(d):
        for e in range(2):
            for m in range(2):
                value, level = normal(e, d, m)
                pout[e, d, m] = value.astype(bf16)
                sout[e, d, m] = jnp.broadcast_to(level, (8, HALF))
            for copy in partial_copies(e, d):
                copy.start()

    def before(n):
        if n == 0:
            for kind in (1, 0, 2):
                settle(kind, 0)
        if n == 1:
            for kind in range(3):
                for slot in (3, 1):
                    arrive(kind, slot)
            for kind in range(3):
                for slot in (3, 1):
                    settle(kind, slot)
        if n == 4:
            for kind in range(3):
                arrive(kind, 2)
            for kind in range(3):
                settle(kind, 2)
        if n == 11:
            send_partial(2)
        if n == 12:
            send_partial(3)
        if n == 13:
            send_partial(1)

    def step(n, carry):
        for k in (0, 1, 4, 11, 12, 13):
            @pl.when(n == k)
            def _(k=k):
                before(k)

        di = jnp.int32(0)
        dk = jnp.int32(0)
        for k, (a, b) in enumerate(WORK):
            di = jnp.where(n == k, a, di)
            dk = jnp.where(n == k, b, dk)

        def one_head(e, inner):
            head = jnp.where(e == 0, c, 1 - c)
            query_block = jnp.where(head == 0, at(di, 0), at(0, di))
            key_block = jnp.where(head == 0, at(0, dk), at(dk, 0))

            @pl.when(key_block < query_block)
            def _():
                tiles(e, di, dk, False)

            @pl.when(key_block == query_block)
            def _():
                tiles(e, di, dk, True)

            return inner

        return lax.fori_loop(0, 2, one_head, carry)

    lax.fori_loop(0, len(WORK), step, 0)

    def out_copy(e, j, sender):
        cols = pl.ds(pl.multiple_of(sender * 128, 128), 128)
        return pltpu.make_async_remote_copy(
            src_ref=obuf.at[e, pl.ds(j * 128, 128), :], dst_ref=out_ref.at[:, cols],
            send_sem=osend.at[e, j], recv_sem=orecv.at[sender],
            device_id=(sp, 4 * c + j), device_id_type=MESH,
        )

    lambda_copy().wait_recv()
    for e in range(2):
        head = t if e == 0 else mate
        for slot in (2, 1, 3):
            pltpu.make_async_remote_copy(
                src_ref=pout.at[e, slot], dst_ref=pin.at[e, slot],
                send_sem=psend.at[e, slot], recv_sem=precv.at[e, slot],
                device_id=(sp, mate), device_id_type=MESH,
            ).wait_recv()
            pltpu.make_async_remote_copy(
                src_ref=sout.at[e, slot], dst_ref=sin.at[e, slot],
                send_sem=ssend.at[e, slot], recv_sem=srecv.at[e, slot],
                device_id=(sp, mate), device_id_type=MESH,
            ).wait_recv()
        mixed = []
        for m in range(2):
            value, level = normal(e, 0, m)
            levels = [level] + [sin[e, slot, m, pl.ds(0, 1), :] for slot in (1, 2, 3)]
            top = jnp.maximum(jnp.maximum(levels[0], levels[1]), jnp.maximum(levels[2], levels[3]))
            share = [jnp.exp2(item - top) for item in levels]
            inverse = 1.0 / (share[0] + share[1] + share[2] + share[3])
            total = value * (share[0] * inverse)
            for slot in (1, 2, 3):
                total = total + pin[e, slot, m].astype(f32) * (share[slot] * inverse)
            mixed.append(total)
        contrast = mixed[0] - lamv[e, pl.ds(0, 1), :] * mixed[1]
        mean = jnp.mean(contrast * contrast, axis=0, keepdims=True)
        contrast = contrast * lax.rsqrt(mean + 1e-05)
        for j in range(4):
            rows = contrast[:, j * 128:(j + 1) * 128].T * gain_ref[...]
            obuf[e, pl.ds(j * 128, 128), :] = rows.astype(bf16)
        for j in range(4):
            @pl.when(t != 4 * c + j)
            def _(e=e, j=j, head=head):
                out_copy(e, j, head).start()
            @pl.when(t == 4 * c + j)
            def _(e=e, j=j, head=head):
                cols = pl.ds(pl.multiple_of(head * 128, 128), 128)
                out_ref[:, cols] = obuf[e, pl.ds(j * 128, 128), :]

    origin = t // 4
    for yy in range(4):
        for core in range(2):
            @pl.when(2 * yy + origin != t)
            def _(yy=yy, core=core):
                out_copy(0, 0, 2 * yy + core).wait_recv()
    for e in range(2):
        for j in range(4):
            @pl.when(t != 4 * c + j)
            def _(e=e, j=j):
                out_copy(e, j, t).wait_send()
    lambda_copy().wait_send()
    for kind in range(3):
        for slot, part, lane in RING:
            ring_copy(kind, slot, part, lane).wait_send()
        for slot in range(4):
            mate_copy(kind, slot).wait_send()
    for e in range(2):
        for d in (1, 2, 3):
            for copy in partial_copies(e, d):
                copy.wait_send()


def attention(lambdas, head_gain, queries, key_rows, value_rows):
    any_space = pl.BlockSpec(memory_space=pl.ANY)
    bf16, f32 = jnp.bfloat16, jnp.float32
    dma = pltpu.SemaphoreType.DMA
    return pl.pallas_call(
        attention_kernel,
        out_shape=jax.ShapeDtypeStruct((128, 1024), jnp.bfloat16),
        in_specs=[
            pl.BlockSpec(memory_space=pltpu.SMEM),
            pl.BlockSpec(memory_space=pltpu.VMEM),
            any_space, any_space, any_space,
        ],
        out_specs=pl.BlockSpec(memory_space=pltpu.VMEM),
        scratch_shapes=[
            pltpu.VMEM((BLK, 128), bf16),
            pltpu.VMEM((2, 8, HALF), f32),
            pltpu.VMEM((4, BLK, 128), bf16),
            pltpu.VMEM((4, HALF, 128), bf16),
            pltpu.VMEM((2, 4, BLK, 128), bf16),
            pltpu.VMEM((2, 4, 128, BLK), bf16),
            pltpu.VMEM((2, 4, 2, HALF, 128), bf16),
            pltpu.VMEM((2, 4, 2, 1, HALF), f32),
            pltpu.VMEM((2, 4, 2, VROWS, HALF), f32),
            pltpu.VMEM((2, 4, 2, 128, HALF), bf16),
            pltpu.VMEM((2, 4, 2, 128, HALF), bf16),
            pltpu.VMEM((2, 4, 2, 8, HALF), f32),
            pltpu.VMEM((2, 4, 2, 8, HALF), f32),
            pltpu.VMEM((2, HALF, 128), bf16),
            pltpu.VMEM((BLK, TQ), f32), pltpu.VMEM((BLK, TQ), f32),
            pltpu.VMEM((1, TQ), f32), pltpu.VMEM((1, TQ), f32),
            pltpu.VMEM((1, TQ), f32), pltpu.VMEM((1, TQ), f32),
            dma((3,)),
            dma, dma,
            dma((3, 4, 2)), dma((3, 4, 2)),
            dma((3, 4)), dma((3, 4)),
            dma((2, 4)), dma((2, 4)),
            dma((2, 4)), dma((2, 4)),
            dma((2, 4)), dma((8,)),
        ],
        compiler_params=pltpu.CompilerParams(
            collective_id=0, has_side_effects=True, vmem_limit_bytes=48 * 1024 * 1024
        ),
        name="attention",
    )(lambdas, head_gain.reshape(1, -1), queries, key_rows, value_rows)


GROUPS = (0, -1, 1, 2)
MAIN = 16
CH = 80
WID = 2048
HW = 1024
REM = 512
BAND = WID + REM
NT = 8


def expert_kernel(
    heads_ref, stream_ref, gain_ref, routes_ref, rw_ref, ow_hbm, gate_hbm, up_hbm, down_hbm,
    out_ref,
    ow, gw, uw, dw, att, nrm, outg, arr, reto, ret, xs, act, ps, pr, rh, rf, cm, cr,
    load_sem, psend, precv, xsend, xrecv, qsend, qrecv, rsend, rhrecv, rfrecv, bsend, brecv,
):
    s = lax.axis_index("sp")
    t = lax.axis_index("tp")
    z, x = s // NX, s % NX
    y, c = t // 2, t % 2
    mate = 2 * y + 1 - c
    bf16, f32 = jnp.bfloat16, jnp.float32

    def at(dz, dx):
        return ((z + dz + NZ) % NZ) * NX + (x + dx + NX) % NX

    def lane(dy, core):
        return 2 * ((y + dy + 4) % 4) + core

    loads = [
        pltpu.make_async_copy(ow_hbm, ow, load_sem.at[0]),
        pltpu.make_async_copy(gate_hbm.at[0], gw, load_sem.at[1]),
        pltpu.make_async_copy(up_hbm.at[0], uw, load_sem.at[2]),
        pltpu.make_async_copy(down_hbm.at[0], dw, load_sem.at[3]),
    ]
    for load in loads:
        load.start()

    barrier = pltpu.get_barrier_semaphore()
    others = [(dz, dx) for dz in GROUPS for dx in (0, 1, -1, 2) if (dz, dx) != (0, 0)]
    for dz, dx in others:
        pl.semaphore_signal(barrier, inc=1, device_id=(at(dz, dx), t), device_id_type=MESH)
    for peer in (lane(1, c), lane(-1, c), mate):
        pl.semaphore_signal(barrier, inc=1, device_id=(s, peer), device_id_type=MESH)

    loads[0].wait()
    heads = heads_ref[...]
    square = jnp.zeros((128, 1), f32)
    for k in range(0, WID, 512):
        cols = pl.ds(k, 512)
        value = stream_ref[:, cols].astype(f32) + jnp.dot(heads, ow[:, cols], preferred_element_type=f32)
        att[:, cols] = value
        square = square + jnp.sum(value * value, axis=1, keepdims=True)
    inverse = lax.rsqrt(square * (1.0 / WID) + 1e-06)
    for k in range(0, WID, 512):
        cols = pl.ds(k, 512)
        nrm[:, cols] = (att[:, cols] * inverse * gain_ref[:, cols]).astype(bf16)

    experts = lax.broadcasted_iota(jnp.int32, (128, 16), 1)
    route = [routes_ref[:, k:k + 1] for k in range(2)]
    hot = [(r == experts).astype(f32) for r in route]
    row_id = lax.broadcasted_iota(jnp.int32, (128, 128), 0)
    col_id = lax.broadcasted_iota(jnp.int32, (128, 128), 1)
    earlier = (col_id < row_id).astype(f32).astype(bf16)
    before = jnp.dot(earlier, (hot[0] + hot[1]).astype(bf16), preferred_element_type=f32)
    place = lax.broadcasted_iota(jnp.int32, (128, 256), 1).astype(f32)
    main_hit, rem_hit = [], []
    for k in range(2):
        slot = jnp.sum(before * hot[k], axis=1, keepdims=True)
        base = route[k].astype(f32) * 16.0 + slot
        low = slot < float(MAIN)
        main_hit.append((jnp.where(low, base, -1.0) == place).astype(f32))
        rem_hit.append([
            (jnp.where(low, -1.0, base + (4.0 * j - 16.0)) == place).astype(f32) for j in range(4)
        ])
    weight = [rw_ref[:, k:k + 1] for k in range(2)]
    over_rows = (((0,), (0,)), ((), ()))
    chosen = (main_hit[0] + main_hit[1]).astype(bf16)
    for k in range(0, WID, 512):
        cols = pl.ds(k, 512)
        outg[:, cols] = lax.dot_general(
            chosen, nrm[:, cols], over_rows, preferred_element_type=f32
        ).astype(bf16)
    extra = jnp.zeros((256, REM), f32)
    for j in range(4):
        extra = extra + lax.dot_general(
            (rem_hit[0][j] + rem_hit[1][j]).astype(bf16), nrm[:, pl.ds(j * REM, REM)], over_rows,
            preferred_element_type=f32,
        )
    outg[:, pl.ds(WID, REM)] = extra.astype(bf16)

    def keep_split(ref, value):
        high = value.astype(bf16)
        ref[:, pl.ds(0, 256)] = high
        ref[:, pl.ds(256, 256)] = (value - high.astype(f32)).astype(bf16)

    pl.semaphore_wait(barrier, len(others) + 3)

    def band(device):
        return pl.ds(pl.multiple_of(device * MAIN, MAIN), MAIN)

    def plane_copy(source, target, ssem, rsem, to, sender):
        return pltpu.make_async_remote_copy(
            src_ref=source.at[band(to), :], dst_ref=target.at[band(sender), :],
            send_sem=ssem.at[to], recv_sem=rsem.at[sender],
            device_id=(to, t), device_id_type=MESH,
        )

    for dz, dx in others:
        plane_copy(outg, arr, psend, precv, at(-dz, -dx), s).start()
    arr[band(s), :] = outg[band(s), :]
    keep_split(cm, weight[0] * main_hit[0] + weight[1] * main_hit[1])
    for j in range(4):
        keep_split(cr.at[j], weight[0] * rem_hit[0][j] + weight[1] * rem_hit[1][j])

    fold_row = lax.broadcasted_iota(jnp.int32, (16, 64), 0)
    fold_col = lax.broadcasted_iota(jnp.int32, (16, 64), 1)
    fold = [
        (fold_col == 16 * (fold_row >> 2) + 4 * j + (fold_row & 3)).astype(f32).astype(bf16)
        for j in range(4)
    ]

    def rows_of(position):
        return pl.ds(pl.multiple_of(position * CH, 16), CH)

    def x_copy(g, position, part, send, to, slot=None):
        cols = pl.ds(0, WID) if part == 2 else pl.ds(part * HW, HW)
        return pltpu.make_async_remote_copy(
            src_ref=xs.at[g, rows_of(position), cols], dst_ref=xs.at[g, rows_of(position), cols],
            send_sem=xsend.at[g, send], recv_sem=xrecv.at[g, position, part % 2],
            device_id=(s, to), device_id_type=MESH,
        )

    def x_sends(g):
        return [
            (g, t, 2, 0, lane(1, c)), (g, t, 2, 1, lane(-1, c)), (g, t, 2, 2, mate),
            (g, lane(-1, c), 0, 3, lane(1, c)), (g, lane(-1, c), 2, 4, mate),
            (g, lane(1, c), 1, 5, lane(-1, c)), (g, lane(1, c), 2, 6, mate),
            (g, lane(2, c), 2, 7, mate),
        ]

    def group_rows(g):
        zz = (z + GROUPS[g] + NZ) % NZ
        return pl.ds(pl.multiple_of(zz * 64, 64), 64)

    def build(g):
        for dx in (0, 1, -1, 2):
            if (GROUPS[g], dx) != (0, 0):
                plane_copy(outg, arr, psend, precv, s, at(GROUPS[g], dx)).wait_recv()
        rows = group_rows(g)
        first = pl.multiple_of(t * CH, 16)
        for k in range(0, WID, 512):
            xs[g, pl.ds(first, 64), pl.ds(k, 512)] = arr[rows, pl.ds(k, 512)]
        for j in range(4):
            xs[g, pl.ds(first + 64, 16), pl.ds(j * REM, REM)] = jnp.dot(
                fold[j], arr[rows, pl.ds(WID, REM)], preferred_element_type=f32
            ).astype(bf16)
        for copy in x_sends(g)[:3]:
            x_copy(*copy).start()

    def forward(g):
        todo = x_sends(g)
        x_copy(g, lane(-1, c), 2, 0, t).wait_recv()
        x_copy(*todo[3]).start()
        x_copy(*todo[4]).start()
        x_copy(g, lane(1, c), 2, 0, t).wait_recv()
        x_copy(*todo[5]).start()
        x_copy(*todo[6]).start()

    def far(g):
        x_copy(g, lane(2, c), 0, 0, t).wait_recv()
        x_copy(g, lane(2, c), 1, 0, t).wait_recv()
        x_copy(*x_sends(g)[7]).start()

    def pair_copy(g, yy):
        return pltpu.make_async_remote_copy(
            src_ref=ps.at[g, rows_of(2 * yy + 1 - c), :], dst_ref=pr.at[g, yy],
            send_sem=qsend.at[g, yy], recv_sem=qrecv.at[g, yy],
            device_id=(s, mate), device_id_type=MESH,
        )

    TURN = (2, 1, 3, 0)

    def compute(g):
        for dy in (0, -1, 1, 2):
            x_copy(g, lane(dy, 1 - c), 2, 0, t).wait_recv()
        if g == 0:
            for load in loads[1:]:
                load.wait()

        def block(i, carry):
            dy = jnp.where(i == 0, 2, jnp.where(i == 1, 1, jnp.where(i == 2, 3, 0)))
            yy = (y + dy) % 4
            rows = pl.ds(pl.multiple_of(yy * 2 * CH, 32), 2 * CH)
            value = xs[g, rows, :]
            gate = jnp.dot(value, gw[...], preferred_element_type=f32)
            upper = jnp.dot(value, uw[...], preferred_element_type=f32)
            act[...] = (gate / (1.0 + jnp.exp(-gate)) * upper).astype(bf16)
            ps[g, rows, :] = jnp.dot(act[...], dw[...], preferred_element_type=f32).astype(bf16)
            pair_copy(g, yy).start()
            return carry

        lax.fori_loop(0, 4, block, 0)

    def add_into(g, position, cols, terms):
        rows = rows_of(position)
        total = ps[g, rows, cols].astype(f32)
        for term in terms:
            total = total + term.astype(f32)
        ps[g, rows, cols] = total.astype(bf16)

    def r_copy(g, dy, part, send, direction, ref, sem, slot):
        cols = pl.ds(part * HW, HW)
        return pltpu.make_async_remote_copy(
            src_ref=ps.at[g, rows_of(lane(dy, c)), cols], dst_ref=ref.at[(g,) + slot],
            send_sem=rsend.at[g, send], recv_sem=sem.at[(g,) + slot],
            device_id=(s, lane(direction, c)), device_id_type=MESH,
        )

    def r_sends(g):
        return [
            (g, 2, 0, 0, 1, rh, rhrecv, (0,)), (g, 2, 1, 1, -1, rh, rhrecv, (1,)),
            (g, 1, 1, 2, 1, rf, rfrecv, (0, 1)), (g, -1, 0, 3, -1, rf, rfrecv, (1, 0)),
            (g, 1, 0, 4, 1, rf, rfrecv, (0, 0)), (g, -1, 1, 5, -1, rf, rfrecv, (1, 1)),
        ]

    def pair(g):
        todo = r_sends(g)
        for turn, dy in enumerate(TURN):
            yy = (y + dy) % 4
            pair_copy(g, yy).wait_recv()
            for k in range(2):
                cols = pl.ds(k * HW, HW)
                add_into(g, 2 * yy + c, cols, [pr[g, yy, :, cols]])
            if turn == 0:
                r_copy(*todo[0]).start()
                r_copy(*todo[1]).start()
            if turn == 1:
                r_copy(*todo[2]).start()
            if turn == 2:
                r_copy(*todo[3]).start()

    def middle(g):
        todo = r_sends(g)
        r_copy(*todo[0]).wait_recv()
        add_into(g, lane(1, c), pl.ds(0, HW), [rh[g, 0]])
        r_copy(*todo[4]).start()
        r_copy(*todo[1]).wait_recv()
        add_into(g, lane(-1, c), pl.ds(HW, HW), [rh[g, 1]])
        r_copy(*todo[5]).start()

    def finish(g):
        todo = r_sends(g)
        for k in range(2, 6):
            r_copy(*todo[k]).wait_recv()
        rows = group_rows(g)
        own = pl.multiple_of(t * CH, 16)
        extra = jnp.zeros((64, REM), f32)
        for j in range(4):
            cols = pl.ds(j * REM, REM)
            inner = pl.ds((j % 2) * REM, REM)
            total = (
                ps[g, pl.ds(own, CH), cols].astype(f32)
                + rf[g, 0, j // 2, :, inner].astype(f32)
                + rf[g, 1, j // 2, :, inner].astype(f32)
            ).astype(bf16)
            reto[rows, cols] = total[:64]
            extra = extra + lax.dot_general(fold[j], total[64:], over_rows, preferred_element_type=f32)
        reto[rows, pl.ds(WID, REM)] = extra.astype(bf16)
        for dx in (0, 1, -1, 2):
            to = at(GROUPS[g], dx)
            if (GROUPS[g], dx) == (0, 0):
                ret[band(s), :] = reto[band(s), :]
            else:
                plane_copy(reto, ret, bsend, brecv, to, s).start()

    for stage, g in (
        (build, 0), (build, 1), (forward, 0), (build, 2), (forward, 1), (build, 3), (far, 0),
        (compute, 0), (pair, 0), (forward, 2), (far, 1), (compute, 1), (pair, 1), (middle, 0),
        (forward, 3), (far, 2), (compute, 2), (pair, 2), (finish, 0), (middle, 1), (far, 3),
        (compute, 3), (pair, 3), (middle, 2), (finish, 1), (middle, 3), (finish, 2), (finish, 3),
    ):
        stage(g)

    for dz, dx in others:
        plane_copy(reto, ret, bsend, brecv, s, at(dz, dx)).wait_recv()
    for j in range(4):
        cols = pl.ds(j * REM, REM)
        back = ret[:, cols]
        tail = ret[:, pl.ds(WID, REM)]
        routed = jnp.dot(cm[...], jnp.concatenate([back, back], axis=0), preferred_element_type=f32)
        routed = routed + jnp.dot(
            cr[j], jnp.concatenate([tail, tail], axis=0), preferred_element_type=f32
        )
        out_ref[:, cols] = (att[:, cols] + routed).astype(bf16)

    for dz, dx in others:
        plane_copy(outg, arr, psend, precv, at(dz, dx), s).wait_send()
        plane_copy(reto, ret, bsend, brecv, at(dz, dx), s).wait_send()
    for g in range(4):
        for copy in x_sends(g):
            x_copy(*copy).wait_send()
        for yy in range(4):
            pair_copy(g, yy).wait_send()
        for copy in r_sends(g):
            r_copy(*copy).wait_send()


def routed_experts(
    heads, stream, ffn_gain, routes, route_weight, out_weight, gate_weight, up_weight, down_weight
):
    any_space = pl.BlockSpec(memory_space=pl.ANY)
    vmem = pl.BlockSpec(memory_space=pltpu.VMEM)
    bf16, f32 = jnp.bfloat16, jnp.float32
    dma = pltpu.SemaphoreType.DMA
    return pl.pallas_call(
        expert_kernel,
        out_shape=jax.ShapeDtypeStruct((128, WID), bf16),
        in_specs=[vmem] * 5 + [any_space] * 4,
        out_specs=vmem,
        scratch_shapes=[
            pltpu.VMEM((1024, WID), bf16),
            pltpu.VMEM((WID, 640), bf16),
            pltpu.VMEM((WID, 640), bf16),
            pltpu.VMEM((640, WID), bf16),
            pltpu.VMEM((128, WID), f32),
            pltpu.VMEM((128, WID), bf16),
            pltpu.VMEM((256, BAND), bf16),
            pltpu.VMEM((256, BAND), bf16),
            pltpu.VMEM((256, BAND), bf16),
            pltpu.VMEM((256, BAND), bf16),
            pltpu.VMEM((4, NT * CH, WID), bf16),
            pltpu.VMEM((2 * CH, 640), bf16),
            pltpu.VMEM((4, NT * CH, WID), bf16),
            pltpu.VMEM((4, 4, CH, WID), bf16),
            pltpu.VMEM((4, 2, CH, HW), bf16),
            pltpu.VMEM((4, 2, 2, CH, HW), bf16),
            pltpu.VMEM((128, 512), bf16),
            pltpu.VMEM((4, 128, 512), bf16),
            dma((4,)),
            dma((16,)), dma((16,)),
            dma((4, 8)), dma((4, 8, 2)),
            dma((4, 4)), dma((4, 4)),
            dma((4, 6)), dma((4, 2)), dma((4, 2, 2)),
            dma((16,)), dma((16,)),
        ],
        compiler_params=pltpu.CompilerParams(
            collective_id=1, has_side_effects=True, vmem_limit_bytes=63 * 1024 * 1024
        ),
        name="experts",
    )(
        heads, stream, ffn_gain.reshape(1, -1), routes, route_weight,
        out_weight, gate_weight, up_weight, down_weight,
    )


def local(
    queries,
    key_rows,
    value_rows,
    lambdas,
    head_gain,
    out_weight,
    stream,
    ffn_gain,
    routes,
    route_weight,
    gate_weight,
    up_weight,
    down_weight,
):
    heads_local = attention(lambdas, head_gain, queries, key_rows, value_rows)
    return routed_experts(
        heads_local, stream, ffn_gain, routes, route_weight,
        out_weight, gate_weight, up_weight, down_weight,
    )


def solution(mesh):
    placed = (
        P("sp", "tp"),
        P("sp", "tp"),
        P("sp", "tp"),
        P("tp"),
        P(),
        P(),
        P(("sp", "tp"), None),
        P(),
        P(("sp", "tp"), None),
        P(("sp", "tp"), None),
        P("sp", None, "tp"),
        P("sp", None, "tp"),
        P("sp", "tp", None),
    )
    return jax.shard_map(
        local, mesh=mesh, in_specs=placed, out_specs=P(("sp", "tp"), None), check_vma=False
    )
```

```python
import functools

import jax
import jax.numpy as jnp
from jax import lax
from jax.experimental import pallas as pl
from jax.experimental.pallas import tpu as pltpu
from jax.sharding import PartitionSpec as P

DH = 64


LOG2E = 1.4426950408889634
MESH = pl.DeviceIdType.MESH
NZ = 4
NX = 4
BLK = 1024
HALF = 512
NEG = -1e30
VROWS = 144
TQ = 512
KB = 256
WORK = (
    (0, 0), (3, 0), (1, 0), (3, 3), (3, 1), (1, 3), (1, 1), (3, 2), (1, 2),
    (2, 0), (2, 3), (2, 1), (2, 2), (0, 3), (0, 1), (0, 2),
)


def attention_kernel(
    lam_hbm, gain_hbm, q_hbm, k_hbm, v_hbm, out_ref,
    lam_ref, gain_ref, vin, lamv, qfull, qother, kb, vb, qm, mx, acc, pout, pin, sout, sin, obuf, sbuf0, sbuf1, fbuf0, fbuf1, nbuf0, nbuf1,
    load_sem, lsend, lrecv, send_sem, recv_sem, msend, mrecv, psend, precv, ssend, srecv, osend, orecv,
):
    sp = lax.axis_index("sp")
    t = lax.axis_index("tp")
    z, x = sp // NX, sp % NX
    y, c = t // 2, t % 2
    mate = 2 * y + 1 - c
    f32, bf16 = jnp.float32, jnp.bfloat16
    sbuf, fbuf, nbuf = (sbuf0, sbuf1), (fbuf0, fbuf1), (nbuf0, nbuf1)

    def at(dz, dx):
        return ((z + dz + NZ) % NZ) * NX + (x + dx + NX) % NX

    loads = [
        pltpu.make_async_copy(q_hbm, qfull.at[0], load_sem.at[0]),
        pltpu.make_async_copy(k_hbm, kb.at[0, 0], load_sem.at[1]),
        pltpu.make_async_copy(v_hbm, vin, load_sem.at[2]),
    ]
    small = [
        pltpu.make_async_copy(lam_hbm, lam_ref, load_sem.at[3]),
        pltpu.make_async_copy(gain_hbm, gain_ref, load_sem.at[4]),
    ]
    for load in loads + small:
        load.start()

    barrier = pltpu.get_barrier_semaphore()
    for dz, dx in ((0, 1), (0, -1), (1, 0), (-1, 0), (2, 0), (0, 2)):
        pl.semaphore_signal(barrier, inc=1, device_id=(at(dz, dx), t), device_id_type=MESH)
    for j in range(1, 8):
        pl.semaphore_signal(barrier, inc=1, device_id=(sp, (t + j) % 8), device_id_type=MESH)

    def along(e, queries, d):
        own = c if e == 0 else 1 - c
        first = at(d, 0) if queries else at(0, d)
        second = at(0, d) if queries else at(d, 0)
        return jnp.where(own == 0, first, second)

    def piece(kind, slot, part):
        span = pl.ds(0, BLK) if part == 2 else pl.ds(part * HALF, HALF)
        if kind == 0:
            return qfull.at[slot, span, :]
        if kind == 1:
            return kb.at[0, slot, span, :]
        return vb.at[0, slot, :, span]

    def ring_copy(kind, slot, part, lane):
        d = 1 if lane == 0 else -1
        return pltpu.make_async_remote_copy(
            src_ref=piece(kind, slot, part), dst_ref=piece(kind, (slot - d) % 4, part),
            send_sem=send_sem.at[kind, slot, lane],
            recv_sem=recv_sem.at[kind, (slot - d) % 4, part % 2],
            device_id=(along(0, kind == 0, d), t), device_id_type=MESH,
        )

    RING = ((0, 2, 0), (0, 2, 1), (3, 0, 0), (1, 1, 1))

    def ring_wait(kind, slot):
        for part in (0, 1) if slot == 2 else (2,):
            pltpu.make_async_remote_copy(
                src_ref=piece(kind, slot, part), dst_ref=piece(kind, slot, part),
                send_sem=send_sem.at[kind, 0, 0], recv_sem=recv_sem.at[kind, slot, part % 2],
                device_id=(sp, mate), device_id_type=MESH,
            ).wait_recv()

    def mate_copy(kind, slot):
        if kind == 0:
            source = qfull.at[slot, pl.ds(pl.multiple_of((1 - c) * HALF, HALF), HALF), :]
            target = qother.at[slot]
        elif kind == 1:
            source, target = kb.at[0, slot], kb.at[1, slot]
        else:
            source, target = vb.at[0, slot], vb.at[1, slot]
        return pltpu.make_async_remote_copy(
            src_ref=source, dst_ref=target,
            send_sem=msend.at[kind, slot], recv_sem=mrecv.at[kind, slot],
            device_id=(sp, mate), device_id_type=MESH,
        )

    def lambda_copy():
        return pltpu.make_async_remote_copy(
            src_ref=lamv.at[0], dst_ref=lamv.at[1], send_sem=lsend, recv_sem=lrecv,
            device_id=(sp, mate), device_id_type=MESH,
        )

    lane_ids = lax.broadcasted_iota(jnp.int32, (HALF, 2 * DH), 1)

    def split_maps(e, slot):
        if e == 0:
            q = qfull[slot, pl.ds(pl.multiple_of(c * HALF, HALF), HALF), :]
        else:
            q = qother[slot]
        zero = jnp.zeros_like(q)
        qm[e, slot, 0] = jnp.where(lane_ids < DH, q, zero)
        qm[e, slot, 1] = jnp.where(lane_ids < DH, zero, q)

    def arrive(kind, slot):
        ring_wait(kind, slot)
        if slot == 3:
            ring_copy(kind, 3, 0, 0).start()
        if slot == 1:
            ring_copy(kind, 1, 1, 1).start()
        mate_copy(kind, slot).start()

    def settle(kind, slot):
        mate_copy(kind, slot).wait_recv()
        if kind == 0:
            split_maps(0, slot)
            split_maps(1, slot)

    for load in loads + small:
        load.wait()
    lamv[0] = jnp.full((8, HALF), lam_ref[0], f32)
    pl.semaphore_wait(barrier, 13)
    for kind in (0, 1):
        for lane in range(2):
            ring_copy(kind, 0, 2, lane).start()
    mate_copy(1, 0).start()
    mate_copy(0, 0).start()
    lambda_copy().start()
    for k in range(4):
        span = pl.ds(k * 256, 256)
        vb[0, 0, :, span] = vin[span, :].astype(f32).T.astype(bf16)
    for lane in range(2):
        ring_copy(2, 0, 2, lane).start()
    mate_copy(2, 0).start()

    mx[...] = jnp.full(mx.shape, NEG, f32)
    acc[...] = jnp.zeros(acc.shape, f32)

    scale = LOG2E * DH ** (-0.5)

    always = sp >= 0

    def tiles(e, di, dk, masked):
        chunks = [(m, r) for m in range(2) for r in range(HALF // TQ)]

        def phase(now, later):
            tops, pv = [], None
            for kk in range(BLK // KB):
                keys = pl.ds(kk * KB, KB)
                if later is not None:
                    m, r = chunks[later]
                    scores = lax.dot_general(
                        kb[e, dk, keys, :], qm[e, di, m, pl.ds(r * TQ, TQ), :],
                        (((1,), (1,)), ((), ())), preferred_element_type=f32,
                    ) * scale
                    if masked:
                        key_id = lax.broadcasted_iota(jnp.int32, scores.shape, 0) + kk * KB
                        query_id = lax.broadcasted_iota(jnp.int32, scores.shape, 1) + (c * HALF + r * TQ)
                        scores = jnp.where(key_id <= query_id, scores, NEG)
                    sbuf[later % 2][keys, :] = scores
                    tops.append(jnp.max(scores, axis=0, keepdims=True))
                if now is not None:
                    m, r = chunks[now]
                    values = jnp.concatenate(
                        [vb[e, dk, :, keys], jnp.ones((VROWS - 128, KB), bf16)], axis=0
                    )
                    weights = jnp.exp2(sbuf[now % 2][keys, :] - nbuf[now % 2][...]).astype(bf16)
                    term = jnp.dot(values, weights, preferred_element_type=f32)
                    pv = term if pv is None else pv + term
            if now is not None:
                m, r = chunks[now]
                cols = pl.ds(r * TQ, TQ)
                acc[e, di, m, :, cols] = acc[e, di, m, :, cols] * fbuf[now % 2][...] + pv
            if later is not None:
                m, r = chunks[later]
                cols = pl.ds(r * TQ, TQ)
                old = mx[e, di, m, :, cols]
                new = functools.reduce(jnp.maximum, tops, old)
                fbuf[later % 2][...] = jnp.exp2(old - new)
                nbuf[later % 2][...] = new
                mx[e, di, m, :, cols] = new

        phase(None, 0)
        for n in range(len(chunks)):
            @pl.when(always)
            def _(n=n):
                phase(n, n + 1 if n + 1 < len(chunks) else None)

    def partial_copies(e, d):
        to = along(e, True, d)
        slot = (4 - d) % 4
        return [
            pltpu.make_async_remote_copy(
                src_ref=pout.at[e, d], dst_ref=pin.at[e, slot],
                send_sem=psend.at[e, d], recv_sem=precv.at[e, slot],
                device_id=(to, t), device_id_type=MESH,
            ),
            pltpu.make_async_remote_copy(
                src_ref=sout.at[e, d], dst_ref=sin.at[e, slot],
                send_sem=ssend.at[e, d], recv_sem=srecv.at[e, slot],
                device_id=(to, t), device_id_type=MESH,
            ),
        ]

    def normal(e, d, m):
        total = acc[e, d, m, pl.ds(128, 1), :]
        some = total > 0.0
        safe = jnp.where(some, total, 1.0)
        level = jnp.where(some, mx[e, d, m] + jnp.log2(safe), NEG)
        return acc[e, d, m, pl.ds(0, 128), :] / safe, level

    def send_partial(d):
        for e in range(2):
            for m in range(2):
                value, level = normal(e, d, m)
                pout[e, d, m] = value.astype(bf16)
                sout[e, d, m] = jnp.broadcast_to(level, (8, HALF))
            for copy in partial_copies(e, d):
                copy.start()

    def before(n):
        if n == 0:
            for kind in (1, 0, 2):
                settle(kind, 0)
        if n == 1:
            for kind in range(3):
                for slot in (3, 1):
                    arrive(kind, slot)
            for kind in range(3):
                for slot in (3, 1):
                    settle(kind, slot)
        if n == 5:
            for kind in range(3):
                arrive(kind, 2)
            for kind in range(3):
                settle(kind, 2)
        if n == 8:
            send_partial(3)
        if n == 9:
            send_partial(1)
        if n == 13:
            send_partial(2)

    def step(n, carry):
        for k in (0, 1, 5, 8, 9, 13):
            @pl.when(n == k)
            def _(k=k):
                before(k)

        di = jnp.int32(0)
        dk = jnp.int32(0)
        for k, (a, b) in enumerate(WORK):
            di = jnp.where(n == k, a, di)
            dk = jnp.where(n == k, b, dk)

        def one_head(e, inner):
            head = jnp.where(e == 0, c, 1 - c)
            query_block = jnp.where(head == 0, at(di, 0), at(0, di))
            key_block = jnp.where(head == 0, at(0, dk), at(dk, 0))

            @pl.when(key_block < query_block)
            def _():
                tiles(e, di, dk, False)

            @pl.when(key_block == query_block)
            def _():
                tiles(e, di, dk, True)

            return inner

        return lax.fori_loop(0, 2, one_head, carry)

    lax.fori_loop(0, len(WORK), step, 0)

    def out_copy(e, j, sender):
        cols = pl.ds(pl.multiple_of(sender * 128, 128), 128)
        return pltpu.make_async_remote_copy(
            src_ref=obuf.at[e, pl.ds(j * 128, 128), :], dst_ref=out_ref.at[:, cols],
            send_sem=osend.at[e, j], recv_sem=orecv.at[sender],
            device_id=(sp, 4 * c + j), device_id_type=MESH,
        )

    def own_copy(e, j, head):
        cols = pl.ds(pl.multiple_of(head * 128, 128), 128)
        return pltpu.make_async_copy(
            obuf.at[e, pl.ds(j * 128, 128), :], out_ref.at[:, cols], osend.at[e, j]
        )

    lambda_copy().wait_recv()
    for e in range(2):
        head = t if e == 0 else mate
        for slot in (1, 3, 2):
            pltpu.make_async_remote_copy(
                src_ref=pout.at[e, slot], dst_ref=pin.at[e, slot],
                send_sem=psend.at[e, slot], recv_sem=precv.at[e, slot],
                device_id=(sp, mate), device_id_type=MESH,
            ).wait_recv()
            pltpu.make_async_remote_copy(
                src_ref=sout.at[e, slot], dst_ref=sin.at[e, slot],
                send_sem=ssend.at[e, slot], recv_sem=srecv.at[e, slot],
                device_id=(sp, mate), device_id_type=MESH,
            ).wait_recv()
        mixed = []
        for m in range(2):
            value, level = normal(e, 0, m)
            levels = [level] + [sin[e, slot, m, pl.ds(0, 1), :] for slot in (1, 2, 3)]
            top = jnp.maximum(jnp.maximum(levels[0], levels[1]), jnp.maximum(levels[2], levels[3]))
            share = [jnp.exp2(item - top) for item in levels]
            inverse = 1.0 / (share[0] + share[1] + share[2] + share[3])
            total = value * (share[0] * inverse)
            for slot in (1, 2, 3):
                total = total + pin[e, slot, m].astype(f32) * (share[slot] * inverse)
            mixed.append(total)
        contrast = mixed[0] - lamv[e, pl.ds(0, 1), :] * mixed[1]
        mean = jnp.mean(contrast * contrast, axis=0, keepdims=True)
        contrast = contrast * lax.rsqrt(mean + 1e-05)
        for j in range(4):
            rows = contrast[:, j * 128:(j + 1) * 128].T * gain_ref[...]
            obuf[e, pl.ds(j * 128, 128), :] = rows.astype(bf16)
        for j in range(4):
            @pl.when(t != 4 * c + j)
            def _(e=e, j=j, head=head):
                out_copy(e, j, head).start()
            @pl.when(t == 4 * c + j)
            def _(e=e, j=j, head=head):
                own_copy(e, j, head).start()

    origin = t // 4
    for yy in range(4):
        for core in range(2):
            @pl.when(2 * yy + origin != t)
            def _(yy=yy, core=core):
                out_copy(0, 0, 2 * yy + core).wait_recv()
    for e in range(2):
        for j in range(4):
            @pl.when(t != 4 * c + j)
            def _(e=e, j=j):
                out_copy(e, j, t).wait_send()
            @pl.when(t == 4 * c + j)
            def _(e=e, j=j):
                own_copy(e, j, t).wait()
    lambda_copy().wait_send()
    for kind in range(3):
        for slot, part, lane in RING:
            ring_copy(kind, slot, part, lane).wait_send()
        for slot in range(4):
            mate_copy(kind, slot).wait_send()
    for e in range(2):
        for d in (1, 2, 3):
            for copy in partial_copies(e, d):
                copy.wait_send()


def attention(lambdas, head_gain, queries, key_rows, value_rows):
    any_space = pl.BlockSpec(memory_space=pltpu.HBM)
    bf16, f32 = jnp.bfloat16, jnp.float32
    dma = pltpu.SemaphoreType.DMA
    return pl.pallas_call(
        attention_kernel,
        out_shape=jax.ShapeDtypeStruct((128, 1024), jnp.bfloat16),
        in_specs=[
            any_space, any_space, any_space, any_space, any_space,
        ],
        out_specs=any_space,
        scratch_shapes=[
            pltpu.SMEM((1,), f32),
            pltpu.VMEM((1, 128), f32),
            pltpu.VMEM((BLK, 128), bf16),
            pltpu.VMEM((2, 8, HALF), f32),
            pltpu.VMEM((4, BLK, 128), bf16),
            pltpu.VMEM((4, HALF, 128), bf16),
            pltpu.VMEM((2, 4, BLK, 128), bf16),
            pltpu.VMEM((2, 4, 128, BLK), bf16),
            pltpu.VMEM((2, 4, 2, HALF, 128), bf16),
            pltpu.VMEM((2, 4, 2, 1, HALF), f32),
            pltpu.VMEM((2, 4, 2, VROWS, HALF), f32),
            pltpu.VMEM((2, 4, 2, 128, HALF), bf16),
            pltpu.VMEM((2, 4, 2, 128, HALF), bf16),
            pltpu.VMEM((2, 4, 2, 8, HALF), f32),
            pltpu.VMEM((2, 4, 2, 8, HALF), f32),
            pltpu.VMEM((2, HALF, 128), bf16),
            pltpu.VMEM((BLK, TQ), f32), pltpu.VMEM((BLK, TQ), f32),
            pltpu.VMEM((1, TQ), f32), pltpu.VMEM((1, TQ), f32),
            pltpu.VMEM((1, TQ), f32), pltpu.VMEM((1, TQ), f32),
            dma((5,)),
            dma, dma,
            dma((3, 4, 2)), dma((3, 4, 2)),
            dma((3, 4)), dma((3, 4)),
            dma((2, 4)), dma((2, 4)),
            dma((2, 4)), dma((2, 4)),
            dma((2, 4)), dma((8,)),
        ],
        compiler_params=pltpu.CompilerParams(
            collective_id=0, has_side_effects=True, vmem_limit_bytes=67043328
        ),
        name="attention",
    )(lambdas, head_gain.reshape(1, -1), queries, key_rows, value_rows)


GROUPS = (0, -1, 1, 2)
MAIN = 16
CH = 80
WID = 2048
HW = 1024
REM = 512
BAND = WID + REM
NT = 8


def expert_kernel(
    heads_hbm, stream_hbm, gain_hbm, routes_hbm, rw_hbm, ow_hbm, gate_hbm, up_hbm, down_hbm,
    out_ref,
    heads_ref, stream_ref, gain_ref, routes_ref, rw_ref, ow, gw, uw, dw, att, nrm, outg, arr, reto, ret, xs, act, ps, pr, rh, rf, cm, cr,
    load_sem, psend, precv, xsend, xrecv, qsend, qrecv, rsend, rhrecv, rfrecv, bsend, brecv,
):
    s = lax.axis_index("sp")
    t = lax.axis_index("tp")
    z, x = s // NX, s % NX
    y, c = t // 2, t % 2
    mate = 2 * y + 1 - c
    bf16, f32 = jnp.bfloat16, jnp.float32

    def at(dz, dx):
        return ((z + dz + NZ) % NZ) * NX + (x + dx + NX) % NX

    def lane(dy, core):
        return 2 * ((y + dy + 4) % 4) + core

    loads = [
        pltpu.make_async_copy(ow_hbm, ow, load_sem.at[0]),
        pltpu.make_async_copy(gate_hbm.at[0], gw, load_sem.at[1]),
        pltpu.make_async_copy(up_hbm.at[0], uw, load_sem.at[2]),
        pltpu.make_async_copy(down_hbm.at[0], dw, load_sem.at[3]),
    ]
    small = [
        pltpu.make_async_copy(routes_hbm, routes_ref, load_sem.at[4]),
        pltpu.make_async_copy(rw_hbm, rw_ref, load_sem.at[5]),
        pltpu.make_async_copy(stream_hbm, stream_ref, load_sem.at[6]),
        pltpu.make_async_copy(gain_hbm, gain_ref, load_sem.at[7]),
        pltpu.make_async_copy(heads_hbm, heads_ref, load_sem.at[8]),
    ]
    for load in small + loads:
        load.start()

    barrier = pltpu.get_barrier_semaphore()
    others = [(dz, dx) for dz in GROUPS for dx in (0, 1, -1, 2) if (dz, dx) != (0, 0)]
    for dz, dx in others:
        pl.semaphore_signal(barrier, inc=1, device_id=(at(dz, dx), t), device_id_type=MESH)
    for peer in (lane(1, c), lane(-1, c), mate):
        pl.semaphore_signal(barrier, inc=1, device_id=(s, peer), device_id_type=MESH)

    for load in small + loads[:1]:
        load.wait()
    heads = heads_ref[...]
    square = jnp.zeros((128, 1), f32)
    for k in range(0, WID, 512):
        cols = pl.ds(k, 512)
        value = stream_ref[:, cols].astype(f32) + jnp.dot(heads, ow[:, cols], preferred_element_type=f32)
        att[:, cols] = value
        square = square + jnp.sum(value * value, axis=1, keepdims=True)
    inverse = lax.rsqrt(square * (1.0 / WID) + 1e-06)
    for k in range(0, WID, 512):
        cols = pl.ds(k, 512)
        nrm[:, cols] = (att[:, cols] * inverse * gain_ref[:, cols]).astype(bf16)

    experts = lax.broadcasted_iota(jnp.int32, (16, 128), 0)
    route = [routes_ref[pl.ds(k, 1), :] for k in range(2)]
    hot = [(r == experts).astype(f32) for r in route]
    row_id = lax.broadcasted_iota(jnp.int32, (128, 128), 0)
    col_id = lax.broadcasted_iota(jnp.int32, (128, 128), 1)
    earlier = (row_id < col_id).astype(f32).astype(bf16)
    before = jnp.dot((hot[0] + hot[1]).astype(bf16), earlier, preferred_element_type=f32)
    place = lax.broadcasted_iota(jnp.int32, (256, 128), 0).astype(f32)
    main_hit, rem_hit = [], []
    for k in range(2):
        slot = jnp.sum(before * hot[k], axis=0, keepdims=True)
        base = route[k].astype(f32) * 16.0 + slot
        low = slot < float(MAIN)
        main_hit.append((jnp.where(low, base, -1.0) == place).astype(f32))
        rem_hit.append([
            (jnp.where(low, -1.0, base + (4.0 * j - 16.0)) == place).astype(f32) for j in range(4)
        ])
    weight = [rw_ref[pl.ds(k, 1), :] for k in range(2)]
    over_rows = (((0,), (0,)), ((), ()))
    chosen = (main_hit[0] + main_hit[1]).astype(bf16)
    for k in range(0, WID, 512):
        cols = pl.ds(k, 512)
        outg[:, cols] = jnp.dot(chosen, nrm[:, cols], preferred_element_type=f32).astype(bf16)
    extra = jnp.zeros((256, REM), f32)
    for j in range(4):
        extra = extra + jnp.dot(
            (rem_hit[0][j] + rem_hit[1][j]).astype(bf16), nrm[:, pl.ds(j * REM, REM)],
            preferred_element_type=f32,
        )
    outg[:, pl.ds(WID, REM)] = extra.astype(bf16)

    def keep_split(ref, value):
        high = value.astype(bf16)
        ref[pl.ds(0, 256), :] = high
        ref[pl.ds(256, 256), :] = (value - high.astype(f32)).astype(bf16)

    pl.semaphore_wait(barrier, len(others) + 3)

    def band(device):
        return pl.ds(pl.multiple_of(device * MAIN, MAIN), MAIN)

    def plane_copy(source, target, ssem, rsem, to, sender):
        return pltpu.make_async_remote_copy(
            src_ref=source.at[band(to), :], dst_ref=target.at[band(sender), :],
            send_sem=ssem.at[to], recv_sem=rsem.at[sender],
            device_id=(to, t), device_id_type=MESH,
        )

    for dz, dx in others:
        plane_copy(outg, arr, psend, precv, at(-dz, -dx), s).start()
    arr[band(s), :] = outg[band(s), :]
    keep_split(cm, weight[0] * main_hit[0] + weight[1] * main_hit[1])
    for j in range(4):
        keep_split(cr.at[j], weight[0] * rem_hit[0][j] + weight[1] * rem_hit[1][j])

    fold_row = lax.broadcasted_iota(jnp.int32, (16, 64), 0)
    fold_col = lax.broadcasted_iota(jnp.int32, (16, 64), 1)
    fold = [
        (fold_col == 16 * (fold_row >> 2) + 4 * j + (fold_row & 3)).astype(f32).astype(bf16)
        for j in range(4)
    ]

    def rows_of(position):
        return pl.ds(pl.multiple_of(position * CH, 16), CH)

    def x_copy(g, position, part, send, to, slot=None):
        cols = pl.ds(0, WID) if part == 2 else pl.ds(part * HW, HW)
        return pltpu.make_async_remote_copy(
            src_ref=xs.at[g, rows_of(position), cols], dst_ref=xs.at[g, rows_of(position), cols],
            send_sem=xsend.at[g, send], recv_sem=xrecv.at[g, position, part % 2],
            device_id=(s, to), device_id_type=MESH,
        )

    def x_sends(g):
        return [
            (g, t, 2, 0, lane(1, c)), (g, t, 2, 1, lane(-1, c)), (g, t, 2, 2, mate),
            (g, lane(-1, c), 0, 3, lane(1, c)), (g, lane(-1, c), 2, 4, mate),
            (g, lane(1, c), 1, 5, lane(-1, c)), (g, lane(1, c), 2, 6, mate),
            (g, lane(2, c), 2, 7, mate),
        ]

    def group_rows(g):
        zz = (z + GROUPS[g] + NZ) % NZ
        return pl.ds(pl.multiple_of(zz * 64, 64), 64)

    def build(g):
        for dx in (0, 1, -1, 2):
            if (GROUPS[g], dx) != (0, 0):
                plane_copy(outg, arr, psend, precv, s, at(GROUPS[g], dx)).wait_recv()
        rows = group_rows(g)
        first = pl.multiple_of(t * CH, 16)
        for k in range(0, WID, 512):
            xs[g, pl.ds(first, 64), pl.ds(k, 512)] = arr[rows, pl.ds(k, 512)]
        for j in range(4):
            xs[g, pl.ds(first + 64, 16), pl.ds(j * REM, REM)] = jnp.dot(
                fold[j], arr[rows, pl.ds(WID, REM)], preferred_element_type=f32
            ).astype(bf16)
        for copy in x_sends(g)[:3]:
            x_copy(*copy).start()

    def forward(g):
        todo = x_sends(g)
        x_copy(g, lane(-1, c), 2, 0, t).wait_recv()
        x_copy(*todo[3]).start()
        x_copy(*todo[4]).start()
        x_copy(g, lane(1, c), 2, 0, t).wait_recv()
        x_copy(*todo[5]).start()
        x_copy(*todo[6]).start()

    def far(g):
        x_copy(g, lane(2, c), 0, 0, t).wait_recv()
        x_copy(g, lane(2, c), 1, 0, t).wait_recv()
        x_copy(*x_sends(g)[7]).start()

    def pair_copy(g, yy):
        return pltpu.make_async_remote_copy(
            src_ref=ps.at[g, rows_of(2 * yy + 1 - c), :], dst_ref=pr.at[g, yy],
            send_sem=qsend.at[g, yy], recv_sem=qrecv.at[g, yy],
            device_id=(s, mate), device_id_type=MESH,
        )

    TURN = (2, 1, 3, 0)

    def compute(g):
        for dy in (0, -1, 1, 2):
            x_copy(g, lane(dy, 1 - c), 2, 0, t).wait_recv()
        if g == 0:
            for load in loads[1:]:
                load.wait()

        def block(i, carry):
            dy = jnp.where(i == 0, 2, jnp.where(i == 1, 1, jnp.where(i == 2, 3, 0)))
            yy = (y + dy) % 4
            rows = pl.ds(pl.multiple_of(yy * 2 * CH, 32), 2 * CH)
            value = xs[g, rows, :]
            gate = jnp.dot(value, gw[...], preferred_element_type=f32)
            upper = jnp.dot(value, uw[...], preferred_element_type=f32)
            act[...] = (gate / (1.0 + jnp.exp(-gate)) * upper).astype(bf16)
            ps[g, rows, :] = jnp.dot(act[...], dw[...], preferred_element_type=f32).astype(bf16)
            pair_copy(g, yy).start()
            return carry

        lax.fori_loop(0, 4, block, 0)

    def add_into(g, position, cols, terms):
        rows = rows_of(position)
        total = ps[g, rows, cols].astype(f32)
        for term in terms:
            total = total + term.astype(f32)
        ps[g, rows, cols] = total.astype(bf16)

    def r_copy(g, dy, part, send, direction, ref, sem, slot):
        cols = pl.ds(part * HW, HW)
        return pltpu.make_async_remote_copy(
            src_ref=ps.at[g, rows_of(lane(dy, c)), cols], dst_ref=ref.at[(g,) + slot],
            send_sem=rsend.at[g, send], recv_sem=sem.at[(g,) + slot],
            device_id=(s, lane(direction, c)), device_id_type=MESH,
        )

    def r_sends(g):
        return [
            (g, 2, 0, 0, 1, rh, rhrecv, (0,)), (g, 2, 1, 1, -1, rh, rhrecv, (1,)),
            (g, 1, 1, 2, 1, rf, rfrecv, (0, 1)), (g, -1, 0, 3, -1, rf, rfrecv, (1, 0)),
            (g, 1, 0, 4, 1, rf, rfrecv, (0, 0)), (g, -1, 1, 5, -1, rf, rfrecv, (1, 1)),
        ]

    def pair(g):
        todo = r_sends(g)
        for turn, dy in enumerate(TURN):
            yy = (y + dy) % 4
            pair_copy(g, yy).wait_recv()
            for k in range(2):
                cols = pl.ds(k * HW, HW)
                add_into(g, 2 * yy + c, cols, [pr[g, yy, :, cols]])
            if turn == 0:
                r_copy(*todo[0]).start()
                r_copy(*todo[1]).start()
            if turn == 1:
                r_copy(*todo[2]).start()
            if turn == 2:
                r_copy(*todo[3]).start()

    def middle(g):
        todo = r_sends(g)
        r_copy(*todo[0]).wait_recv()
        add_into(g, lane(1, c), pl.ds(0, HW), [rh[g, 0]])
        r_copy(*todo[4]).start()
        r_copy(*todo[1]).wait_recv()
        add_into(g, lane(-1, c), pl.ds(HW, HW), [rh[g, 1]])
        r_copy(*todo[5]).start()

    def finish(g):
        todo = r_sends(g)
        for k in range(2, 6):
            r_copy(*todo[k]).wait_recv()
        rows = group_rows(g)
        own = pl.multiple_of(t * CH, 16)
        extra = jnp.zeros((64, REM), f32)
        for j in range(4):
            cols = pl.ds(j * REM, REM)
            inner = pl.ds((j % 2) * REM, REM)
            total = (
                ps[g, pl.ds(own, CH), cols].astype(f32)
                + rf[g, 0, j // 2, :, inner].astype(f32)
                + rf[g, 1, j // 2, :, inner].astype(f32)
            ).astype(bf16)
            reto[rows, cols] = total[:64]
            extra = extra + lax.dot_general(fold[j], total[64:], over_rows, preferred_element_type=f32)
        reto[rows, pl.ds(WID, REM)] = extra.astype(bf16)
        for dx in (0, 1, -1, 2):
            to = at(GROUPS[g], dx)
            if (GROUPS[g], dx) == (0, 0):
                ret[band(s), :] = reto[band(s), :]
            else:
                plane_copy(reto, ret, bsend, brecv, to, s).start()

    for stage, g in (
        (build, 0), (build, 1), (forward, 0), (build, 2), (forward, 1), (build, 3), (far, 0),
        (compute, 0), (pair, 0), (forward, 2), (far, 1), (compute, 1), (pair, 1), (middle, 0),
        (forward, 3), (far, 2), (compute, 2), (pair, 2), (finish, 0), (middle, 1), (far, 3),
        (compute, 3), (pair, 3), (middle, 2), (finish, 1), (middle, 3), (finish, 2), (finish, 3),
    ):
        stage(g)

    for dz, dx in others:
        plane_copy(reto, ret, bsend, brecv, s, at(dz, dx)).wait_recv()
    for j in range(4):
        cols = pl.ds(j * REM, REM)
        back = ret[:, cols]
        tail = ret[:, pl.ds(WID, REM)]
        routed = lax.dot_general(
            cm[...], jnp.concatenate([back, back], axis=0), over_rows, preferred_element_type=f32
        ) + lax.dot_general(
            cr[j], jnp.concatenate([tail, tail], axis=0), over_rows, preferred_element_type=f32
        )
        out_ref[:, cols] = (att[:, cols] + routed).astype(bf16)

    for dz, dx in others:
        plane_copy(outg, arr, psend, precv, at(dz, dx), s).wait_send()
        plane_copy(reto, ret, bsend, brecv, at(dz, dx), s).wait_send()
    for g in range(4):
        for copy in x_sends(g):
            x_copy(*copy).wait_send()
        for yy in range(4):
            pair_copy(g, yy).wait_send()
        for copy in r_sends(g):
            r_copy(*copy).wait_send()


def routed_experts(
    heads, stream, ffn_gain, routes, route_weight, out_weight, gate_weight, up_weight, down_weight
):
    any_space = pl.BlockSpec(memory_space=pltpu.HBM)
    vmem = pl.BlockSpec(memory_space=pltpu.VMEM)
    bf16, f32 = jnp.bfloat16, jnp.float32
    dma = pltpu.SemaphoreType.DMA
    return pl.pallas_call(
        expert_kernel,
        out_shape=jax.ShapeDtypeStruct((128, WID), bf16),
        in_specs=[any_space] * 9,
        out_specs=vmem,
        scratch_shapes=[
            pltpu.VMEM((128, 1024), bf16),
            pltpu.VMEM((128, WID), bf16),
            pltpu.VMEM((1, WID), f32),
            pltpu.VMEM((2, 128), jnp.int32),
            pltpu.VMEM((2, 128), f32),
            pltpu.VMEM((1024, WID), bf16),
            pltpu.VMEM((WID, 640), bf16),
            pltpu.VMEM((WID, 640), bf16),
            pltpu.VMEM((640, WID), bf16),
            pltpu.VMEM((128, WID), f32),
            pltpu.VMEM((128, WID), bf16),
            pltpu.VMEM((256, BAND), bf16),
            pltpu.VMEM((256, BAND), bf16),
            pltpu.VMEM((256, BAND), bf16),
            pltpu.VMEM((256, BAND), bf16),
            pltpu.VMEM((4, NT * CH, WID), bf16),
            pltpu.VMEM((2 * CH, 640), bf16),
            pltpu.VMEM((4, NT * CH, WID), bf16),
            pltpu.VMEM((4, 4, CH, WID), bf16),
            pltpu.VMEM((4, 2, CH, HW), bf16),
            pltpu.VMEM((4, 2, 2, CH, HW), bf16),
            pltpu.VMEM((512, 128), bf16),
            pltpu.VMEM((4, 512, 128), bf16),
            dma((9,)),
            dma((16,)), dma((16,)),
            dma((4, 8)), dma((4, 8, 2)),
            dma((4, 4)), dma((4, 4)),
            dma((4, 6)), dma((4, 2)), dma((4, 2, 2)),
            dma((16,)), dma((16,)),
        ],
        compiler_params=pltpu.CompilerParams(
            collective_id=1, has_side_effects=True, vmem_limit_bytes=67043328
        ),
        name="experts",
    )(
        heads, stream, ffn_gain.reshape(1, -1), routes.T, route_weight.T,
        out_weight, gate_weight, up_weight, down_weight,
    )


def local(
    queries,
    key_rows,
    value_rows,
    lambdas,
    head_gain,
    out_weight,
    stream,
    ffn_gain,
    routes,
    route_weight,
    gate_weight,
    up_weight,
    down_weight,
):
    heads_local = attention(lambdas, head_gain, queries, key_rows, value_rows)
    return routed_experts(
        heads_local, stream, ffn_gain, routes, route_weight,
        out_weight, gate_weight, up_weight, down_weight,
    )


def solution(mesh):
    placed = (
        P("sp", "tp"),
        P("sp", "tp"),
        P("sp", "tp"),
        P("tp"),
        P(),
        P(),
        P(("sp", "tp"), None),
        P(),
        P(("sp", "tp"), None),
        P(("sp", "tp"), None),
        P("sp", None, "tp"),
        P("sp", None, "tp"),
        P("sp", "tp", None),
    )
    return jax.shard_map(
        local, mesh=mesh, in_specs=placed, out_specs=P(("sp", "tp"), None), check_vma=False
    )
```

```python
import functools

import jax
import jax.numpy as jnp
from jax import lax
from jax.experimental import pallas as pl
from jax.experimental.pallas import tpu as pltpu
from jax.sharding import PartitionSpec as P

DH = 64


LOG2E = 1.4426950408889634
MESH = pl.DeviceIdType.MESH
NZ = 4
NX = 4
BLK = 1024
HALF = 512
NEG = -1e30
VROWS = 144
TQ = 512
KB = 256
WORK = (
    (0, 0), (3, 0), (1, 0), (3, 3), (3, 1), (1, 3), (1, 1), (3, 2), (1, 2),
    (2, 0), (2, 3), (2, 1), (2, 2), (0, 3), (0, 1), (0, 2),
)


def attention_kernel(
    lam_hbm, gain_hbm, q_hbm, k_hbm, v_hbm, out_ref,
    lam_ref, gain_ref, vin, lamv, qfull, qother, kb, vb, qm, mx, acc, pout, pin, sout, sin, obuf, sbuf0, sbuf1, fbuf0, fbuf1, nbuf0, nbuf1,
    load_sem, lsend, lrecv, send_sem, recv_sem, msend, mrecv, psend, precv, ssend, srecv, osend, orecv,
):
    sp = lax.axis_index("sp")
    t = lax.axis_index("tp")
    z, x = sp // NX, sp % NX
    y, c = t // 2, t % 2
    mate = 2 * y + 1 - c
    f32, bf16 = jnp.float32, jnp.bfloat16
    sbuf, fbuf, nbuf = (sbuf0, sbuf1), (fbuf0, fbuf1), (nbuf0, nbuf1)

    def at(dz, dx):
        return ((z + dz + NZ) % NZ) * NX + (x + dx + NX) % NX

    loads = [
        pltpu.make_async_copy(q_hbm, qfull.at[0], load_sem.at[0]),
        pltpu.make_async_copy(k_hbm, kb.at[0, 0], load_sem.at[1]),
        pltpu.make_async_copy(v_hbm, vin, load_sem.at[2]),
    ]
    small = [
        pltpu.make_async_copy(lam_hbm, lam_ref, load_sem.at[3]),
        pltpu.make_async_copy(gain_hbm, gain_ref, load_sem.at[4]),
    ]
    for load in loads + small:
        load.start()

    barrier = pltpu.get_barrier_semaphore()
    for dz, dx in ((0, 1), (0, -1), (1, 0), (-1, 0), (2, 0), (0, 2)):
        pl.semaphore_signal(barrier, inc=1, device_id=(at(dz, dx), t), device_id_type=MESH)
    for j in range(1, 8):
        pl.semaphore_signal(barrier, inc=1, device_id=(sp, (t + j) % 8), device_id_type=MESH)

    def along(e, queries, d):
        own = c if e == 0 else 1 - c
        first = at(d, 0) if queries else at(0, d)
        second = at(0, d) if queries else at(d, 0)
        return jnp.where(own == 0, first, second)

    def piece(kind, slot, part):
        span = pl.ds(0, BLK) if part == 2 else pl.ds(part * HALF, HALF)
        if kind == 0:
            return qfull.at[slot, span, :]
        if kind == 1:
            return kb.at[0, slot, span, :]
        return vb.at[0, slot, :, span]

    def ring_copy(kind, slot, part, lane):
        d = 1 if lane == 0 else -1
        return pltpu.make_async_remote_copy(
            src_ref=piece(kind, slot, part), dst_ref=piece(kind, (slot - d) % 4, part),
            send_sem=send_sem.at[kind, slot, lane],
            recv_sem=recv_sem.at[kind, (slot - d) % 4, part % 2],
            device_id=(along(0, kind == 0, d), t), device_id_type=MESH,
        )

    RING = ((0, 2, 0), (0, 2, 1), (3, 0, 0), (1, 1, 1))

    def ring_wait(kind, slot):
        for part in (0, 1) if slot == 2 else (2,):
            pltpu.make_async_remote_copy(
                src_ref=piece(kind, slot, part), dst_ref=piece(kind, slot, part),
                send_sem=send_sem.at[kind, 0, 0], recv_sem=recv_sem.at[kind, slot, part % 2],
                device_id=(sp, mate), device_id_type=MESH,
            ).wait_recv()

    def mate_copy(kind, slot):
        if kind == 0:
            source = qfull.at[slot, pl.ds(pl.multiple_of((1 - c) * HALF, HALF), HALF), :]
            target = qother.at[slot]
        elif kind == 1:
            source, target = kb.at[0, slot], kb.at[1, slot]
        else:
            source, target = vb.at[0, slot], vb.at[1, slot]
        return pltpu.make_async_remote_copy(
            src_ref=source, dst_ref=target,
            send_sem=msend.at[kind, slot], recv_sem=mrecv.at[kind, slot],
            device_id=(sp, mate), device_id_type=MESH,
        )

    def lambda_copy():
        return pltpu.make_async_remote_copy(
            src_ref=lamv.at[0], dst_ref=lamv.at[1], send_sem=lsend, recv_sem=lrecv,
            device_id=(sp, mate), device_id_type=MESH,
        )

    lane_ids = lax.broadcasted_iota(jnp.int32, (HALF, 2 * DH), 1)

    def split_maps(e, slot):
        if e == 0:
            q = qfull[slot, pl.ds(pl.multiple_of(c * HALF, HALF), HALF), :]
        else:
            q = qother[slot]
        zero = jnp.zeros_like(q)
        qm[e, slot, 0] = jnp.where(lane_ids < DH, q, zero)
        qm[e, slot, 1] = jnp.where(lane_ids < DH, zero, q)

    def arrive(kind, slot):
        ring_wait(kind, slot)
        if slot == 3:
            ring_copy(kind, 3, 0, 0).start()
        if slot == 1:
            ring_copy(kind, 1, 1, 1).start()
        mate_copy(kind, slot).start()

    def settle(kind, slot):
        mate_copy(kind, slot).wait_recv()
        if kind == 0:
            split_maps(0, slot)
            split_maps(1, slot)

    for load in loads + small:
        load.wait()
    lamv[0] = jnp.full((8, HALF), lam_ref[0], f32)
    pl.semaphore_wait(barrier, 13)
    for kind in (0, 1):
        for lane in range(2):
            ring_copy(kind, 0, 2, lane).start()
    mate_copy(1, 0).start()
    mate_copy(0, 0).start()
    lambda_copy().start()
    for k in range(4):
        span = pl.ds(k * 256, 256)
        vb[0, 0, :, span] = vin[span, :].astype(f32).T.astype(bf16)
    for lane in range(2):
        ring_copy(2, 0, 2, lane).start()
    mate_copy(2, 0).start()

    mx[...] = jnp.full(mx.shape, NEG, f32)
    acc[...] = jnp.zeros(acc.shape, f32)

    scale = LOG2E * DH ** (-0.5)

    always = sp >= 0

    def tiles(e, di, dk, masked):
        chunks = [(m, r) for m in range(2) for r in range(HALF // TQ)]

        def phase(now, later):
            tops, pv = [], None
            for kk in range(BLK // KB):
                keys = pl.ds(kk * KB, KB)
                if later is not None:
                    m, r = chunks[later]
                    scores = lax.dot_general(
                        kb[e, dk, keys, :], qm[e, di, m, pl.ds(r * TQ, TQ), :],
                        (((1,), (1,)), ((), ())), preferred_element_type=f32,
                    ) * scale
                    if masked:
                        key_id = lax.broadcasted_iota(jnp.int32, scores.shape, 0) + kk * KB
                        query_id = lax.broadcasted_iota(jnp.int32, scores.shape, 1) + (c * HALF + r * TQ)
                        scores = jnp.where(key_id <= query_id, scores, NEG)
                    sbuf[later % 2][keys, :] = scores
                    tops.append(jnp.max(scores, axis=0, keepdims=True))
                if now is not None:
                    m, r = chunks[now]
                    values = jnp.concatenate(
                        [vb[e, dk, :, keys], jnp.ones((VROWS - 128, KB), bf16)], axis=0
                    )
                    weights = jnp.exp2(sbuf[now % 2][keys, :] - nbuf[now % 2][...]).astype(bf16)
                    term = jnp.dot(values, weights, preferred_element_type=f32)
                    pv = term if pv is None else pv + term
            if now is not None:
                m, r = chunks[now]
                cols = pl.ds(r * TQ, TQ)
                acc[e, di, m, :, cols] = acc[e, di, m, :, cols] * fbuf[now % 2][...] + pv
            if later is not None:
                m, r = chunks[later]
                cols = pl.ds(r * TQ, TQ)
                old = mx[e, di, m, :, cols]
                new = functools.reduce(jnp.maximum, tops, old)
                fbuf[later % 2][...] = jnp.exp2(old - new)
                nbuf[later % 2][...] = new
                mx[e, di, m, :, cols] = new

        phase(None, 0)
        for n in range(len(chunks)):
            @pl.when(always)
            def _(n=n):
                phase(n, n + 1 if n + 1 < len(chunks) else None)

    def partial_copies(e, d):
        to = along(e, True, d)
        slot = (4 - d) % 4
        return [
            pltpu.make_async_remote_copy(
                src_ref=pout.at[e, d], dst_ref=pin.at[e, slot],
                send_sem=psend.at[e, d], recv_sem=precv.at[e, slot],
                device_id=(to, t), device_id_type=MESH,
            ),
            pltpu.make_async_remote_copy(
                src_ref=sout.at[e, d], dst_ref=sin.at[e, slot],
                send_sem=ssend.at[e, d], recv_sem=srecv.at[e, slot],
                device_id=(to, t), device_id_type=MESH,
            ),
        ]

    def normal(e, d, m):
        total = acc[e, d, m, pl.ds(128, 1), :]
        some = total > 0.0
        safe = jnp.where(some, total, 1.0)
        level = jnp.where(some, mx[e, d, m] + jnp.log2(safe), NEG)
        return acc[e, d, m, pl.ds(0, 128), :] / safe, level

    def send_partial(d):
        for e in range(2):
            for m in range(2):
                value, level = normal(e, d, m)
                pout[e, d, m] = value.astype(bf16)
                sout[e, d, m] = jnp.broadcast_to(level, (8, HALF))
            for copy in partial_copies(e, d):
                copy.start()

    def before(n):
        if n == 0:
            for kind in (1, 0, 2):
                settle(kind, 0)
        if n == 1:
            for kind in range(3):
                for slot in (3, 1):
                    arrive(kind, slot)
            for kind in range(3):
                for slot in (3, 1):
                    settle(kind, slot)
        if n == 5:
            for kind in range(3):
                arrive(kind, 2)
            for kind in range(3):
                settle(kind, 2)
        if n == 8:
            send_partial(3)
        if n == 9:
            send_partial(1)
        if n == 13:
            send_partial(2)

    def step(n, carry):
        for k in (0, 1, 5, 8, 9, 13):
            @pl.when(n == k)
            def _(k=k):
                before(k)

        di = jnp.int32(0)
        dk = jnp.int32(0)
        for k, (a, b) in enumerate(WORK):
            di = jnp.where(n == k, a, di)
            dk = jnp.where(n == k, b, dk)

        def one_head(e, inner):
            head = jnp.where(e == 0, c, 1 - c)
            query_block = jnp.where(head == 0, at(di, 0), at(0, di))
            key_block = jnp.where(head == 0, at(0, dk), at(dk, 0))

            @pl.when(key_block < query_block)
            def _():
                tiles(e, di, dk, False)

            @pl.when(key_block == query_block)
            def _():
                tiles(e, di, dk, True)

            return inner

        return lax.fori_loop(0, 2, one_head, carry)

    lax.fori_loop(0, len(WORK), step, 0)

    def out_copy(e, j, sender):
        cols = pl.ds(pl.multiple_of(sender * 128, 128), 128)
        return pltpu.make_async_remote_copy(
            src_ref=obuf.at[e, pl.ds(j * 128, 128), :], dst_ref=out_ref.at[:, cols],
            send_sem=osend.at[e, j], recv_sem=orecv.at[sender],
            device_id=(sp, 4 * c + j), device_id_type=MESH,
        )

    def own_copy(e, j, head):
        cols = pl.ds(pl.multiple_of(head * 128, 128), 128)
        return pltpu.make_async_copy(
            obuf.at[e, pl.ds(j * 128, 128), :], out_ref.at[:, cols], osend.at[e, j]
        )

    lambda_copy().wait_recv()
    for e in range(2):
        head = t if e == 0 else mate
        for slot in (1, 3, 2):
            pltpu.make_async_remote_copy(
                src_ref=pout.at[e, slot], dst_ref=pin.at[e, slot],
                send_sem=psend.at[e, slot], recv_sem=precv.at[e, slot],
                device_id=(sp, mate), device_id_type=MESH,
            ).wait_recv()
            pltpu.make_async_remote_copy(
                src_ref=sout.at[e, slot], dst_ref=sin.at[e, slot],
                send_sem=ssend.at[e, slot], recv_sem=srecv.at[e, slot],
                device_id=(sp, mate), device_id_type=MESH,
            ).wait_recv()
        mixed = []
        for m in range(2):
            value, level = normal(e, 0, m)
            levels = [level] + [sin[e, slot, m, pl.ds(0, 1), :] for slot in (1, 2, 3)]
            top = jnp.maximum(jnp.maximum(levels[0], levels[1]), jnp.maximum(levels[2], levels[3]))
            share = [jnp.exp2(item - top) for item in levels]
            inverse = 1.0 / (share[0] + share[1] + share[2] + share[3])
            total = value * (share[0] * inverse)
            for slot in (1, 2, 3):
                total = total + pin[e, slot, m].astype(f32) * (share[slot] * inverse)
            mixed.append(total)
        contrast = mixed[0] - lamv[e, pl.ds(0, 1), :] * mixed[1]
        mean = jnp.mean(contrast * contrast, axis=0, keepdims=True)
        contrast = contrast * lax.rsqrt(mean + 1e-05)
        for j in range(4):
            rows = contrast[:, j * 128:(j + 1) * 128].T * gain_ref[...]
            obuf[e, pl.ds(j * 128, 128), :] = rows.astype(bf16)
        for j in range(4):
            @pl.when(t != 4 * c + j)
            def _(e=e, j=j, head=head):
                out_copy(e, j, head).start()
            @pl.when(t == 4 * c + j)
            def _(e=e, j=j, head=head):
                own_copy(e, j, head).start()

    origin = t // 4
    for yy in range(4):
        for core in range(2):
            @pl.when(2 * yy + origin != t)
            def _(yy=yy, core=core):
                out_copy(0, 0, 2 * yy + core).wait_recv()
    for e in range(2):
        for j in range(4):
            @pl.when(t != 4 * c + j)
            def _(e=e, j=j):
                out_copy(e, j, t).wait_send()
            @pl.when(t == 4 * c + j)
            def _(e=e, j=j):
                own_copy(e, j, t).wait()
    lambda_copy().wait_send()
    for kind in range(3):
        for slot, part, lane in RING:
            ring_copy(kind, slot, part, lane).wait_send()
        for slot in range(4):
            mate_copy(kind, slot).wait_send()
    for e in range(2):
        for d in (1, 2, 3):
            for copy in partial_copies(e, d):
                copy.wait_send()


def attention(lambdas, head_gain, queries, key_rows, value_rows):
    any_space = pl.BlockSpec(memory_space=pltpu.HBM)
    bf16, f32 = jnp.bfloat16, jnp.float32
    dma = pltpu.SemaphoreType.DMA
    return pl.pallas_call(
        attention_kernel,
        out_shape=jax.ShapeDtypeStruct((128, 1024), jnp.bfloat16),
        in_specs=[
            any_space, any_space, any_space, any_space, any_space,
        ],
        out_specs=any_space,
        scratch_shapes=[
            pltpu.SMEM((1,), f32),
            pltpu.VMEM((1, 128), f32),
            pltpu.VMEM((BLK, 128), bf16),
            pltpu.VMEM((2, 8, HALF), f32),
            pltpu.VMEM((4, BLK, 128), bf16),
            pltpu.VMEM((4, HALF, 128), bf16),
            pltpu.VMEM((2, 4, BLK, 128), bf16),
            pltpu.VMEM((2, 4, 128, BLK), bf16),
            pltpu.VMEM((2, 4, 2, HALF, 128), bf16),
            pltpu.VMEM((2, 4, 2, 1, HALF), f32),
            pltpu.VMEM((2, 4, 2, VROWS, HALF), f32),
            pltpu.VMEM((2, 4, 2, 128, HALF), bf16),
            pltpu.VMEM((2, 4, 2, 128, HALF), bf16),
            pltpu.VMEM((2, 4, 2, 8, HALF), f32),
            pltpu.VMEM((2, 4, 2, 8, HALF), f32),
            pltpu.VMEM((2, HALF, 128), bf16),
            pltpu.VMEM((BLK, TQ), f32), pltpu.VMEM((BLK, TQ), f32),
            pltpu.VMEM((1, TQ), f32), pltpu.VMEM((1, TQ), f32),
            pltpu.VMEM((1, TQ), f32), pltpu.VMEM((1, TQ), f32),
            dma((5,)),
            dma, dma,
            dma((3, 4, 2)), dma((3, 4, 2)),
            dma((3, 4)), dma((3, 4)),
            dma((2, 4)), dma((2, 4)),
            dma((2, 4)), dma((2, 4)),
            dma((2, 4)), dma((8,)),
        ],
        compiler_params=pltpu.CompilerParams(
            collective_id=0, has_side_effects=True, vmem_limit_bytes=67043328
        ),
        name="attention",
    )(lambdas, head_gain.reshape(1, -1), queries, key_rows, value_rows)


GROUPS = (0, -1, 1, 2)
MAIN = 16
CH = 80
WID = 2048
HW = 1024
AW = 1024
AH = AW // 2
REMA = AW // 4
REM = 512
BAND = WID + REM
NT = 8


def expert_kernel(
    heads_hbm, stream_hbm, gain_hbm, routes_hbm, rw_hbm, ow_hbm, gate_hbm, up_hbm, down_hbm,
    out_ref,
    heads_ref, stream_ref, gain_ref, routes_ref, rw_ref, infos, toks, outb, arrb, ow, gw, uw, dw, att, nrm, outg, arr, reto, ret, xs, act, ps, pr, rh, rf, cm, cr,
    load_sem, isend, irecv, tsend, trecv, obsend, obrecv, xbsend, xbrecv, psend, precv, xsend, xrecv, qsend, qrecv, rsend, rhrecv, rfrecv, bsend, brecv,
):
    s = lax.axis_index("sp")
    t = lax.axis_index("tp")
    z, x = s // NX, s % NX
    y, c = t // 2, t % 2
    mate = 2 * y + 1 - c
    bf16, f32 = jnp.bfloat16, jnp.float32

    def at(dz, dx):
        return ((z + dz + NZ) % NZ) * NX + (x + dx + NX) % NX

    def lane(dy, core):
        return 2 * ((y + dy + 4) % 4) + core

    loads = [
        pltpu.make_async_copy(ow_hbm, ow, load_sem.at[0]),
        pltpu.make_async_copy(gate_hbm.at[0], gw, load_sem.at[1]),
        pltpu.make_async_copy(up_hbm.at[0], uw, load_sem.at[2]),
        pltpu.make_async_copy(down_hbm.at[0], dw, load_sem.at[3]),
    ]
    small = [
        pltpu.make_async_copy(routes_hbm, routes_ref, load_sem.at[4]),
        pltpu.make_async_copy(rw_hbm, rw_ref, load_sem.at[5]),
        pltpu.make_async_copy(stream_hbm, stream_ref, load_sem.at[6]),
        pltpu.make_async_copy(gain_hbm, gain_ref, load_sem.at[7]),
        pltpu.make_async_copy(heads_hbm, heads_ref, load_sem.at[8]),
    ]
    for load in small + loads:
        load.start()

    barrier = pltpu.get_barrier_semaphore()
    others = [(dz, dx) for dz in GROUPS for dx in (0, 1, -1, 2) if (dz, dx) != (0, 0)]
    for dz, dx in others:
        pl.semaphore_signal(barrier, inc=1, device_id=(at(dz, dx), t), device_id_type=MESH)
    for peer in (lane(1, c), lane(-1, c), lane(2, c), mate):
        pl.semaphore_signal(barrier, inc=1, device_id=(s, peer), device_id_type=MESH)

    for load in small + loads[:1]:
        load.wait()
    heads = heads_ref[...]
    square = jnp.zeros((128, 1), f32)
    for k in range(0, WID, 512):
        cols = pl.ds(k, 512)
        value = stream_ref[:, cols].astype(f32) + jnp.dot(heads, ow[:, cols], preferred_element_type=f32)
        att[:, cols] = value
        square = square + jnp.sum(value * value, axis=1, keepdims=True)
    inverse = lax.rsqrt(square * (1.0 / WID) + 1e-06)
    for k in range(0, WID, 512):
        cols = pl.ds(k, 512)
        value = (att[:, cols] * inverse * gain_ref[:, cols]).astype(bf16)
        if k < AW:
            nrm[:, cols] = value
        else:
            toks[y, :, pl.ds(k - AW, 512)] = value

    route = [routes_ref[pl.ds(k, 1), :].astype(f32) for k in range(2)]
    infos[y] = jnp.concatenate(route + [jnp.zeros((6, 128), f32)], axis=0)

    def token_copies(d):
        return [
            pltpu.make_async_remote_copy(
                src_ref=infos.at[y], dst_ref=infos.at[y], send_sem=isend.at[d], recv_sem=irecv.at[d],
                device_id=(s, lane(d, c)), device_id_type=MESH,
            ),
            pltpu.make_async_remote_copy(
                src_ref=toks.at[y], dst_ref=toks.at[y], send_sem=tsend.at[d], recv_sem=trecv.at[d],
                device_id=(s, lane(d, c)), device_id_type=MESH,
            ),
        ]

    pl.semaphore_wait(barrier, len(others) + 4)
    for d in (1, 3, 2):
        for copy in token_copies(d):
            copy.start()

    experts = lax.broadcasted_iota(jnp.int32, (16, 128), 0).astype(f32)
    row_id = lax.broadcasted_iota(jnp.int32, (128, 128), 0)
    col_id = lax.broadcasted_iota(jnp.int32, (128, 128), 1)
    earlier = (row_id < col_id).astype(f32).astype(bf16)
    place = lax.broadcasted_iota(jnp.int32, (256, 128), 0).astype(f32)

    def hits(routes_of, parts):
        hot = [(r == experts).astype(f32) for r in routes_of]
        before = jnp.dot((hot[0] + hot[1]).astype(bf16), earlier, preferred_element_type=f32)
        main, rem = [], []
        for k in range(2):
            slot = jnp.sum(before * hot[k], axis=0, keepdims=True)
            base = routes_of[k] * 16.0 + slot
            low = slot < float(MAIN)
            main.append((jnp.where(low, base, -1.0) == place).astype(f32))
            rem.append([
                (jnp.where(low, -1.0, base + (4.0 * j - 16.0)) == place).astype(f32) for j in parts
            ])
        return main, rem

    main_hit, rem_hit = hits(route, range(4))
    weight = [rw_ref[pl.ds(k, 1), :] for k in range(2)]
    over_rows = (((0,), (0,)), ((), ()))
    chosen = (main_hit[0] + main_hit[1]).astype(bf16)
    for k in range(0, AW, 512):
        cols = pl.ds(k, 512)
        outg[:, cols] = jnp.dot(chosen, nrm[:, cols], preferred_element_type=f32).astype(bf16)
    extra = jnp.zeros((256, REMA), f32)
    for j in range(4):
        extra = extra + jnp.dot(
            (rem_hit[0][j] + rem_hit[1][j]).astype(bf16), nrm[:, pl.ds(j * REMA, REMA)],
            preferred_element_type=f32,
        )
    outg[:, pl.ds(AW, REMA)] = extra.astype(bf16)

    def keep_split(ref, value):
        high = value.astype(bf16)
        ref[pl.ds(0, 256), :] = high
        ref[pl.ds(256, 256), :] = (value - high.astype(f32)).astype(bf16)

    def band(device):
        return pl.ds(pl.multiple_of(device * MAIN, MAIN), MAIN)

    def plane_copy(source, target, ssem, rsem, to, sender):
        return pltpu.make_async_remote_copy(
            src_ref=source.at[band(to), :], dst_ref=target.at[band(sender), :],
            send_sem=ssem.at[to], recv_sem=rsem.at[sender],
            device_id=(to, t), device_id_type=MESH,
        )

    for dz, dx in others:
        plane_copy(outg, arr, psend, precv, at(-dz, -dx), s).start()
    arr[band(s), :] = outg[band(s), :]
    keep_split(cm, weight[0] * main_hit[0] + weight[1] * main_hit[1])
    for j in range(4):
        keep_split(cr.at[j], weight[0] * rem_hit[0][j] + weight[1] * rem_hit[1][j])

    fold_row = lax.broadcasted_iota(jnp.int32, (16, 64), 0)
    fold_col = lax.broadcasted_iota(jnp.int32, (16, 64), 1)
    fold = [
        (fold_col == 16 * (fold_row >> 2) + 4 * j + (fold_row & 3)).astype(f32).astype(bf16)
        for j in range(4)
    ]

    def rows_of(position):
        return pl.ds(pl.multiple_of(position * CH, 16), CH)

    def x_copy(g, position, part, send, to, slot=None):
        cols = pl.ds(0, AW) if part == 2 else pl.ds(part * AH, AH)
        return pltpu.make_async_remote_copy(
            src_ref=xs.at[g, rows_of(position), cols], dst_ref=xs.at[g, rows_of(position), cols],
            send_sem=xsend.at[g, send], recv_sem=xrecv.at[g, position, part % 2],
            device_id=(s, to), device_id_type=MESH,
        )

    def x_sends(g):
        return [
            (g, t, 2, 0, lane(1, c)), (g, t, 2, 1, lane(-1, c)), (g, t, 2, 2, mate),
            (g, lane(-1, c), 0, 3, lane(1, c)), (g, lane(-1, c), 2, 4, mate),
            (g, lane(1, c), 1, 5, lane(-1, c)), (g, lane(1, c), 2, 6, mate),
            (g, lane(2, c), 2, 7, mate),
        ]

    def group_rows(g):
        zz = (z + GROUPS[g] + NZ) % NZ
        return pl.ds(pl.multiple_of(zz * 64, 64), 64)

    def build(g):
        for dx in (0, 1, -1, 2):
            if (GROUPS[g], dx) != (0, 0):
                plane_copy(outg, arr, psend, precv, s, at(GROUPS[g], dx)).wait_recv()
        rows = group_rows(g)
        first = pl.multiple_of(t * CH, 16)
        for k in range(0, AW, 512):
            xs[g, pl.ds(first, 64), pl.ds(k, 512)] = arr[rows, pl.ds(k, 512)]
        for j in range(4):
            xs[g, pl.ds(first + 64, 16), pl.ds(j * REMA, REMA)] = jnp.dot(
                fold[j], arr[rows, pl.ds(AW, REMA)], preferred_element_type=f32
            ).astype(bf16)
        for copy in x_sends(g)[:3]:
            x_copy(*copy).start()

    def forward(g):
        todo = x_sends(g)
        x_copy(g, lane(-1, c), 2, 0, t).wait_recv()
        x_copy(*todo[3]).start()
        x_copy(*todo[4]).start()
        x_copy(g, lane(1, c), 2, 0, t).wait_recv()
        x_copy(*todo[5]).start()
        x_copy(*todo[6]).start()

    def far(g):
        x_copy(g, lane(2, c), 0, 0, t).wait_recv()
        x_copy(g, lane(2, c), 1, 0, t).wait_recv()
        x_copy(*x_sends(g)[7]).start()

    def slot_copy(to, sender):
        return pltpu.make_async_remote_copy(
            src_ref=outb.at[to], dst_ref=arrb.at[sender],
            send_sem=obsend.at[to], recv_sem=obrecv.at[sender],
            device_id=(to, t), device_id_type=MESH,
        )

    def spread(_):
        for d in (1, 3, 2):
            for copy in token_copies(d):
                copy.wait_recv()
        mains, rems = [], []
        for yy in range(4):
            main, rem = hits([infos[yy, pl.ds(k, 1), :] for k in range(2)], (yy,))
            mains.append((main[0] + main[1]).astype(bf16))
            rems.append((rem[0][0] + rem[1][0]).astype(bf16))
        rems = jnp.concatenate(rems, axis=1)
        for k in range(0, WID - AW, 512):
            cols = pl.ds(k, 512)
            for yy in range(4):
                value = jnp.dot(mains[yy], toks[yy, :, cols], preferred_element_type=f32)
                outb[:, pl.ds(16 * yy, 16), cols] = value.astype(bf16).reshape(16, 16, 512)
            every = jnp.concatenate([toks[yy, :, cols] for yy in range(4)], axis=0)
            value = jnp.dot(rems, every, preferred_element_type=f32)
            outb[:, pl.ds(64, 16), cols] = value.astype(bf16).reshape(16, 16, 512)
        for dz, dx in others:
            slot_copy(at(-dz, -dx), s).start()
        arrb[s] = outb[s]

    move_row = lax.broadcasted_iota(jnp.int32, (64, 64), 0)
    move_col = lax.broadcasted_iota(jnp.int32, (64, 64), 1)
    move = (
        move_col == 16 * ((move_row >> 2) & 3) + 4 * (move_row >> 4) + (move_row & 3)
    ).astype(f32).astype(bf16)

    def far_copy(g, yy, core):
        cols = pl.ds(AW, WID - AW)
        return pltpu.make_async_remote_copy(
            src_ref=xs.at[g, rows_of(2 * yy + core), cols], dst_ref=xs.at[g, rows_of(2 * yy + core), cols],
            send_sem=xbsend.at[g, yy], recv_sem=xbrecv.at[g, yy],
            device_id=(s, mate), device_id_type=MESH,
        )

    def gather(g):
        for dx in (0, 1, -1, 2):
            if (GROUPS[g], dx) != (0, 0):
                slot_copy(s, at(GROUPS[g], dx)).wait_recv()
        first = ((z + GROUPS[g] + NZ) % NZ) * NX
        moved = []
        for k in range(0, WID - AW, 512):
            cols = pl.ds(k, 512)
            tails = jnp.concatenate([arrb[first + xx, pl.ds(64, 16), cols] for xx in range(4)], axis=0)
            moved.append(jnp.dot(move, tails, preferred_element_type=f32).astype(bf16))
        for yy in range(4):
            row = pl.multiple_of((2 * yy + c) * CH, 16)
            for i, k in enumerate(range(0, WID - AW, 512)):
                into = pl.ds(AW + k, 512)
                for xx in range(4):
                    xs[g, pl.ds(row + 16 * xx, 16), into] = arrb[
                        first + xx, pl.ds(16 * yy, 16), pl.ds(k, 512)
                    ]
                xs[g, pl.ds(row + 64, 16), into] = moved[i][16 * yy:16 * yy + 16]
            far_copy(g, yy, c).start()

    def pair_copy(g, yy):
        return pltpu.make_async_remote_copy(
            src_ref=ps.at[g, rows_of(2 * yy + 1 - c), :], dst_ref=pr.at[g, yy],
            send_sem=qsend.at[g, yy], recv_sem=qrecv.at[g, yy],
            device_id=(s, mate), device_id_type=MESH,
        )

    TURN = (2, 1, 3, 0)

    def compute(g):
        for dy in (0, -1, 1, 2):
            x_copy(g, lane(dy, 1 - c), 2, 0, t).wait_recv()
        for yy in range(4):
            far_copy(g, yy, 1 - c).wait_recv()
        if g == 0:
            for load in loads[1:]:
                load.wait()

        def block(i, carry):
            dy = jnp.where(i == 0, 2, jnp.where(i == 1, 1, jnp.where(i == 2, 3, 0)))
            yy = (y + dy) % 4
            rows = pl.ds(pl.multiple_of(yy * 2 * CH, 32), 2 * CH)
            value = xs[g, rows, :]
            gate = jnp.dot(value, gw[...], preferred_element_type=f32)
            upper = jnp.dot(value, uw[...], preferred_element_type=f32)
            act[...] = (gate / (1.0 + jnp.exp(-gate)) * upper).astype(bf16)
            ps[g, rows, :] = jnp.dot(act[...], dw[...], preferred_element_type=f32).astype(bf16)
            pair_copy(g, yy).start()
            return carry

        lax.fori_loop(0, 4, block, 0)

    def add_into(g, position, cols, terms):
        rows = rows_of(position)
        total = ps[g, rows, cols].astype(f32)
        for term in terms:
            total = total + term.astype(f32)
        ps[g, rows, cols] = total.astype(bf16)

    def r_copy(g, dy, part, send, direction, ref, sem, slot):
        cols = pl.ds(part * HW, HW)
        return pltpu.make_async_remote_copy(
            src_ref=ps.at[g, rows_of(lane(dy, c)), cols], dst_ref=ref.at[(g,) + slot],
            send_sem=rsend.at[g, send], recv_sem=sem.at[(g,) + slot],
            device_id=(s, lane(direction, c)), device_id_type=MESH,
        )

    def r_sends(g):
        return [
            (g, 2, 0, 0, 1, rh, rhrecv, (0,)), (g, 2, 1, 1, -1, rh, rhrecv, (1,)),
            (g, 1, 1, 2, 1, rf, rfrecv, (0, 1)), (g, -1, 0, 3, -1, rf, rfrecv, (1, 0)),
            (g, 1, 0, 4, 1, rf, rfrecv, (0, 0)), (g, -1, 1, 5, -1, rf, rfrecv, (1, 1)),
        ]

    def pair(g):
        todo = r_sends(g)
        for turn, dy in enumerate(TURN):
            yy = (y + dy) % 4
            pair_copy(g, yy).wait_recv()
            for k in range(2):
                cols = pl.ds(k * HW, HW)
                add_into(g, 2 * yy + c, cols, [pr[g, yy, :, cols]])
            if turn == 0:
                r_copy(*todo[0]).start()
                r_copy(*todo[1]).start()
            if turn == 1:
                r_copy(*todo[2]).start()
            if turn == 2:
                r_copy(*todo[3]).start()

    def middle(g):
        todo = r_sends(g)
        r_copy(*todo[0]).wait_recv()
        add_into(g, lane(1, c), pl.ds(0, HW), [rh[g, 0]])
        r_copy(*todo[4]).start()
        r_copy(*todo[1]).wait_recv()
        add_into(g, lane(-1, c), pl.ds(HW, HW), [rh[g, 1]])
        r_copy(*todo[5]).start()

    def finish(g):
        todo = r_sends(g)
        for k in range(2, 6):
            r_copy(*todo[k]).wait_recv()
        rows = group_rows(g)
        own = pl.multiple_of(t * CH, 16)
        extra = jnp.zeros((64, REM), f32)
        for j in range(4):
            cols = pl.ds(j * REM, REM)
            inner = pl.ds((j % 2) * REM, REM)
            total = (
                ps[g, pl.ds(own, CH), cols].astype(f32)
                + rf[g, 0, j // 2, :, inner].astype(f32)
                + rf[g, 1, j // 2, :, inner].astype(f32)
            ).astype(bf16)
            reto[rows, cols] = total[:64]
            extra = extra + lax.dot_general(fold[j], total[64:], over_rows, preferred_element_type=f32)
        reto[rows, pl.ds(WID, REM)] = extra.astype(bf16)
        for dx in (0, 1, -1, 2):
            to = at(GROUPS[g], dx)
            if (GROUPS[g], dx) == (0, 0):
                ret[band(s), :] = reto[band(s), :]
            else:
                plane_copy(reto, ret, bsend, brecv, to, s).start()

    for stage, g in (
        (build, 0), (build, 1), (spread, 0), (forward, 0), (build, 2), (forward, 1), (build, 3),
        (far, 0), (gather, 0), (compute, 0), (pair, 0),
        (forward, 2), (far, 1), (gather, 1), (compute, 1), (pair, 1), (middle, 0),
        (forward, 3), (far, 2), (gather, 2), (compute, 2), (pair, 2), (finish, 0), (middle, 1),
        (far, 3), (gather, 3), (compute, 3), (pair, 3), (middle, 2), (finish, 1), (middle, 3),
        (finish, 2), (finish, 3),
    ):
        stage(g)

    for dz, dx in others:
        plane_copy(reto, ret, bsend, brecv, s, at(dz, dx)).wait_recv()
    for j in range(4):
        cols = pl.ds(j * REM, REM)
        back = ret[:, cols]
        tail = ret[:, pl.ds(WID, REM)]
        routed = lax.dot_general(
            cm[...], jnp.concatenate([back, back], axis=0), over_rows, preferred_element_type=f32
        ) + lax.dot_general(
            cr[j], jnp.concatenate([tail, tail], axis=0), over_rows, preferred_element_type=f32
        )
        out_ref[:, cols] = (att[:, cols] + routed).astype(bf16)

    for dz, dx in others:
        plane_copy(outg, arr, psend, precv, at(dz, dx), s).wait_send()
        plane_copy(reto, ret, bsend, brecv, at(dz, dx), s).wait_send()
        slot_copy(at(dz, dx), s).wait_send()
    for d in (1, 2, 3):
        for copy in token_copies(d):
            copy.wait_send()
    for g in range(4):
        for copy in x_sends(g):
            x_copy(*copy).wait_send()
        for yy in range(4):
            pair_copy(g, yy).wait_send()
            far_copy(g, yy, c).wait_send()
        for copy in r_sends(g):
            r_copy(*copy).wait_send()


def routed_experts(
    heads, stream, ffn_gain, routes, route_weight, out_weight, gate_weight, up_weight, down_weight
):
    any_space = pl.BlockSpec(memory_space=pltpu.HBM)
    vmem = pl.BlockSpec(memory_space=pltpu.VMEM)
    bf16, f32 = jnp.bfloat16, jnp.float32
    dma = pltpu.SemaphoreType.DMA
    return pl.pallas_call(
        expert_kernel,
        out_shape=jax.ShapeDtypeStruct((128, WID), bf16),
        in_specs=[any_space] * 9,
        out_specs=vmem,
        scratch_shapes=[
            pltpu.VMEM((128, 1024), bf16),
            pltpu.VMEM((128, WID), bf16),
            pltpu.VMEM((1, WID), f32),
            pltpu.VMEM((2, 128), jnp.int32),
            pltpu.VMEM((2, 128), f32),
            pltpu.VMEM((4, 8, 128), f32),
            pltpu.VMEM((4, 128, WID - AW), bf16),
            pltpu.VMEM((16, CH, WID - AW), bf16),
            pltpu.VMEM((16, CH, WID - AW), bf16),
            pltpu.VMEM((1024, WID), bf16),
            pltpu.VMEM((WID, 640), bf16),
            pltpu.VMEM((WID, 640), bf16),
            pltpu.VMEM((640, WID), bf16),
            pltpu.VMEM((128, WID), f32),
            pltpu.VMEM((128, AW), bf16),
            pltpu.VMEM((256, AW + REMA), bf16),
            pltpu.VMEM((256, AW + REMA), bf16),
            pltpu.VMEM((256, BAND), bf16),
            pltpu.VMEM((256, BAND), bf16),
            pltpu.VMEM((4, NT * CH, WID), bf16),
            pltpu.VMEM((2 * CH, 640), bf16),
            pltpu.VMEM((4, NT * CH, WID), bf16),
            pltpu.VMEM((4, 4, CH, WID), bf16),
            pltpu.VMEM((4, 2, CH, HW), bf16),
            pltpu.VMEM((4, 2, 2, CH, HW), bf16),
            pltpu.VMEM((512, 128), bf16),
            pltpu.VMEM((4, 512, 128), bf16),
            dma((9,)),
            dma((4,)), dma((4,)), dma((4,)), dma((4,)),
            dma((16,)), dma((16,)), dma((4, 4)), dma((4, 4)),
            dma((16,)), dma((16,)),
            dma((4, 8)), dma((4, 8, 2)),
            dma((4, 4)), dma((4, 4)),
            dma((4, 6)), dma((4, 2)), dma((4, 2, 2)),
            dma((16,)), dma((16,)),
        ],
        compiler_params=pltpu.CompilerParams(
            collective_id=1, has_side_effects=True, vmem_limit_bytes=67043328
        ),
        name="experts",
    )(
        heads, stream, ffn_gain.reshape(1, -1), routes.T, route_weight.T,
        out_weight, gate_weight, up_weight, down_weight,
    )


def local(
    queries,
    key_rows,
    value_rows,
    lambdas,
    head_gain,
    out_weight,
    stream,
    ffn_gain,
    routes,
    route_weight,
    gate_weight,
    up_weight,
    down_weight,
):
    heads_local = attention(lambdas, head_gain, queries, key_rows, value_rows)
    return routed_experts(
        heads_local, stream, ffn_gain, routes, route_weight,
        out_weight, gate_weight, up_weight, down_weight,
    )


def solution(mesh):
    placed = (
        P("sp", "tp"),
        P("sp", "tp"),
        P("sp", "tp"),
        P("tp"),
        P(),
        P(),
        P(("sp", "tp"), None),
        P(),
        P(("sp", "tp"), None),
        P(("sp", "tp"), None),
        P("sp", None, "tp"),
        P("sp", None, "tp"),
        P("sp", "tp", None),
    )
    return jax.shard_map(
        local, mesh=mesh, in_specs=placed, out_specs=P(("sp", "tp"), None), check_vma=False
    )
```

```python
import functools

import jax
import jax.numpy as jnp
from jax import lax
from jax.experimental import pallas as pl
from jax.experimental.pallas import tpu as pltpu
from jax.sharding import PartitionSpec as P

DH = 64


LOG2E = 1.4426950408889634
MESH = pl.DeviceIdType.MESH
NZ = 4
NX = 4
BLK = 1024
HALF = 512
NEG = -1e30
VROWS = 144
TQ = 512
KB = 512
WORK = (
    (0, 0), (3, 0), (1, 0), (3, 3), (3, 1), (1, 3), (1, 1), (3, 2), (1, 2),
    (2, 0), (2, 3), (2, 1), (2, 2), (0, 3), (0, 1), (0, 2),
)


def attention_kernel(
    lam_hbm, gain_hbm, q_hbm, k_hbm, v_hbm, out_ref,
    lam_ref, gain_ref, vin, lamv, qfull, qother, kb, vb, qm, mx, acc, pout, pin, sout, sin, obuf, sbuf0, sbuf1, fbuf0, fbuf1, nbuf0, nbuf1,
    load_sem, lsend, lrecv, send_sem, recv_sem, msend, mrecv, psend, precv, ssend, srecv, osend, orecv,
):
    sp = lax.axis_index("sp")
    t = lax.axis_index("tp")
    z, x = sp // NX, sp % NX
    y, c = t // 2, t % 2
    mate = 2 * y + 1 - c
    f32, bf16 = jnp.float32, jnp.bfloat16
    sbuf, fbuf, nbuf = (sbuf0, sbuf1), (fbuf0, fbuf1), (nbuf0, nbuf1)

    def at(dz, dx):
        return ((z + dz + NZ) % NZ) * NX + (x + dx + NX) % NX

    loads = [
        pltpu.make_async_copy(q_hbm, qfull.at[0], load_sem.at[0]),
        pltpu.make_async_copy(k_hbm, kb.at[0, 0], load_sem.at[1]),
        pltpu.make_async_copy(v_hbm, vin, load_sem.at[2]),
    ]
    small = [
        pltpu.make_async_copy(lam_hbm, lam_ref, load_sem.at[3]),
        pltpu.make_async_copy(gain_hbm, gain_ref, load_sem.at[4]),
    ]
    for load in loads + small:
        load.start()

    barrier = pltpu.get_barrier_semaphore()
    for dz, dx in ((0, 1), (0, -1), (1, 0), (-1, 0), (2, 0), (0, 2)):
        pl.semaphore_signal(barrier, inc=1, device_id=(at(dz, dx), t), device_id_type=MESH)
    for j in range(1, 8):
        pl.semaphore_signal(barrier, inc=1, device_id=(sp, (t + j) % 8), device_id_type=MESH)

    def along(e, queries, d):
        own = c if e == 0 else 1 - c
        first = at(d, 0) if queries else at(0, d)
        second = at(0, d) if queries else at(d, 0)
        return jnp.where(own == 0, first, second)

    def piece(kind, slot, part):
        span = pl.ds(0, BLK) if part == 2 else pl.ds(part * HALF, HALF)
        if kind == 0:
            return qfull.at[slot, span, :]
        if kind == 1:
            return kb.at[0, slot, span, :]
        return vb.at[0, slot, :, span]

    def ring_copy(kind, slot, part, lane):
        d = 1 if lane == 0 else -1
        return pltpu.make_async_remote_copy(
            src_ref=piece(kind, slot, part), dst_ref=piece(kind, (slot - d) % 4, part),
            send_sem=send_sem.at[kind, slot, lane],
            recv_sem=recv_sem.at[kind, (slot - d) % 4, part % 2],
            device_id=(along(0, kind == 0, d), t), device_id_type=MESH,
        )

    RING = ((0, 2, 0), (0, 2, 1), (3, 0, 0), (1, 1, 1))

    def ring_wait(kind, slot):
        for part in (0, 1) if slot == 2 else (2,):
            pltpu.make_async_remote_copy(
                src_ref=piece(kind, slot, part), dst_ref=piece(kind, slot, part),
                send_sem=send_sem.at[kind, 0, 0], recv_sem=recv_sem.at[kind, slot, part % 2],
                device_id=(sp, mate), device_id_type=MESH,
            ).wait_recv()

    def mate_copy(kind, slot):
        if kind == 0:
            source = qfull.at[slot, pl.ds(pl.multiple_of((1 - c) * HALF, HALF), HALF), :]
            target = qother.at[slot]
        elif kind == 1:
            source, target = kb.at[0, slot], kb.at[1, slot]
        else:
            source, target = vb.at[0, slot], vb.at[1, slot]
        return pltpu.make_async_remote_copy(
            src_ref=source, dst_ref=target,
            send_sem=msend.at[kind, slot], recv_sem=mrecv.at[kind, slot],
            device_id=(sp, mate), device_id_type=MESH,
        )

    def lambda_copy():
        return pltpu.make_async_remote_copy(
            src_ref=lamv.at[0], dst_ref=lamv.at[1], send_sem=lsend, recv_sem=lrecv,
            device_id=(sp, mate), device_id_type=MESH,
        )

    lane_ids = lax.broadcasted_iota(jnp.int32, (HALF, 2 * DH), 1)

    def split_maps(e, slot):
        if e == 0:
            q = qfull[slot, pl.ds(pl.multiple_of(c * HALF, HALF), HALF), :]
        else:
            q = qother[slot]
        zero = jnp.zeros_like(q)
        qm[e, slot, 0] = jnp.where(lane_ids < DH, q, zero)
        qm[e, slot, 1] = jnp.where(lane_ids < DH, zero, q)

    def arrive(kind, slot):
        ring_wait(kind, slot)
        if slot == 3:
            ring_copy(kind, 3, 0, 0).start()
        if slot == 1:
            ring_copy(kind, 1, 1, 1).start()
        mate_copy(kind, slot).start()

    def settle(kind, slot):
        mate_copy(kind, slot).wait_recv()
        if kind == 0:
            split_maps(0, slot)
            split_maps(1, slot)

    for load in loads + small:
        load.wait()
    lamv[0] = jnp.full((8, HALF), lam_ref[0], f32)
    pl.semaphore_wait(barrier, 13)
    for kind in (0, 1):
        for lane in range(2):
            ring_copy(kind, 0, 2, lane).start()
    mate_copy(1, 0).start()
    mate_copy(0, 0).start()
    lambda_copy().start()
    for k in range(4):
        span = pl.ds(k * 256, 256)
        vb[0, 0, :, span] = vin[span, :].astype(f32).T.astype(bf16)
    for lane in range(2):
        ring_copy(2, 0, 2, lane).start()
    mate_copy(2, 0).start()

    mx[...] = jnp.full(mx.shape, NEG, f32)
    acc[...] = jnp.zeros(acc.shape, f32)

    scale = LOG2E * DH ** (-0.5)

    always = sp >= 0

    def tiles(e, di, dk, masked):
        chunks = [(m, r) for m in range(2) for r in range(HALF // TQ)]

        def phase(now, later):
            tops, pv = [], None
            for kk in range(BLK // KB):
                keys = pl.ds(kk * KB, KB)
                if later is not None:
                    m, r = chunks[later]
                    scores = lax.dot_general(
                        kb[e, dk, keys, :], qm[e, di, m, pl.ds(r * TQ, TQ), :],
                        (((1,), (1,)), ((), ())), preferred_element_type=f32,
                    ) * scale
                    if masked:
                        key_id = lax.broadcasted_iota(jnp.int32, scores.shape, 0) + kk * KB
                        query_id = lax.broadcasted_iota(jnp.int32, scores.shape, 1) + (c * HALF + r * TQ)
                        scores = jnp.where(key_id <= query_id, scores, NEG)
                    sbuf[later % 2][keys, :] = scores
                    tops.append(jnp.max(scores, axis=0, keepdims=True))
                if now is not None:
                    m, r = chunks[now]
                    values = jnp.concatenate(
                        [vb[e, dk, :, keys], jnp.ones((VROWS - 128, KB), bf16)], axis=0
                    )
                    weights = jnp.exp2(sbuf[now % 2][keys, :] - nbuf[now % 2][...]).astype(bf16)
                    term = jnp.dot(values, weights, preferred_element_type=f32)
                    pv = term if pv is None else pv + term
            if now is not None:
                m, r = chunks[now]
                cols = pl.ds(r * TQ, TQ)
                acc[e, di, m, :, cols] = acc[e, di, m, :, cols] * fbuf[now % 2][...] + pv
            if later is not None:
                m, r = chunks[later]
                cols = pl.ds(r * TQ, TQ)
                old = mx[e, di, m, :, cols]
                new = functools.reduce(jnp.maximum, tops, old)
                fbuf[later % 2][...] = jnp.exp2(old - new)
                nbuf[later % 2][...] = new
                mx[e, di, m, :, cols] = new

        phase(None, 0)
        for n in range(len(chunks)):
            @pl.when(always)
            def _(n=n):
                phase(n, n + 1 if n + 1 < len(chunks) else None)

    def partial_copies(e, d):
        to = along(e, True, d)
        slot = (4 - d) % 4
        return [
            pltpu.make_async_remote_copy(
                src_ref=pout.at[e, d], dst_ref=pin.at[e, slot],
                send_sem=psend.at[e, d], recv_sem=precv.at[e, slot],
                device_id=(to, t), device_id_type=MESH,
            ),
            pltpu.make_async_remote_copy(
                src_ref=sout.at[e, d], dst_ref=sin.at[e, slot],
                send_sem=ssend.at[e, d], recv_sem=srecv.at[e, slot],
                device_id=(to, t), device_id_type=MESH,
            ),
        ]

    def normal(e, d, m):
        total = acc[e, d, m, pl.ds(128, 1), :]
        some = total > 0.0
        safe = jnp.where(some, total, 1.0)
        level = jnp.where(some, mx[e, d, m] + jnp.log2(safe), NEG)
        return acc[e, d, m, pl.ds(0, 128), :] * (1.0 / safe), level

    def send_partial(d):
        for e in range(2):
            for m in range(2):
                value, level = normal(e, d, m)
                pout[e, d, m] = value.astype(bf16)
                sout[e, d, m] = jnp.broadcast_to(level, (8, HALF))
            for copy in partial_copies(e, d):
                copy.start()

    def before(n):
        if n == 0:
            for kind in (1, 0, 2):
                settle(kind, 0)
        if n == 1:
            for kind in (0, 1):
                for slot in (3, 1):
                    arrive(kind, slot)
            for slot in (3, 1):
                settle(0, slot)
        if n == 3:
            for slot in (3, 1):
                arrive(2, slot)
            for kind in (1, 2):
                for slot in (3, 1):
                    settle(kind, slot)
        if n == 6:
            for kind in range(3):
                arrive(kind, 2)
            for kind in range(3):
                settle(kind, 2)
        if n == 8:
            send_partial(3)
        if n == 9:
            send_partial(1)
        if n == 13:
            send_partial(2)

    def step(n, carry):
        for k in (0, 1, 3, 6, 8, 9, 13):
            @pl.when(n == k)
            def _(k=k):
                before(k)

        di = jnp.int32(0)
        dk = jnp.int32(0)
        for k, (a, b) in enumerate(WORK):
            di = jnp.where(n == k, a, di)
            dk = jnp.where(n == k, b, dk)

        def one_head(e, inner):
            head = jnp.where(e == 0, c, 1 - c)
            query_block = jnp.where(head == 0, at(di, 0), at(0, di))
            key_block = jnp.where(head == 0, at(0, dk), at(dk, 0))

            @pl.when(key_block < query_block)
            def _():
                tiles(e, di, dk, False)

            @pl.when(key_block == query_block)
            def _():
                tiles(e, di, dk, True)

            return inner

        return lax.fori_loop(0, 2, one_head, carry)

    lax.fori_loop(0, len(WORK), step, 0)

    def out_copy(e, j, sender):
        cols = pl.ds(pl.multiple_of(sender * 128, 128), 128)
        return pltpu.make_async_remote_copy(
            src_ref=obuf.at[e, pl.ds(j * 128, 128), :], dst_ref=out_ref.at[:, cols],
            send_sem=osend.at[e, j], recv_sem=orecv.at[sender],
            device_id=(sp, 4 * c + j), device_id_type=MESH,
        )

    def own_copy(e, j, head):
        cols = pl.ds(pl.multiple_of(head * 128, 128), 128)
        return pltpu.make_async_copy(
            obuf.at[e, pl.ds(j * 128, 128), :], out_ref.at[:, cols], osend.at[e, j]
        )

    lambda_copy().wait_recv()
    for e in range(2):
        head = t if e == 0 else mate
        for slot in (1, 3, 2):
            pltpu.make_async_remote_copy(
                src_ref=pout.at[e, slot], dst_ref=pin.at[e, slot],
                send_sem=psend.at[e, slot], recv_sem=precv.at[e, slot],
                device_id=(sp, mate), device_id_type=MESH,
            ).wait_recv()
            pltpu.make_async_remote_copy(
                src_ref=sout.at[e, slot], dst_ref=sin.at[e, slot],
                send_sem=ssend.at[e, slot], recv_sem=srecv.at[e, slot],
                device_id=(sp, mate), device_id_type=MESH,
            ).wait_recv()
        mixed = []
        for m in range(2):
            value, level = normal(e, 0, m)
            levels = [level] + [sin[e, slot, m, pl.ds(0, 1), :] for slot in (1, 2, 3)]
            top = jnp.maximum(jnp.maximum(levels[0], levels[1]), jnp.maximum(levels[2], levels[3]))
            share = [jnp.exp2(item - top) for item in levels]
            inverse = 1.0 / (share[0] + share[1] + share[2] + share[3])
            total = value * (share[0] * inverse)
            for slot in (1, 2, 3):
                total = total + pin[e, slot, m].astype(f32) * (share[slot] * inverse)
            mixed.append(total)
        contrast = mixed[0] - lamv[e, pl.ds(0, 1), :] * mixed[1]
        mean = jnp.mean(contrast * contrast, axis=0, keepdims=True)
        contrast = contrast * lax.rsqrt(mean + 1e-05)
        for j in range(4):
            rows = contrast[:, j * 128:(j + 1) * 128].T * gain_ref[...]
            obuf[e, pl.ds(j * 128, 128), :] = rows.astype(bf16)
        for j in range(4):
            @pl.when(t != 4 * c + j)
            def _(e=e, j=j, head=head):
                out_copy(e, j, head).start()
            @pl.when(t == 4 * c + j)
            def _(e=e, j=j, head=head):
                own_copy(e, j, head).start()

    origin = t // 4
    for yy in range(4):
        for core in range(2):
            @pl.when(2 * yy + origin != t)
            def _(yy=yy, core=core):
                out_copy(0, 0, 2 * yy + core).wait_recv()
    for e in range(2):
        for j in range(4):
            @pl.when(t != 4 * c + j)
            def _(e=e, j=j):
                out_copy(e, j, t).wait_send()
            @pl.when(t == 4 * c + j)
            def _(e=e, j=j):
                own_copy(e, j, t).wait()
    lambda_copy().wait_send()
    for kind in range(3):
        for slot, part, lane in RING:
            ring_copy(kind, slot, part, lane).wait_send()
        for slot in range(4):
            mate_copy(kind, slot).wait_send()
    for e in range(2):
        for d in (1, 2, 3):
            for copy in partial_copies(e, d):
                copy.wait_send()


def attention(lambdas, head_gain, queries, key_rows, value_rows):
    any_space = pl.BlockSpec(memory_space=pltpu.HBM)
    bf16, f32 = jnp.bfloat16, jnp.float32
    dma = pltpu.SemaphoreType.DMA
    return pl.pallas_call(
        attention_kernel,
        out_shape=jax.ShapeDtypeStruct((128, 1024), jnp.bfloat16),
        in_specs=[
            any_space, any_space, any_space, any_space, any_space,
        ],
        out_specs=any_space,
        scratch_shapes=[
            pltpu.SMEM((1,), f32),
            pltpu.VMEM((1, 128), f32),
            pltpu.VMEM((BLK, 128), bf16),
            pltpu.VMEM((2, 8, HALF), f32),
            pltpu.VMEM((4, BLK, 128), bf16),
            pltpu.VMEM((4, HALF, 128), bf16),
            pltpu.VMEM((2, 4, BLK, 128), bf16),
            pltpu.VMEM((2, 4, 128, BLK), bf16),
            pltpu.VMEM((2, 4, 2, HALF, 128), bf16),
            pltpu.VMEM((2, 4, 2, 1, HALF), f32),
            pltpu.VMEM((2, 4, 2, VROWS, HALF), f32),
            pltpu.VMEM((2, 4, 2, 128, HALF), bf16),
            pltpu.VMEM((2, 4, 2, 128, HALF), bf16),
            pltpu.VMEM((2, 4, 2, 8, HALF), f32),
            pltpu.VMEM((2, 4, 2, 8, HALF), f32),
            pltpu.VMEM((2, HALF, 128), bf16),
            pltpu.VMEM((BLK, TQ), f32), pltpu.VMEM((BLK, TQ), f32),
            pltpu.VMEM((1, TQ), f32), pltpu.VMEM((1, TQ), f32),
            pltpu.VMEM((1, TQ), f32), pltpu.VMEM((1, TQ), f32),
            dma((5,)),
            dma, dma,
            dma((3, 4, 2)), dma((3, 4, 2)),
            dma((3, 4)), dma((3, 4)),
            dma((2, 4)), dma((2, 4)),
            dma((2, 4)), dma((2, 4)),
            dma((2, 4)), dma((8,)),
        ],
        compiler_params=pltpu.CompilerParams(
            collective_id=0, has_side_effects=True, vmem_limit_bytes=67043328
        ),
        name="attention",
    )(lambdas, head_gain.reshape(1, -1), queries, key_rows, value_rows)


GROUPS = (1, 2, -1, 0)
MAIN = 16
CH = 80
WID = 2048
HW = 1024
AW = 1536
AH = AW // 2
REMA = AW // 4
REM = 512
BAND = WID + REM
NT = 8


def expert_kernel(
    heads_hbm, stream_hbm, gain_hbm, routes_hbm, rw_hbm, ow_hbm, gate_hbm, up_hbm, down_hbm,
    out_ref,
    heads_ref, stream_ref, gain_ref, routes_ref, rw_ref, infos, toks, outb, arrb, ow, guw, dw, att, nrm, outg, arr, reto, ret, xs, act, ps, pr, rh, rf, cm, cr,
    load_sem, isend, irecv, tsend, trecv, obsend, obrecv, xbsend, xbrecv, psend, precv, xsend, xrecv, qsend, qrecv, rsend, rhrecv, rfrecv, bsend, brecv,
):
    s = lax.axis_index("sp")
    t = lax.axis_index("tp")
    z, x = s // NX, s % NX
    y, c = t // 2, t % 2
    mate = 2 * y + 1 - c
    bf16, f32 = jnp.bfloat16, jnp.float32

    def at(dz, dx):
        return ((z + dz + NZ) % NZ) * NX + (x + dx + NX) % NX

    def lane(dy, core):
        return 2 * ((y + dy + 4) % 4) + core

    loads = [
        pltpu.make_async_copy(ow_hbm, ow, load_sem.at[0]),
        pltpu.make_async_copy(gate_hbm.at[0], guw.at[:, pl.ds(0, 640)], load_sem.at[1]),
        pltpu.make_async_copy(up_hbm.at[0], guw.at[:, pl.ds(640, 640)], load_sem.at[2]),
        pltpu.make_async_copy(down_hbm.at[0], dw, load_sem.at[3]),
    ]
    small = [
        pltpu.make_async_copy(routes_hbm, routes_ref, load_sem.at[4]),
        pltpu.make_async_copy(rw_hbm, rw_ref, load_sem.at[5]),
        pltpu.make_async_copy(stream_hbm, stream_ref, load_sem.at[6]),
        pltpu.make_async_copy(gain_hbm, gain_ref, load_sem.at[7]),
        pltpu.make_async_copy(heads_hbm, heads_ref, load_sem.at[8]),
    ]
    for load in small + loads:
        load.start()

    barrier = pltpu.get_barrier_semaphore()
    others = [(dz, dx) for dz in GROUPS for dx in (0, 1, -1, 2) if (dz, dx) != (0, 0)]
    for dz, dx in others:
        pl.semaphore_signal(barrier, inc=1, device_id=(at(dz, dx), t), device_id_type=MESH)
    for peer in (lane(1, c), lane(-1, c), lane(2, c), mate):
        pl.semaphore_signal(barrier, inc=1, device_id=(s, peer), device_id_type=MESH)

    for load in small + loads[:1]:
        load.wait()
    heads = heads_ref[...]
    square = jnp.zeros((128, 1), f32)
    for k in range(0, WID, 512):
        cols = pl.ds(k, 512)
        value = stream_ref[:, cols].astype(f32) + jnp.dot(heads, ow[:, cols], preferred_element_type=f32)
        att[:, cols] = value
        square = square + jnp.sum(value * value, axis=1, keepdims=True)
    inverse = lax.rsqrt(square * (1.0 / WID) + 1e-06)
    for k in range(0, WID, 512):
        cols = pl.ds(k, 512)
        value = (att[:, cols] * inverse * gain_ref[:, cols]).astype(bf16)
        if k < AW:
            nrm[:, cols] = value
        else:
            toks[y, :, pl.ds(k - AW, 512)] = value

    route = [routes_ref[pl.ds(k, 1), :].astype(f32) for k in range(2)]
    infos[y] = jnp.concatenate(route + [jnp.zeros((6, 128), f32)], axis=0)

    def token_copies(d):
        return [
            pltpu.make_async_remote_copy(
                src_ref=infos.at[y], dst_ref=infos.at[y], send_sem=isend.at[d], recv_sem=irecv.at[d],
                device_id=(s, lane(d, c)), device_id_type=MESH,
            ),
            pltpu.make_async_remote_copy(
                src_ref=toks.at[y], dst_ref=toks.at[y], send_sem=tsend.at[d], recv_sem=trecv.at[d],
                device_id=(s, lane(d, c)), device_id_type=MESH,
            ),
        ]

    pl.semaphore_wait(barrier, len(others) + 4)
    for d in (1, 3, 2):
        for copy in token_copies(d):
            copy.start()

    experts = lax.broadcasted_iota(jnp.int32, (16, 128), 0).astype(f32)
    row_id = lax.broadcasted_iota(jnp.int32, (128, 128), 0)
    col_id = lax.broadcasted_iota(jnp.int32, (128, 128), 1)
    earlier = (row_id < col_id).astype(f32).astype(bf16)
    place = lax.broadcasted_iota(jnp.int32, (256, 128), 0).astype(f32)

    def hits(routes_of, parts):
        hot = [(r == experts).astype(f32) for r in routes_of]
        before = jnp.dot((hot[0] + hot[1]).astype(bf16), earlier, preferred_element_type=f32)
        main, rem = [], []
        for k in range(2):
            slot = jnp.sum(before * hot[k], axis=0, keepdims=True)
            base = routes_of[k] * 16.0 + slot
            low = slot < float(MAIN)
            main.append((jnp.where(low, base, -1.0) == place).astype(f32))
            rem.append([
                (jnp.where(low, -1.0, base + (4.0 * j - 16.0)) == place).astype(f32) for j in parts
            ])
        return main, rem

    main_hit, rem_hit = hits(route, range(4))
    weight = [rw_ref[pl.ds(k, 1), :] for k in range(2)]
    over_rows = (((0,), (0,)), ((), ()))
    chosen = (main_hit[0] + main_hit[1]).astype(bf16)
    for k in range(0, AW, 512):
        cols = pl.ds(k, 512)
        outg[:, cols] = jnp.dot(chosen, nrm[:, cols], preferred_element_type=f32).astype(bf16)
    extra = jnp.zeros((256, REMA), f32)
    for j in range(4):
        extra = extra + jnp.dot(
            (rem_hit[0][j] + rem_hit[1][j]).astype(bf16), nrm[:, pl.ds(j * REMA, REMA)],
            preferred_element_type=f32,
        )
    outg[:, pl.ds(AW, REMA)] = extra.astype(bf16)

    def keep_split(ref, value):
        high = value.astype(bf16)
        ref[pl.ds(0, 256), :] = high
        ref[pl.ds(256, 256), :] = (value - high.astype(f32)).astype(bf16)

    def band(device):
        return pl.ds(pl.multiple_of(device * MAIN, MAIN), MAIN)

    def plane_copy(source, target, ssem, rsem, to, sender):
        return pltpu.make_async_remote_copy(
            src_ref=source.at[band(to), :], dst_ref=target.at[band(sender), :],
            send_sem=ssem.at[to], recv_sem=rsem.at[sender],
            device_id=(to, t), device_id_type=MESH,
        )

    for dz, dx in others:
        plane_copy(outg, arr, psend, precv, at(-dz, -dx), s).start()
    arr[band(s), :] = outg[band(s), :]
    keep_split(cm, weight[0] * main_hit[0] + weight[1] * main_hit[1])
    for j in range(4):
        keep_split(cr.at[j], weight[0] * rem_hit[0][j] + weight[1] * rem_hit[1][j])

    fold_row = lax.broadcasted_iota(jnp.int32, (16, 64), 0)
    fold_col = lax.broadcasted_iota(jnp.int32, (16, 64), 1)
    fold = [
        (fold_col == 16 * (fold_row >> 2) + 4 * j + (fold_row & 3)).astype(f32).astype(bf16)
        for j in range(4)
    ]

    def rows_of(position):
        return pl.ds(pl.multiple_of(position * CH, 16), CH)

    def x_copy(g, position, part, send, to, slot=None):
        cols = pl.ds(0, AW) if part == 2 else pl.ds(part * AH, AH)
        return pltpu.make_async_remote_copy(
            src_ref=xs.at[g, rows_of(position), cols], dst_ref=xs.at[g, rows_of(position), cols],
            send_sem=xsend.at[g, send], recv_sem=xrecv.at[g, position, part % 2],
            device_id=(s, to), device_id_type=MESH,
        )

    def x_sends(g):
        return [
            (g, t, 2, 0, lane(1, c)), (g, t, 2, 1, lane(-1, c)), (g, t, 2, 2, mate),
            (g, lane(-1, c), 0, 3, lane(1, c)), (g, lane(-1, c), 2, 4, mate),
            (g, lane(1, c), 1, 5, lane(-1, c)), (g, lane(1, c), 2, 6, mate),
            (g, lane(2, c), 2, 7, mate),
        ]

    def group_rows(g):
        zz = (z + GROUPS[g] + NZ) % NZ
        return pl.ds(pl.multiple_of(zz * 64, 64), 64)

    def build(g):
        for dx in (0, 1, -1, 2):
            if (GROUPS[g], dx) != (0, 0):
                plane_copy(outg, arr, psend, precv, s, at(GROUPS[g], dx)).wait_recv()
        rows = group_rows(g)
        first = pl.multiple_of(t * CH, 16)
        for k in range(0, AW, 512):
            xs[g, pl.ds(first, 64), pl.ds(k, 512)] = arr[rows, pl.ds(k, 512)]
        for j in range(4):
            xs[g, pl.ds(first + 64, 16), pl.ds(j * REMA, REMA)] = jnp.dot(
                fold[j], arr[rows, pl.ds(AW, REMA)], preferred_element_type=f32
            ).astype(bf16)
        for copy in x_sends(g)[:3]:
            x_copy(*copy).start()

    def forward(g):
        todo = x_sends(g)
        x_copy(g, lane(-1, c), 2, 0, t).wait_recv()
        x_copy(*todo[3]).start()
        x_copy(*todo[4]).start()
        x_copy(g, lane(1, c), 2, 0, t).wait_recv()
        x_copy(*todo[5]).start()
        x_copy(*todo[6]).start()

    def far(g):
        x_copy(g, lane(2, c), 0, 0, t).wait_recv()
        x_copy(g, lane(2, c), 1, 0, t).wait_recv()
        x_copy(*x_sends(g)[7]).start()

    def slot_copy(to, sender):
        return pltpu.make_async_remote_copy(
            src_ref=outb.at[to], dst_ref=arrb.at[sender],
            send_sem=obsend.at[to], recv_sem=obrecv.at[sender],
            device_id=(to, t), device_id_type=MESH,
        )

    def spread(_):
        for d in (1, 3, 2):
            for copy in token_copies(d):
                copy.wait_recv()
        mains, rems = [], []
        for yy in range(4):
            main, rem = hits([infos[yy, pl.ds(k, 1), :] for k in range(2)], (yy,))
            mains.append((main[0] + main[1]).astype(bf16))
            rems.append((rem[0][0] + rem[1][0]).astype(bf16))
        rems = jnp.concatenate(rems, axis=1)
        for k in range(0, WID - AW, 512):
            cols = pl.ds(k, 512)
            for yy in range(4):
                value = jnp.dot(mains[yy], toks[yy, :, cols], preferred_element_type=f32)
                outb[:, pl.ds(16 * yy, 16), cols] = value.astype(bf16).reshape(16, 16, 512)
            every = jnp.concatenate([toks[yy, :, cols] for yy in range(4)], axis=0)
            value = jnp.dot(rems, every, preferred_element_type=f32)
            outb[:, pl.ds(64, 16), cols] = value.astype(bf16).reshape(16, 16, 512)
        for dz, dx in others:
            slot_copy(at(-dz, -dx), s).start()
        arrb[s] = outb[s]

    move_row = lax.broadcasted_iota(jnp.int32, (64, 64), 0)
    move_col = lax.broadcasted_iota(jnp.int32, (64, 64), 1)
    move = (
        move_col == 16 * ((move_row >> 2) & 3) + 4 * (move_row >> 4) + (move_row & 3)
    ).astype(f32).astype(bf16)

    def far_copy(g, yy, core):
        cols = pl.ds(AW, WID - AW)
        return pltpu.make_async_remote_copy(
            src_ref=xs.at[g, rows_of(2 * yy + core), cols], dst_ref=xs.at[g, rows_of(2 * yy + core), cols],
            send_sem=xbsend.at[g, yy], recv_sem=xbrecv.at[g, yy],
            device_id=(s, mate), device_id_type=MESH,
        )

    def gather(g):
        for dx in (0, 1, -1, 2):
            if (GROUPS[g], dx) != (0, 0):
                slot_copy(s, at(GROUPS[g], dx)).wait_recv()
        first = ((z + GROUPS[g] + NZ) % NZ) * NX
        moved = []
        for k in range(0, WID - AW, 512):
            cols = pl.ds(k, 512)
            tails = jnp.concatenate([arrb[first + xx, pl.ds(64, 16), cols] for xx in range(4)], axis=0)
            moved.append(jnp.dot(move, tails, preferred_element_type=f32).astype(bf16))
        for yy in range(4):
            row = pl.multiple_of((2 * yy + c) * CH, 16)
            for i, k in enumerate(range(0, WID - AW, 512)):
                into = pl.ds(AW + k, 512)
                for xx in range(4):
                    xs[g, pl.ds(row + 16 * xx, 16), into] = arrb[
                        first + xx, pl.ds(16 * yy, 16), pl.ds(k, 512)
                    ]
                xs[g, pl.ds(row + 64, 16), into] = moved[i][16 * yy:16 * yy + 16]
            far_copy(g, yy, c).start()

    def pair_copy(g, yy):
        return pltpu.make_async_remote_copy(
            src_ref=ps.at[g, rows_of(2 * yy + 1 - c), :], dst_ref=pr.at[g, yy],
            send_sem=qsend.at[g, yy], recv_sem=qrecv.at[g, yy],
            device_id=(s, mate), device_id_type=MESH,
        )

    TURN = (2, 1, 3, 0)

    def compute(g):
        for dy in (0, -1, 1, 2):
            x_copy(g, lane(dy, 1 - c), 2, 0, t).wait_recv()
        for yy in range(4):
            far_copy(g, yy, 1 - c).wait_recv()
        if g == 0:
            for load in loads[1:]:
                load.wait()

        def block(i, carry):
            dy = jnp.where(i == 0, 2, jnp.where(i == 1, 1, jnp.where(i == 2, 3, 0)))
            yy = (y + dy) % 4
            rows = pl.ds(pl.multiple_of(yy * 2 * CH, 32), 2 * CH)
            value = xs[g, rows, :]
            both = jnp.dot(value, guw[...], preferred_element_type=f32)
            gate, upper = both[:, :640], both[:, 640:]
            act[...] = (gate / (1.0 + jnp.exp(-gate)) * upper).astype(bf16)
            ps[g, rows, :] = jnp.dot(act[...], dw[...], preferred_element_type=f32).astype(bf16)
            pair_copy(g, yy).start()
            return carry

        lax.fori_loop(0, 4, block, 0)

    def add_into(g, position, cols, terms):
        rows = rows_of(position)
        total = ps[g, rows, cols].astype(f32)
        for term in terms:
            total = total + term.astype(f32)
        ps[g, rows, cols] = total.astype(bf16)

    def r_copy(g, dy, part, send, direction, ref, sem, slot):
        cols = pl.ds(part * HW, HW)
        return pltpu.make_async_remote_copy(
            src_ref=ps.at[g, rows_of(lane(dy, c)), cols], dst_ref=ref.at[(g,) + slot],
            send_sem=rsend.at[g, send], recv_sem=sem.at[(g,) + slot],
            device_id=(s, lane(direction, c)), device_id_type=MESH,
        )

    def r_sends(g):
        return [
            (g, 2, 0, 0, 1, rh, rhrecv, (0,)), (g, 2, 1, 1, -1, rh, rhrecv, (1,)),
            (g, 1, 1, 2, 1, rf, rfrecv, (0, 1)), (g, -1, 0, 3, -1, rf, rfrecv, (1, 0)),
            (g, 1, 0, 4, 1, rf, rfrecv, (0, 0)), (g, -1, 1, 5, -1, rf, rfrecv, (1, 1)),
        ]

    def pair(g):
        todo = r_sends(g)
        for turn, dy in enumerate(TURN):
            yy = (y + dy) % 4
            pair_copy(g, yy).wait_recv()
            for k in range(2):
                cols = pl.ds(k * HW, HW)
                add_into(g, 2 * yy + c, cols, [pr[g, yy, :, cols]])
            if turn == 0:
                r_copy(*todo[0]).start()
                r_copy(*todo[1]).start()
            if turn == 1:
                r_copy(*todo[2]).start()
            if turn == 2:
                r_copy(*todo[3]).start()

    def middle(g):
        todo = r_sends(g)
        r_copy(*todo[0]).wait_recv()
        add_into(g, lane(1, c), pl.ds(0, HW), [rh[g, 0]])
        r_copy(*todo[4]).start()
        r_copy(*todo[1]).wait_recv()
        add_into(g, lane(-1, c), pl.ds(HW, HW), [rh[g, 1]])
        r_copy(*todo[5]).start()

    def finish(g):
        todo = r_sends(g)
        for k in range(2, 6):
            r_copy(*todo[k]).wait_recv()
        rows = group_rows(g)
        own = pl.multiple_of(t * CH, 16)
        extra = jnp.zeros((64, REM), f32)
        for j in range(4):
            cols = pl.ds(j * REM, REM)
            inner = pl.ds((j % 2) * REM, REM)
            total = (
                ps[g, pl.ds(own, CH), cols].astype(f32)
                + rf[g, 0, j // 2, :, inner].astype(f32)
                + rf[g, 1, j // 2, :, inner].astype(f32)
            ).astype(bf16)
            reto[rows, cols] = total[:64]
            extra = extra + lax.dot_general(fold[j], total[64:], over_rows, preferred_element_type=f32)
        reto[rows, pl.ds(WID, REM)] = extra.astype(bf16)
        for dx in (0, 1, -1, 2):
            to = at(GROUPS[g], dx)
            if (GROUPS[g], dx) == (0, 0):
                ret[band(s), :] = reto[band(s), :]
            else:
                plane_copy(reto, ret, bsend, brecv, to, s).start()

    def collect(g):
        for dx in (0, 1, -1, 2):
            if (GROUPS[g], dx) != (0, 0):
                plane_copy(reto, ret, bsend, brecv, s, at(-GROUPS[g], dx)).wait_recv()
        first = ((z - GROUPS[g] + NZ) % NZ) * 64
        rows = pl.ds(pl.multiple_of(first, 64), 64)
        low = pl.ds(pl.multiple_of(first + 256, 64), 64)
        factor = jnp.concatenate([cm[rows, :], cm[low, :]], axis=0)
        tail = ret[rows, pl.ds(WID, REM)]
        for j in range(4):
            cols = pl.ds(j * REM, REM)
            back = ret[rows, cols]
            routed = lax.dot_general(
                jnp.concatenate([factor, cr[j, rows, :], cr[j, low, :]], axis=0),
                jnp.concatenate([back, back, tail, tail], axis=0), over_rows,
                preferred_element_type=f32,
            )
            if g == 3:
                out_ref[:, cols] = (att[:, cols] + routed).astype(bf16)
            else:
                att[:, cols] = att[:, cols] + routed

    for stage, g in (
        (build, 0), (build, 1), (spread, 0), (forward, 0), (build, 2), (forward, 1),
        (build, 3), (far, 0), (gather, 0), (compute, 0), (pair, 0), (forward, 2),
        (far, 1), (gather, 1), (compute, 1), (pair, 1), (middle, 0), (forward, 3),
        (far, 2), (gather, 2), (compute, 2), (middle, 1), (pair, 2), (finish, 0),
        (far, 3), (gather, 3), (compute, 3), (middle, 2), (pair, 3), (finish, 1),
        (middle, 3), (finish, 2), (finish, 3), (collect, 0), (collect, 1), (collect, 2),
        (collect, 3),
    ):
        stage(g)

    for dz, dx in others:
        plane_copy(outg, arr, psend, precv, at(dz, dx), s).wait_send()
        plane_copy(reto, ret, bsend, brecv, at(dz, dx), s).wait_send()
        slot_copy(at(dz, dx), s).wait_send()
    for d in (1, 2, 3):
        for copy in token_copies(d):
            copy.wait_send()
    for g in range(4):
        for copy in x_sends(g):
            x_copy(*copy).wait_send()
        for yy in range(4):
            pair_copy(g, yy).wait_send()
            far_copy(g, yy, c).wait_send()
        for copy in r_sends(g):
            r_copy(*copy).wait_send()


def routed_experts(
    heads, stream, ffn_gain, routes, route_weight, out_weight, gate_weight, up_weight, down_weight
):
    any_space = pl.BlockSpec(memory_space=pltpu.HBM)
    vmem = pl.BlockSpec(memory_space=pltpu.VMEM)
    bf16, f32 = jnp.bfloat16, jnp.float32
    dma = pltpu.SemaphoreType.DMA
    return pl.pallas_call(
        expert_kernel,
        out_shape=jax.ShapeDtypeStruct((128, WID), bf16),
        in_specs=[any_space] * 9,
        out_specs=vmem,
        scratch_shapes=[
            pltpu.VMEM((128, 1024), bf16),
            pltpu.VMEM((128, WID), bf16),
            pltpu.VMEM((1, WID), f32),
            pltpu.VMEM((2, 128), jnp.int32),
            pltpu.VMEM((2, 128), f32),
            pltpu.VMEM((4, 8, 128), f32),
            pltpu.VMEM((4, 128, WID - AW), bf16),
            pltpu.VMEM((16, CH, WID - AW), bf16),
            pltpu.VMEM((16, CH, WID - AW), bf16),
            pltpu.VMEM((1024, WID), bf16),
            pltpu.VMEM((WID, 1280), bf16),
            pltpu.VMEM((640, WID), bf16),
            pltpu.VMEM((128, WID), f32),
            pltpu.VMEM((128, AW), bf16),
            pltpu.VMEM((256, AW + REMA), bf16),
            pltpu.VMEM((256, AW + REMA), bf16),
            pltpu.VMEM((256, BAND), bf16),
            pltpu.VMEM((256, BAND), bf16),
            pltpu.VMEM((4, NT * CH, WID), bf16),
            pltpu.VMEM((2 * CH, 640), bf16),
            pltpu.VMEM((4, NT * CH, WID), bf16),
            pltpu.VMEM((4, 4, CH, WID), bf16),
            pltpu.VMEM((4, 2, CH, HW), bf16),
            pltpu.VMEM((4, 2, 2, CH, HW), bf16),
            pltpu.VMEM((512, 128), bf16),
            pltpu.VMEM((4, 512, 128), bf16),
            dma((9,)),
            dma((4,)), dma((4,)), dma((4,)), dma((4,)),
            dma((16,)), dma((16,)), dma((4, 4)), dma((4, 4)),
            dma((16,)), dma((16,)),
            dma((4, 8)), dma((4, 8, 2)),
            dma((4, 4)), dma((4, 4)),
            dma((4, 6)), dma((4, 2)), dma((4, 2, 2)),
            dma((16,)), dma((16,)),
        ],
        compiler_params=pltpu.CompilerParams(
            collective_id=1, has_side_effects=True, vmem_limit_bytes=67043328
        ),
        name="experts",
    )(
        heads, stream, ffn_gain.reshape(1, -1), routes.T, route_weight.T,
        out_weight, gate_weight, up_weight, down_weight,
    )


def local(
    queries,
    key_rows,
    value_rows,
    lambdas,
    head_gain,
    out_weight,
    stream,
    ffn_gain,
    routes,
    route_weight,
    gate_weight,
    up_weight,
    down_weight,
):
    heads_local = attention(lambdas, head_gain, queries, key_rows, value_rows)
    return routed_experts(
        heads_local, stream, ffn_gain, routes, route_weight,
        out_weight, gate_weight, up_weight, down_weight,
    )


def solution(mesh):
    placed = (
        P("sp", "tp"),
        P("sp", "tp"),
        P("sp", "tp"),
        P("tp"),
        P(),
        P(),
        P(("sp", "tp"), None),
        P(),
        P(("sp", "tp"), None),
        P(("sp", "tp"), None),
        P("sp", None, "tp"),
        P("sp", None, "tp"),
        P("sp", "tp", None),
    )
    return jax.shard_map(
        local, mesh=mesh, in_specs=placed, out_specs=P(("sp", "tp"), None), check_vma=False
    )
```

```python
import functools

import jax
import jax.numpy as jnp
from jax import lax
from jax.experimental import pallas as pl
from jax.experimental.pallas import tpu as pltpu
from jax.sharding import PartitionSpec as P

DH = 64


LOG2E = 1.4426950408889634
MESH = pl.DeviceIdType.MESH
NZ = 4
NX = 4
BLK = 1024
HALF = 512
NEG = -1e30
VROWS = 144
TQ = 512
KB = 512
WORK = (
    (0, 0), (3, 0), (1, 0), (3, 3), (3, 1), (1, 3), (1, 1), (3, 2), (1, 2),
    (2, 0), (2, 3), (2, 1), (2, 2), (0, 3), (0, 1), (0, 2),
)


def attention_kernel(
    lam_hbm, gain_hbm, q_hbm, k_hbm, v_hbm, out_ref,
    lam_ref, gain_ref, vin, lamv, qfull, qother, kb, vb, qm, mx, acc, pout, pin, sout, sin, obuf, sbuf0, sbuf1, fbuf0, fbuf1, nbuf0, nbuf1,
    load_sem, lsend, lrecv, send_sem, recv_sem, msend, mrecv, psend, precv, ssend, srecv, osend, orecv,
):
    sp = lax.axis_index("sp")
    t = lax.axis_index("tp")
    z, x = sp // NX, sp % NX
    y, c = t // 2, t % 2
    mate = 2 * y + 1 - c
    f32, bf16 = jnp.float32, jnp.bfloat16
    sbuf, fbuf, nbuf = (sbuf0, sbuf1), (fbuf0, fbuf1), (nbuf0, nbuf1)

    def at(dz, dx):
        return ((z + dz + NZ) % NZ) * NX + (x + dx + NX) % NX

    loads = [
        pltpu.make_async_copy(q_hbm, qfull.at[0], load_sem.at[0]),
        pltpu.make_async_copy(k_hbm, kb.at[0, 0], load_sem.at[1]),
        pltpu.make_async_copy(v_hbm, vin, load_sem.at[2]),
    ]
    small = [
        pltpu.make_async_copy(lam_hbm, lam_ref, load_sem.at[3]),
        pltpu.make_async_copy(gain_hbm, gain_ref, load_sem.at[4]),
    ]
    for load in loads + small:
        load.start()

    barrier = pltpu.get_barrier_semaphore()
    for dz, dx in ((0, 1), (0, -1), (1, 0), (-1, 0), (2, 0), (0, 2)):
        pl.semaphore_signal(barrier, inc=1, device_id=(at(dz, dx), t), device_id_type=MESH)
    for j in range(1, 8):
        pl.semaphore_signal(barrier, inc=1, device_id=(sp, (t + j) % 8), device_id_type=MESH)

    def along(e, queries, d):
        own = c if e == 0 else 1 - c
        first = at(d, 0) if queries else at(0, d)
        second = at(0, d) if queries else at(d, 0)
        return jnp.where(own == 0, first, second)

    def piece(kind, slot, part):
        span = pl.ds(0, BLK) if part == 2 else pl.ds(part * HALF, HALF)
        if kind == 0:
            return qfull.at[slot, span, :]
        if kind == 1:
            return kb.at[0, slot, span, :]
        return vb.at[0, slot, :, span]

    def ring_copy(kind, slot, part, lane):
        d = 1 if lane == 0 else -1
        return pltpu.make_async_remote_copy(
            src_ref=piece(kind, slot, part), dst_ref=piece(kind, (slot - d) % 4, part),
            send_sem=send_sem.at[kind, slot, lane],
            recv_sem=recv_sem.at[kind, (slot - d) % 4, part % 2],
            device_id=(along(0, kind == 0, d), t), device_id_type=MESH,
        )

    RING = ((0, 2, 0), (0, 2, 1), (3, 0, 0), (1, 1, 1))

    def ring_wait(kind, slot):
        for part in (0, 1) if slot == 2 else (2,):
            pltpu.make_async_remote_copy(
                src_ref=piece(kind, slot, part), dst_ref=piece(kind, slot, part),
                send_sem=send_sem.at[kind, 0, 0], recv_sem=recv_sem.at[kind, slot, part % 2],
                device_id=(sp, mate), device_id_type=MESH,
            ).wait_recv()

    def mate_copy(kind, slot):
        if kind == 0:
            source = qfull.at[slot, pl.ds(pl.multiple_of((1 - c) * HALF, HALF), HALF), :]
            target = qother.at[slot]
        elif kind == 1:
            source, target = kb.at[0, slot], kb.at[1, slot]
        else:
            source, target = vb.at[0, slot], vb.at[1, slot]
        return pltpu.make_async_remote_copy(
            src_ref=source, dst_ref=target,
            send_sem=msend.at[kind, slot], recv_sem=mrecv.at[kind, slot],
            device_id=(sp, mate), device_id_type=MESH,
        )

    def lambda_copy():
        return pltpu.make_async_remote_copy(
            src_ref=lamv.at[0], dst_ref=lamv.at[1], send_sem=lsend, recv_sem=lrecv,
            device_id=(sp, mate), device_id_type=MESH,
        )

    lane_ids = lax.broadcasted_iota(jnp.int32, (HALF, 2 * DH), 1)

    def split_maps(e, slot):
        if e == 0:
            q = qfull[slot, pl.ds(pl.multiple_of(c * HALF, HALF), HALF), :]
        else:
            q = qother[slot]
        zero = jnp.zeros_like(q)
        qm[e, slot, 0] = jnp.where(lane_ids < DH, q, zero)
        qm[e, slot, 1] = jnp.where(lane_ids < DH, zero, q)

    def arrive(kind, slot):
        ring_wait(kind, slot)
        if slot == 3:
            ring_copy(kind, 3, 0, 0).start()
        if slot == 1:
            ring_copy(kind, 1, 1, 1).start()
        mate_copy(kind, slot).start()

    def settle(kind, slot):
        mate_copy(kind, slot).wait_recv()
        if kind == 0:
            split_maps(0, slot)
            split_maps(1, slot)

    for load in loads + small:
        load.wait()
    lamv[0] = jnp.full((8, HALF), lam_ref[0], f32)
    pl.semaphore_wait(barrier, 13)
    for kind in (0, 1):
        for lane in range(2):
            ring_copy(kind, 0, 2, lane).start()
    mate_copy(1, 0).start()
    mate_copy(0, 0).start()
    lambda_copy().start()
    for k in range(4):
        span = pl.ds(k * 256, 256)
        vb[0, 0, :, span] = vin[span, :].astype(f32).T.astype(bf16)
    for lane in range(2):
        ring_copy(2, 0, 2, lane).start()
    mate_copy(2, 0).start()

    mx[...] = jnp.full(mx.shape, NEG, f32)
    acc[...] = jnp.zeros(acc.shape, f32)

    scale = LOG2E * DH ** (-0.5)

    always = sp >= 0

    def tiles(e, di, dk, masked):
        chunks = [(m, r) for m in range(2) for r in range(HALF // TQ)]

        def phase(now, later):
            tops, pv = [], None
            for kk in range(BLK // KB):
                keys = pl.ds(kk * KB, KB)
                if later is not None:
                    m, r = chunks[later]
                    scores = lax.dot_general(
                        kb[e, dk, keys, :], qm[e, di, m, pl.ds(r * TQ, TQ), :],
                        (((1,), (1,)), ((), ())), preferred_element_type=f32,
                    ) * scale
                    if masked:
                        key_id = lax.broadcasted_iota(jnp.int32, scores.shape, 0) + kk * KB
                        query_id = lax.broadcasted_iota(jnp.int32, scores.shape, 1) + (c * HALF + r * TQ)
                        scores = jnp.where(key_id <= query_id, scores, NEG)
                    sbuf[later % 2][keys, :] = scores
                    tops.append(jnp.max(scores, axis=0, keepdims=True))
                if now is not None:
                    m, r = chunks[now]
                    values = jnp.concatenate(
                        [vb[e, dk, :, keys], jnp.ones((VROWS - 128, KB), bf16)], axis=0
                    )
                    weights = jnp.exp2(sbuf[now % 2][keys, :] - nbuf[now % 2][...]).astype(bf16)
                    term = jnp.dot(values, weights, preferred_element_type=f32)
                    pv = term if pv is None else pv + term
            if now is not None:
                m, r = chunks[now]
                cols = pl.ds(r * TQ, TQ)
                acc[e, di, m, :, cols] = acc[e, di, m, :, cols] * fbuf[now % 2][...] + pv
            if later is not None:
                m, r = chunks[later]
                cols = pl.ds(r * TQ, TQ)
                old = mx[e, di, m, :, cols]
                new = functools.reduce(jnp.maximum, tops, old)
                fbuf[later % 2][...] = jnp.exp2(old - new)
                nbuf[later % 2][...] = new
                mx[e, di, m, :, cols] = new

        phase(None, 0)
        for n in range(len(chunks)):
            @pl.when(always)
            def _(n=n):
                phase(n, n + 1 if n + 1 < len(chunks) else None)

    def partial_copies(e, d):
        to = along(e, True, d)
        slot = (4 - d) % 4
        return [
            pltpu.make_async_remote_copy(
                src_ref=pout.at[e, d], dst_ref=pin.at[e, slot],
                send_sem=psend.at[e, d], recv_sem=precv.at[e, slot],
                device_id=(to, t), device_id_type=MESH,
            ),
            pltpu.make_async_remote_copy(
                src_ref=sout.at[e, d], dst_ref=sin.at[e, slot],
                send_sem=ssend.at[e, d], recv_sem=srecv.at[e, slot],
                device_id=(to, t), device_id_type=MESH,
            ),
        ]

    def normal(e, d, m):
        total = acc[e, d, m, pl.ds(128, 1), :]
        some = total > 0.0
        safe = jnp.where(some, total, 1.0)
        level = jnp.where(some, mx[e, d, m] + jnp.log2(safe), NEG)
        return acc[e, d, m, pl.ds(0, 128), :] * (1.0 / safe), level

    def send_partial(d):
        for e in range(2):
            for m in range(2):
                value, level = normal(e, d, m)
                pout[e, d, m] = value.astype(bf16)
                sout[e, d, m] = jnp.broadcast_to(level, (8, HALF))
            for copy in partial_copies(e, d):
                copy.start()

    def before(n):
        if n == 0:
            for kind in (1, 0, 2):
                settle(kind, 0)
        if n == 1:
            for kind in (0, 1):
                for slot in (3, 1):
                    arrive(kind, slot)
            for slot in (3, 1):
                settle(0, slot)
        if n == 3:
            for slot in (3, 1):
                arrive(2, slot)
            for kind in (1, 2):
                for slot in (3, 1):
                    settle(kind, slot)
        if n == 6:
            for kind in range(3):
                arrive(kind, 2)
            for kind in range(3):
                settle(kind, 2)
        if n == 8:
            send_partial(3)
        if n == 9:
            send_partial(1)
        if n == 13:
            send_partial(2)

    def step(n, carry):
        for k in (0, 1, 3, 6, 8, 9, 13):
            @pl.when(n == k)
            def _(k=k):
                before(k)

        di = jnp.int32(0)
        dk = jnp.int32(0)
        for k, (a, b) in enumerate(WORK):
            di = jnp.where(n == k, a, di)
            dk = jnp.where(n == k, b, dk)

        def one_head(e, inner):
            head = jnp.where(e == 0, c, 1 - c)
            query_block = jnp.where(head == 0, at(di, 0), at(0, di))
            key_block = jnp.where(head == 0, at(0, dk), at(dk, 0))

            @pl.when(key_block < query_block)
            def _():
                tiles(e, di, dk, False)

            @pl.when(key_block == query_block)
            def _():
                tiles(e, di, dk, True)

            return inner

        return lax.fori_loop(0, 2, one_head, carry)

    lax.fori_loop(0, len(WORK), step, 0)

    def out_copy(e, j, sender):
        cols = pl.ds(pl.multiple_of(sender * 128, 128), 128)
        return pltpu.make_async_remote_copy(
            src_ref=obuf.at[e, pl.ds(j * 128, 128), :], dst_ref=out_ref.at[:, cols],
            send_sem=osend.at[e, j], recv_sem=orecv.at[sender],
            device_id=(sp, 4 * c + j), device_id_type=MESH,
        )

    def own_copy(e, j, head):
        cols = pl.ds(pl.multiple_of(head * 128, 128), 128)
        return pltpu.make_async_copy(
            obuf.at[e, pl.ds(j * 128, 128), :], out_ref.at[:, cols], osend.at[e, j]
        )

    lambda_copy().wait_recv()
    for e in range(2):
        head = t if e == 0 else mate
        for slot in (1, 3, 2):
            pltpu.make_async_remote_copy(
                src_ref=pout.at[e, slot], dst_ref=pin.at[e, slot],
                send_sem=psend.at[e, slot], recv_sem=precv.at[e, slot],
                device_id=(sp, mate), device_id_type=MESH,
            ).wait_recv()
            pltpu.make_async_remote_copy(
                src_ref=sout.at[e, slot], dst_ref=sin.at[e, slot],
                send_sem=ssend.at[e, slot], recv_sem=srecv.at[e, slot],
                device_id=(sp, mate), device_id_type=MESH,
            ).wait_recv()
        mixed = []
        for m in range(2):
            value, level = normal(e, 0, m)
            levels = [level] + [sin[e, slot, m, pl.ds(0, 1), :] for slot in (1, 2, 3)]
            top = jnp.maximum(jnp.maximum(levels[0], levels[1]), jnp.maximum(levels[2], levels[3]))
            share = [jnp.exp2(item - top) for item in levels]
            inverse = 1.0 / (share[0] + share[1] + share[2] + share[3])
            total = value * (share[0] * inverse)
            for slot in (1, 2, 3):
                total = total + pin[e, slot, m].astype(f32) * (share[slot] * inverse)
            mixed.append(total)
        contrast = mixed[0] - lamv[e, pl.ds(0, 1), :] * mixed[1]
        mean = jnp.mean(contrast * contrast, axis=0, keepdims=True)
        contrast = contrast * lax.rsqrt(mean + 1e-05)
        for j in range(4):
            rows = contrast[:, j * 128:(j + 1) * 128].T * gain_ref[...]
            obuf[e, pl.ds(j * 128, 128), :] = rows.astype(bf16)
        for j in range(4):
            @pl.when(t != 4 * c + j)
            def _(e=e, j=j, head=head):
                out_copy(e, j, head).start()
            @pl.when(t == 4 * c + j)
            def _(e=e, j=j, head=head):
                own_copy(e, j, head).start()

    origin = t // 4
    for yy in range(4):
        for core in range(2):
            @pl.when(2 * yy + origin != t)
            def _(yy=yy, core=core):
                out_copy(0, 0, 2 * yy + core).wait_recv()
    for e in range(2):
        for j in range(4):
            @pl.when(t != 4 * c + j)
            def _(e=e, j=j):
                out_copy(e, j, t).wait_send()
            @pl.when(t == 4 * c + j)
            def _(e=e, j=j):
                own_copy(e, j, t).wait()
    lambda_copy().wait_send()
    for kind in range(3):
        for slot, part, lane in RING:
            ring_copy(kind, slot, part, lane).wait_send()
        for slot in range(4):
            mate_copy(kind, slot).wait_send()
    for e in range(2):
        for d in (1, 2, 3):
            for copy in partial_copies(e, d):
                copy.wait_send()


def attention(lambdas, head_gain, queries, key_rows, value_rows):
    any_space = pl.BlockSpec(memory_space=pltpu.HBM)
    bf16, f32 = jnp.bfloat16, jnp.float32
    dma = pltpu.SemaphoreType.DMA
    return pl.pallas_call(
        attention_kernel,
        out_shape=jax.ShapeDtypeStruct((128, 1024), jnp.bfloat16),
        in_specs=[
            any_space, any_space, any_space, any_space, any_space,
        ],
        out_specs=any_space,
        scratch_shapes=[
            pltpu.SMEM((1,), f32),
            pltpu.VMEM((1, 128), f32),
            pltpu.VMEM((BLK, 128), bf16),
            pltpu.VMEM((2, 8, HALF), f32),
            pltpu.VMEM((4, BLK, 128), bf16),
            pltpu.VMEM((4, HALF, 128), bf16),
            pltpu.VMEM((2, 4, BLK, 128), bf16),
            pltpu.VMEM((2, 4, 128, BLK), bf16),
            pltpu.VMEM((2, 4, 2, HALF, 128), bf16),
            pltpu.VMEM((2, 4, 2, 1, HALF), f32),
            pltpu.VMEM((2, 4, 2, VROWS, HALF), f32),
            pltpu.VMEM((2, 4, 2, 128, HALF), bf16),
            pltpu.VMEM((2, 4, 2, 128, HALF), bf16),
            pltpu.VMEM((2, 4, 2, 8, HALF), f32),
            pltpu.VMEM((2, 4, 2, 8, HALF), f32),
            pltpu.VMEM((2, HALF, 128), bf16),
            pltpu.VMEM((BLK, TQ), f32), pltpu.VMEM((BLK, TQ), f32),
            pltpu.VMEM((1, TQ), f32), pltpu.VMEM((1, TQ), f32),
            pltpu.VMEM((1, TQ), f32), pltpu.VMEM((1, TQ), f32),
            dma((5,)),
            dma, dma,
            dma((3, 4, 2)), dma((3, 4, 2)),
            dma((3, 4)), dma((3, 4)),
            dma((2, 4)), dma((2, 4)),
            dma((2, 4)), dma((2, 4)),
            dma((2, 4)), dma((8,)),
        ],
        compiler_params=pltpu.CompilerParams(
            collective_id=0, has_side_effects=True, vmem_limit_bytes=67043328
        ),
        name="attention",
    )(lambdas, head_gain.reshape(1, -1), queries, key_rows, value_rows)


GROUPS = (0, 1, 2, -1)
MAIN = 16
CH = 80
WID = 2048
HW = 1024
AW = 1536
AH = AW // 2
REMA = AW // 4
REM = 512
BAND = WID + REM
NT = 8


def expert_kernel(
    heads_hbm, stream_hbm, gain_hbm, routes_hbm, rw_hbm, ow_hbm, gate_hbm, up_hbm, down_hbm,
    out_ref,
    heads_ref, stream_ref, gain_ref, routes_ref, rw_ref, infos, toks, outb, arrb, ow, guw, dw, att, nrm, outg, arr, reto, ret, xs, act, ps, pr, rh, rf, cm, cr,
    load_sem, isend, irecv, tsend, trecv, obsend, obrecv, xbsend, xbrecv, psend, precv, xsend, xrecv, qsend, qrecv, rsend, rhrecv, rfrecv, bsend, brecv,
):
    s = lax.axis_index("sp")
    t = lax.axis_index("tp")
    z, x = s // NX, s % NX
    y, c = t // 2, t % 2
    mate = 2 * y + 1 - c
    bf16, f32 = jnp.bfloat16, jnp.float32

    def at(dz, dx):
        return ((z + dz + NZ) % NZ) * NX + (x + dx + NX) % NX

    def lane(dy, core):
        return 2 * ((y + dy + 4) % 4) + core

    loads = [
        pltpu.make_async_copy(ow_hbm, ow, load_sem.at[0]),
        pltpu.make_async_copy(gate_hbm.at[0], guw.at[:, pl.ds(0, 640)], load_sem.at[1]),
        pltpu.make_async_copy(up_hbm.at[0], guw.at[:, pl.ds(640, 640)], load_sem.at[2]),
        pltpu.make_async_copy(down_hbm.at[0], dw, load_sem.at[3]),
    ]
    small = [
        pltpu.make_async_copy(routes_hbm, routes_ref, load_sem.at[4]),
        pltpu.make_async_copy(rw_hbm, rw_ref, load_sem.at[5]),
        pltpu.make_async_copy(stream_hbm, stream_ref, load_sem.at[6]),
        pltpu.make_async_copy(gain_hbm, gain_ref, load_sem.at[7]),
        pltpu.make_async_copy(heads_hbm, heads_ref, load_sem.at[8]),
    ]
    for load in small + loads:
        load.start()

    barrier = pltpu.get_barrier_semaphore()
    others = [(dz, dx) for dz in GROUPS for dx in (0, 1, -1, 2) if (dz, dx) != (0, 0)]
    for dz, dx in others:
        pl.semaphore_signal(barrier, inc=1, device_id=(at(dz, dx), t), device_id_type=MESH)
    for peer in (lane(1, c), lane(-1, c), lane(2, c), mate):
        pl.semaphore_signal(barrier, inc=1, device_id=(s, peer), device_id_type=MESH)

    for load in small + loads[:1]:
        load.wait()
    heads = heads_ref[...]
    square = jnp.zeros((128, 1), f32)
    for k in range(0, WID, 512):
        cols = pl.ds(k, 512)
        value = stream_ref[:, cols].astype(f32) + jnp.dot(heads, ow[:, cols], preferred_element_type=f32)
        att[:, cols] = value
        square = square + jnp.sum(value * value, axis=1, keepdims=True)
    inverse = lax.rsqrt(square * (1.0 / WID) + 1e-06)
    for k in range(0, WID, 512):
        cols = pl.ds(k, 512)
        value = (att[:, cols] * inverse * gain_ref[:, cols]).astype(bf16)
        if k < AW:
            nrm[:, cols] = value
        else:
            toks[y, :, pl.ds(k - AW, 512)] = value

    route = [routes_ref[pl.ds(k, 1), :].astype(f32) for k in range(2)]
    infos[y] = jnp.concatenate(route + [jnp.zeros((6, 128), f32)], axis=0)

    def token_copies(d):
        return [
            pltpu.make_async_remote_copy(
                src_ref=infos.at[y], dst_ref=infos.at[y], send_sem=isend.at[d], recv_sem=irecv.at[d],
                device_id=(s, lane(d, c)), device_id_type=MESH,
            ),
            pltpu.make_async_remote_copy(
                src_ref=toks.at[y], dst_ref=toks.at[y], send_sem=tsend.at[d], recv_sem=trecv.at[d],
                device_id=(s, lane(d, c)), device_id_type=MESH,
            ),
        ]

    pl.semaphore_wait(barrier, len(others) + 4)
    for d in (1, 3, 2):
        for copy in token_copies(d):
            copy.start()

    experts = lax.broadcasted_iota(jnp.int32, (16, 128), 0).astype(f32)
    row_id = lax.broadcasted_iota(jnp.int32, (128, 128), 0)
    col_id = lax.broadcasted_iota(jnp.int32, (128, 128), 1)
    earlier = (row_id < col_id).astype(f32).astype(bf16)
    place = lax.broadcasted_iota(jnp.int32, (256, 128), 0).astype(f32)

    def hits(routes_of, parts):
        hot = [(r == experts).astype(f32) for r in routes_of]
        before = jnp.dot((hot[0] + hot[1]).astype(bf16), earlier, preferred_element_type=f32)
        main, rem = [], []
        for k in range(2):
            slot = jnp.sum(before * hot[k], axis=0, keepdims=True)
            base = routes_of[k] * 16.0 + slot
            low = slot < float(MAIN)
            main.append((jnp.where(low, base, -1.0) == place).astype(f32))
            rem.append([
                (jnp.where(low, -1.0, base + (4.0 * j - 16.0)) == place).astype(f32) for j in parts
            ])
        return main, rem

    main_hit, rem_hit = hits(route, range(4))
    weight = [rw_ref[pl.ds(k, 1), :] for k in range(2)]
    over_rows = (((0,), (0,)), ((), ()))
    chosen = (main_hit[0] + main_hit[1]).astype(bf16)
    for k in range(0, AW, 512):
        cols = pl.ds(k, 512)
        outg[:, cols] = jnp.dot(chosen, nrm[:, cols], preferred_element_type=f32).astype(bf16)
    extra = jnp.zeros((256, REMA), f32)
    for j in range(4):
        extra = extra + jnp.dot(
            (rem_hit[0][j] + rem_hit[1][j]).astype(bf16), nrm[:, pl.ds(j * REMA, REMA)],
            preferred_element_type=f32,
        )
    outg[:, pl.ds(AW, REMA)] = extra.astype(bf16)

    def keep_split(ref, value):
        high = value.astype(bf16)
        ref[pl.ds(0, 256), :] = high
        ref[pl.ds(256, 256), :] = (value - high.astype(f32)).astype(bf16)

    def band(device):
        return pl.ds(pl.multiple_of(device * MAIN, MAIN), MAIN)

    def plane_copy(source, target, ssem, rsem, to, sender):
        return pltpu.make_async_remote_copy(
            src_ref=source.at[band(to), :], dst_ref=target.at[band(sender), :],
            send_sem=ssem.at[to], recv_sem=rsem.at[sender],
            device_id=(to, t), device_id_type=MESH,
        )

    for dz, dx in others:
        plane_copy(outg, arr, psend, precv, at(-dz, -dx), s).start()
    arr[band(s), :] = outg[band(s), :]
    keep_split(cm, weight[0] * main_hit[0] + weight[1] * main_hit[1])
    for j in range(4):
        keep_split(cr.at[j], weight[0] * rem_hit[0][j] + weight[1] * rem_hit[1][j])

    fold_row = lax.broadcasted_iota(jnp.int32, (16, 64), 0)
    fold_col = lax.broadcasted_iota(jnp.int32, (16, 64), 1)
    fold = [
        (fold_col == 16 * (fold_row >> 2) + 4 * j + (fold_row & 3)).astype(f32).astype(bf16)
        for j in range(4)
    ]

    def rows_of(position):
        return pl.ds(pl.multiple_of(position * CH, 16), CH)

    def x_copy(g, position, part, send, to, slot=None):
        cols = pl.ds(0, AW) if part == 2 else pl.ds(part * AH, AH)
        return pltpu.make_async_remote_copy(
            src_ref=xs.at[g, rows_of(position), cols], dst_ref=xs.at[g, rows_of(position), cols],
            send_sem=xsend.at[g, send], recv_sem=xrecv.at[g, position, part % 2],
            device_id=(s, to), device_id_type=MESH,
        )

    def x_sends(g):
        return [
            (g, t, 2, 0, lane(1, c)), (g, t, 2, 1, lane(-1, c)), (g, t, 2, 2, mate),
            (g, lane(-1, c), 0, 3, lane(1, c)), (g, lane(-1, c), 2, 4, mate),
            (g, lane(1, c), 1, 5, lane(-1, c)), (g, lane(1, c), 2, 6, mate),
            (g, lane(2, c), 2, 7, mate),
        ]

    def group_rows(g):
        zz = (z + GROUPS[g] + NZ) % NZ
        return pl.ds(pl.multiple_of(zz * 64, 64), 64)

    def build(g):
        for dx in (0, 1, -1, 2):
            if (GROUPS[g], dx) != (0, 0):
                plane_copy(outg, arr, psend, precv, s, at(GROUPS[g], dx)).wait_recv()
        rows = group_rows(g)
        first = pl.multiple_of(t * CH, 16)
        for k in range(0, AW, 512):
            xs[g, pl.ds(first, 64), pl.ds(k, 512)] = arr[rows, pl.ds(k, 512)]
        for j in range(4):
            xs[g, pl.ds(first + 64, 16), pl.ds(j * REMA, REMA)] = jnp.dot(
                fold[j], arr[rows, pl.ds(AW, REMA)], preferred_element_type=f32
            ).astype(bf16)
        for copy in x_sends(g)[:3]:
            x_copy(*copy).start()

    def forward(g):
        todo = x_sends(g)
        x_copy(g, lane(-1, c), 2, 0, t).wait_recv()
        x_copy(*todo[3]).start()
        x_copy(*todo[4]).start()
        x_copy(g, lane(1, c), 2, 0, t).wait_recv()
        x_copy(*todo[5]).start()
        x_copy(*todo[6]).start()

    def far(g):
        x_copy(g, lane(2, c), 0, 0, t).wait_recv()
        x_copy(g, lane(2, c), 1, 0, t).wait_recv()
        x_copy(*x_sends(g)[7]).start()

    def slot_copy(to, sender):
        return pltpu.make_async_remote_copy(
            src_ref=outb.at[to], dst_ref=arrb.at[sender],
            send_sem=obsend.at[to], recv_sem=obrecv.at[sender],
            device_id=(to, t), device_id_type=MESH,
        )

    def spread(_):
        for d in (1, 3, 2):
            for copy in token_copies(d):
                copy.wait_recv()
        mains, rems = [], []
        for yy in range(4):
            main, rem = hits([infos[yy, pl.ds(k, 1), :] for k in range(2)], (yy,))
            mains.append((main[0] + main[1]).astype(bf16))
            rems.append((rem[0][0] + rem[1][0]).astype(bf16))
        rems = jnp.concatenate(rems, axis=1)
        for k in range(0, WID - AW, 512):
            cols = pl.ds(k, 512)
            for yy in range(4):
                value = jnp.dot(mains[yy], toks[yy, :, cols], preferred_element_type=f32)
                outb[:, pl.ds(16 * yy, 16), cols] = value.astype(bf16).reshape(16, 16, 512)
            every = jnp.concatenate([toks[yy, :, cols] for yy in range(4)], axis=0)
            value = jnp.dot(rems, every, preferred_element_type=f32)
            outb[:, pl.ds(64, 16), cols] = value.astype(bf16).reshape(16, 16, 512)
        for dz, dx in others:
            slot_copy(at(-dz, -dx), s).start()
        arrb[s] = outb[s]

    move_row = lax.broadcasted_iota(jnp.int32, (64, 64), 0)
    move_col = lax.broadcasted_iota(jnp.int32, (64, 64), 1)
    move = (
        move_col == 16 * ((move_row >> 2) & 3) + 4 * (move_row >> 4) + (move_row & 3)
    ).astype(f32).astype(bf16)

    def far_copy(g, yy, core):
        cols = pl.ds(AW, WID - AW)
        return pltpu.make_async_remote_copy(
            src_ref=xs.at[g, rows_of(2 * yy + core), cols], dst_ref=xs.at[g, rows_of(2 * yy + core), cols],
            send_sem=xbsend.at[g, yy], recv_sem=xbrecv.at[g, yy],
            device_id=(s, mate), device_id_type=MESH,
        )

    def gather(g):
        for dx in (0, 1, -1, 2):
            if (GROUPS[g], dx) != (0, 0):
                slot_copy(s, at(GROUPS[g], dx)).wait_recv()
        first = ((z + GROUPS[g] + NZ) % NZ) * NX
        moved = []
        for k in range(0, WID - AW, 512):
            cols = pl.ds(k, 512)
            tails = jnp.concatenate([arrb[first + xx, pl.ds(64, 16), cols] for xx in range(4)], axis=0)
            moved.append(jnp.dot(move, tails, preferred_element_type=f32).astype(bf16))
        for yy in range(4):
            row = pl.multiple_of((2 * yy + c) * CH, 16)
            for i, k in enumerate(range(0, WID - AW, 512)):
                into = pl.ds(AW + k, 512)
                for xx in range(4):
                    xs[g, pl.ds(row + 16 * xx, 16), into] = arrb[
                        first + xx, pl.ds(16 * yy, 16), pl.ds(k, 512)
                    ]
                xs[g, pl.ds(row + 64, 16), into] = moved[i][16 * yy:16 * yy + 16]
            far_copy(g, yy, c).start()

    def pair_copy(g, yy):
        return pltpu.make_async_remote_copy(
            src_ref=ps.at[g, rows_of(2 * yy + 1 - c), :], dst_ref=pr.at[g, yy],
            send_sem=qsend.at[g, yy], recv_sem=qrecv.at[g, yy],
            device_id=(s, mate), device_id_type=MESH,
        )

    TURN = (2, 1, 3, 0)

    def compute(g):
        for dy in (0, -1, 1, 2):
            x_copy(g, lane(dy, 1 - c), 2, 0, t).wait_recv()
        for yy in range(4):
            far_copy(g, yy, 1 - c).wait_recv()
        if g == 0:
            for load in loads[1:]:
                load.wait()

        def block(i, carry):
            dy = jnp.where(i == 0, 2, jnp.where(i == 1, 1, jnp.where(i == 2, 3, 0)))
            yy = (y + dy) % 4
            rows = pl.ds(pl.multiple_of(yy * 2 * CH, 32), 2 * CH)
            value = xs[g, rows, :]
            both = jnp.dot(value, guw[...], preferred_element_type=f32)
            gate, upper = both[:, :640], both[:, 640:]
            act[...] = (gate / (1.0 + jnp.exp(-gate)) * upper).astype(bf16)
            ps[g, rows, :] = jnp.dot(act[...], dw[...], preferred_element_type=f32).astype(bf16)
            pair_copy(g, yy).start()
            return carry

        lax.fori_loop(0, 4, block, 0)

    def add_into(g, position, cols, terms):
        rows = rows_of(position)
        total = ps[g, rows, cols].astype(f32)
        for term in terms:
            total = total + term.astype(f32)
        ps[g, rows, cols] = total.astype(bf16)

    def r_copy(g, dy, part, send, direction, ref, sem, slot):
        cols = pl.ds(part * HW, HW)
        return pltpu.make_async_remote_copy(
            src_ref=ps.at[g, rows_of(lane(dy, c)), cols], dst_ref=ref.at[(g,) + slot],
            send_sem=rsend.at[g, send], recv_sem=sem.at[(g,) + slot],
            device_id=(s, lane(direction, c)), device_id_type=MESH,
        )

    def r_sends(g):
        return [
            (g, 2, 0, 0, 1, rh, rhrecv, (0,)), (g, 2, 1, 1, -1, rh, rhrecv, (1,)),
            (g, 1, 1, 2, 1, rf, rfrecv, (0, 1)), (g, -1, 0, 3, -1, rf, rfrecv, (1, 0)),
            (g, 1, 0, 4, 1, rf, rfrecv, (0, 0)), (g, -1, 1, 5, -1, rf, rfrecv, (1, 1)),
        ]

    def pair(g):
        todo = r_sends(g)
        for turn, dy in enumerate(TURN):
            yy = (y + dy) % 4
            pair_copy(g, yy).wait_recv()
            for k in range(2):
                cols = pl.ds(k * HW, HW)
                add_into(g, 2 * yy + c, cols, [pr[g, yy, :, cols]])
            if turn == 0:
                r_copy(*todo[0]).start()
                r_copy(*todo[1]).start()
            if turn == 1:
                r_copy(*todo[2]).start()
            if turn == 2:
                r_copy(*todo[3]).start()

    def middle(g):
        todo = r_sends(g)
        r_copy(*todo[0]).wait_recv()
        add_into(g, lane(1, c), pl.ds(0, HW), [rh[g, 0]])
        r_copy(*todo[4]).start()
        r_copy(*todo[1]).wait_recv()
        add_into(g, lane(-1, c), pl.ds(HW, HW), [rh[g, 1]])
        r_copy(*todo[5]).start()

    def finish(g):
        todo = r_sends(g)
        for k in range(2, 6):
            r_copy(*todo[k]).wait_recv()
        rows = group_rows(g)
        own = pl.multiple_of(t * CH, 16)
        extra = jnp.zeros((64, REM), f32)
        for j in range(4):
            cols = pl.ds(j * REM, REM)
            inner = pl.ds((j % 2) * REM, REM)
            total = (
                ps[g, pl.ds(own, CH), cols].astype(f32)
                + rf[g, 0, j // 2, :, inner].astype(f32)
                + rf[g, 1, j // 2, :, inner].astype(f32)
            ).astype(bf16)
            reto[rows, cols] = total[:64]
            extra = extra + lax.dot_general(fold[j], total[64:], over_rows, preferred_element_type=f32)
        reto[rows, pl.ds(WID, REM)] = extra.astype(bf16)
        for dx in (0, 1, -1, 2):
            to = at(GROUPS[g], dx)
            if (GROUPS[g], dx) == (0, 0):
                ret[band(s), :] = reto[band(s), :]
            else:
                plane_copy(reto, ret, bsend, brecv, to, s).start()

    def collect(g):
        for dx in (0, 1, -1, 2):
            if (GROUPS[g], dx) != (0, 0):
                plane_copy(reto, ret, bsend, brecv, s, at(-GROUPS[g], dx)).wait_recv()
        first = ((z - GROUPS[g] + NZ) % NZ) * 64
        rows = pl.ds(pl.multiple_of(first, 64), 64)
        low = pl.ds(pl.multiple_of(first + 256, 64), 64)
        factor = jnp.concatenate([cm[rows, :], cm[low, :]], axis=0)
        tail = ret[rows, pl.ds(WID, REM)]
        for j in range(4):
            cols = pl.ds(j * REM, REM)
            back = ret[rows, cols]
            routed = lax.dot_general(
                jnp.concatenate([factor, cr[j, rows, :], cr[j, low, :]], axis=0),
                jnp.concatenate([back, back, tail, tail], axis=0), over_rows,
                preferred_element_type=f32,
            )
            if g == 3:
                out_ref[:, cols] = (att[:, cols] + routed).astype(bf16)
            else:
                att[:, cols] = att[:, cols] + routed

    for stage, g in (
        (build, 0), (build, 1), (spread, 0), (forward, 0), (build, 2), (forward, 1),
        (build, 3), (far, 0), (gather, 0), (compute, 0), (pair, 0), (forward, 2),
        (far, 1), (gather, 1), (compute, 1), (pair, 1), (middle, 0), (forward, 3),
        (far, 2), (gather, 2), (compute, 2), (middle, 1), (pair, 2), (finish, 0),
        (far, 3), (gather, 3), (compute, 3), (middle, 2), (pair, 3), (finish, 1),
        (middle, 3), (finish, 2), (finish, 3), (collect, 0), (collect, 1), (collect, 2),
        (collect, 3),
    ):
        stage(g)

    for dz, dx in others:
        plane_copy(outg, arr, psend, precv, at(dz, dx), s).wait_send()
        plane_copy(reto, ret, bsend, brecv, at(dz, dx), s).wait_send()
        slot_copy(at(dz, dx), s).wait_send()
    for d in (1, 2, 3):
        for copy in token_copies(d):
            copy.wait_send()
    for g in range(4):
        for copy in x_sends(g):
            x_copy(*copy).wait_send()
        for yy in range(4):
            pair_copy(g, yy).wait_send()
            far_copy(g, yy, c).wait_send()
        for copy in r_sends(g):
            r_copy(*copy).wait_send()


def routed_experts(
    heads, stream, ffn_gain, routes, route_weight, out_weight, gate_weight, up_weight, down_weight
):
    any_space = pl.BlockSpec(memory_space=pltpu.HBM)
    vmem = pl.BlockSpec(memory_space=pltpu.VMEM)
    bf16, f32 = jnp.bfloat16, jnp.float32
    dma = pltpu.SemaphoreType.DMA
    return pl.pallas_call(
        expert_kernel,
        out_shape=jax.ShapeDtypeStruct((128, WID), bf16),
        in_specs=[any_space] * 9,
        out_specs=vmem,
        scratch_shapes=[
            pltpu.VMEM((128, 1024), bf16),
            pltpu.VMEM((128, WID), bf16),
            pltpu.VMEM((1, WID), f32),
            pltpu.VMEM((2, 128), jnp.int32),
            pltpu.VMEM((2, 128), f32),
            pltpu.VMEM((4, 8, 128), f32),
            pltpu.VMEM((4, 128, WID - AW), bf16),
            pltpu.VMEM((16, CH, WID - AW), bf16),
            pltpu.VMEM((16, CH, WID - AW), bf16),
            pltpu.VMEM((1024, WID), bf16),
            pltpu.VMEM((WID, 1280), bf16),
            pltpu.VMEM((640, WID), bf16),
            pltpu.VMEM((128, WID), f32),
            pltpu.VMEM((128, AW), bf16),
            pltpu.VMEM((256, AW + REMA), bf16),
            pltpu.VMEM((256, AW + REMA), bf16),
            pltpu.VMEM((256, BAND), bf16),
            pltpu.VMEM((256, BAND), bf16),
            pltpu.VMEM((4, NT * CH, WID), bf16),
            pltpu.VMEM((2 * CH, 640), bf16),
            pltpu.VMEM((4, NT * CH, WID), bf16),
            pltpu.VMEM((4, 4, CH, WID), bf16),
            pltpu.VMEM((4, 2, CH, HW), bf16),
            pltpu.VMEM((4, 2, 2, CH, HW), bf16),
            pltpu.VMEM((512, 128), bf16),
            pltpu.VMEM((4, 512, 128), bf16),
            dma((9,)),
            dma((4,)), dma((4,)), dma((4,)), dma((4,)),
            dma((16,)), dma((16,)), dma((4, 4)), dma((4, 4)),
            dma((16,)), dma((16,)),
            dma((4, 8)), dma((4, 8, 2)),
            dma((4, 4)), dma((4, 4)),
            dma((4, 6)), dma((4, 2)), dma((4, 2, 2)),
            dma((16,)), dma((16,)),
        ],
        compiler_params=pltpu.CompilerParams(
            collective_id=1, has_side_effects=True, vmem_limit_bytes=67043328
        ),
        name="experts",
    )(
        heads, stream, ffn_gain.reshape(1, -1), routes.T, route_weight.T,
        out_weight, gate_weight, up_weight, down_weight,
    )


def local(
    queries,
    key_rows,
    value_rows,
    lambdas,
    head_gain,
    out_weight,
    stream,
    ffn_gain,
    routes,
    route_weight,
    gate_weight,
    up_weight,
    down_weight,
):
    heads_local = attention(lambdas, head_gain, queries, key_rows, value_rows)
    return routed_experts(
        heads_local, stream, ffn_gain, routes, route_weight,
        out_weight, gate_weight, up_weight, down_weight,
    )


def solution(mesh):
    placed = (
        P("sp", "tp"),
        P("sp", "tp"),
        P("sp", "tp"),
        P("tp"),
        P(),
        P(),
        P(("sp", "tp"), None),
        P(),
        P(("sp", "tp"), None),
        P(("sp", "tp"), None),
        P("sp", None, "tp"),
        P("sp", None, "tp"),
        P("sp", "tp", None),
    )
    return jax.shard_map(
        local, mesh=mesh, in_specs=placed, out_specs=P(("sp", "tp"), None), check_vma=False
    )
```
